128 devices in a mesh: sp: 16 (over z, x), tp: 8 (over y, core).
Axes of the slice: x: 4, y: 4, z: 4, core: 2. Of those that a mesh axis runs over, the one named last changes fastest.
Arguments:
- query_small: bfloat16 [12288, 1024], P('sp', 'tp'), may hold values from -6 to 6
- key_small: bfloat16 [12288, 1024], P('sp', 'tp'), may hold values from -6 to 6
- value_small: bfloat16 [12288, 1024], P('sp', 'tp'), may hold values from -6 to 6
- gates_small: float32 [12288, 16], P('sp', 'tp'), as said below
- query_large: bfloat16 [12288, 1024], P('sp', 'tp'), may hold values from -6 to 6
- key_large: bfloat16 [12288, 1024], P('sp', 'tp'), may hold values from -6 to 6
- value_large: bfloat16 [12288, 1024], P('sp', 'tp'), may hold values from -6 to 6
- gates_large: float32 [12288, 8], P('sp', 'tp'), as said below
- residual: bfloat16 [12288, 2048], P(('sp', 'tp')), may hold values from -6 to 6
- mixer_small: bfloat16 [1024, 2048], P('tp'), may hold values from -1 to 1
- mixer_large: bfloat16 [1024, 2048], P('tp'), may hold values from -1 to 1
- mix_gain: float32 [2048], replicated, may hold values from 0.1 to 1.9
- value_weight: bfloat16 [2048, 5632], P('sp', 'tp'), may hold values from -0.125 to 0.125
- gate_weight: bfloat16 [2048, 5632], P('sp', 'tp'), may hold values from -0.125 to 0.125
- value_taps: float32 [3, 5632], P(None, 'tp'), may hold values from -3 to 3
- gate_taps: float32 [3, 5632], P(None, 'tp'), may hold values from -3 to 3
- down_weight: bfloat16 [5632, 2048], P('tp', 'sp'), may hold values from -0.078125 to 0.078125
- final_gain: float32 [2048], replicated, may hold values from 0.1 to 1.9
Outputs:
- layer_out: bfloat16 [12288, 2048], P(('sp', 'tp'))
The draws below stay inside these ranges and needn't reach their ends.
Inputs may be any that keep to these rules, and one draw needn't show every extreme that they name: `gates_small`: each column never rises from one position to the next, and its first entry is negative. `gates_large`: each column never rises from one position to the next, and its first entry is negative.
All inputs are finite; a program needn't handle non-finite values.
Results may differ from the reference program's by a relative error of at most 0.018.
Values may be sent and summed in bfloat16 or wider, within the bound.
A program may use at most 128 MiB of HBM per device.

```python
import math
import jax
import jax.numpy as jnp
from jax import lax

D = 2048
FF = 5632
HS = 16
DS = 64
HL = 8
DL = 128
TOK_DEV = 768
SEQUENCE_TOKENS = 12288


def plant_pair(key, head_group, head_dim, salt):
    base_level = jax.random.fold_in(key, salt)
    width = head_group * head_dim
    queries = jnp.clip(jax.random.normal(jax.random.fold_in(base_level, 1), (SEQUENCE_TOKENS, width), jnp.float32), -6.0, 6.0)
    key_rows = jnp.clip(jax.random.normal(jax.random.fold_in(base_level, 2), (SEQUENCE_TOKENS, width), jnp.float32), -6.0, 6.0)
    return (queries, key_rows)


def gate_totals(key, head_group, salt):
    base_level = jax.random.fold_in(key, salt)
    share_fast = 0.5
    rapid_decay = jax.random.uniform(jax.random.fold_in(base_level, 1), (head_group,), jnp.float32) < share_fast
    rate = jnp.where(rapid_decay, 1.0 / 40.0, 0.5 / SEQUENCE_TOKENS)
    block_count = SEQUENCE_TOKENS // TOK_DEV
    factor = jnp.exp(jax.random.uniform(jax.random.fold_in(base_level, 2), (block_count, head_group), jnp.float32, -0.7, 0.7))
    factor = jnp.repeat(factor, TOK_DEV, axis=0)
    jitter = jax.random.uniform(jax.random.fold_in(base_level, 3), (SEQUENCE_TOKENS, head_group), jnp.float32, 0.3, 1.7)
    forget_decrements = rate[None, :] * factor * jitter
    spike_locations = jax.random.randint(jax.random.fold_in(base_level, 4), (3, head_group), 0, SEQUENCE_TOKENS)
    spike_magnitudes = jax.random.uniform(jax.random.fold_in(base_level, 5), (3, head_group), jnp.float32, 0.22, 0.69)
    token_positions = jnp.arange(SEQUENCE_TOKENS)
    match_events = jnp.where(token_positions[:, None, None] == spike_locations[None, :, :], spike_magnitudes[None, :, :], 0.0)
    spike_events = jnp.sum(match_events, axis=1) * jnp.where(rapid_decay, 0.0, 1.0)[None, :]
    return jnp.cumsum(-(forget_decrements + spike_events), axis=0)


def draw_query_small(key, part):
    return plant_pair(key, HS, DS, 11)[0].astype(jnp.bfloat16)


def draw_key_small(key, part):
    return plant_pair(key, HS, DS, 11)[1].astype(jnp.bfloat16)


def draw_query_large(key, part):
    return plant_pair(key, HL, DL, 23)[0].astype(jnp.bfloat16)


def draw_key_large(key, part):
    return plant_pair(key, HL, DL, 23)[1].astype(jnp.bfloat16)


def draw_gates_small(key, part):
    return gate_totals(key, HS, 37)


def draw_gates_large(key, part):
    return gate_totals(key, HL, 41)


def shard_levels(own_key, extent, pieces, low, largest):
    factor_of = 1.0
    for position, shards_of in pieces:
        heights = jax.random.uniform(jax.random.fold_in(jax.random.fold_in(own_key, 6), position), (shards_of,), jnp.float32, low / len(pieces), largest / len(pieces))
        factor_of = factor_of * jnp.repeat(jnp.exp(heights), extent[position] // shards_of).reshape((-1,) + (1,) * (len(extent) - 1 - position))
    return factor_of


def gaussian(stream_key, extent, scale, reach, split=(), kind=jnp.bfloat16):
    array = scale * jax.random.normal(stream_key, extent, jnp.float32)
    if split:
        array = array * shard_levels(stream_key, extent, split, -0.22, 0.18)
    return jnp.clip(array, -reach, reach).astype(kind)


def setup_inputs(seed: int = 0) -> dict:
    key_list = jax.random.split(jax.random.key(seed), 19)
    return {
        "query_small": draw_query_small(jax.random.fold_in(key_list[18], 71), 0),
        "key_small": draw_key_small(jax.random.fold_in(key_list[18], 71), 0),
        "value_small": gaussian(key_list[2], (SEQUENCE_TOKENS, HS * DS), 1.0, 6.0, ((0, 16), (1, 8))),
        "gates_small": draw_gates_small(jax.random.fold_in(key_list[18], 71), 0),
        "query_large": draw_query_large(jax.random.fold_in(key_list[18], 71), 0),
        "key_large": draw_key_large(jax.random.fold_in(key_list[18], 71), 0),
        "value_large": gaussian(key_list[6], (SEQUENCE_TOKENS, HL * DL), 1.0, 6.0, ((0, 16), (1, 8))),
        "gates_large": draw_gates_large(jax.random.fold_in(key_list[18], 71), 0),
        "residual": gaussian(key_list[8], (SEQUENCE_TOKENS, D), 1.0, 6.0, ((0, 128),)),
        "mixer_small": gaussian(key_list[9], (HS * DS, D), ((HS * DS + HL * DL) // 64) ** -0.5, 1.0, ((0, 8),)),
        "mixer_large": gaussian(key_list[10], (HL * DL, D), ((HS * DS + HL * DL) // 64) ** -0.5, 1.0, ((0, 8),)),
        "mix_gain": jnp.clip(1.0 + 0.18 * jax.random.normal(key_list[11], (D,), jnp.float32), 0.1, 1.9),
        "value_weight": gaussian(key_list[12], (D, FF), D ** -0.5, 0.125, ((0, 16), (1, 8))),
        "gate_weight": gaussian(key_list[13], (D, FF), D ** -0.5, 0.125, ((0, 16), (1, 8))),
        "value_taps": gaussian(key_list[14], (3, FF), 0.577, 3.0, ((1, 8),), jnp.float32),
        "gate_taps": gaussian(key_list[15], (3, FF), 0.577, 3.0, ((1, 8),), jnp.float32),
        "down_weight": gaussian(key_list[16], (FF, D), FF ** -0.5, 0.078125, ((0, 8), (1, 16))),
        "final_gain": jnp.clip(1.0 + 0.18 * jax.random.normal(key_list[17], (D,), jnp.float32), 0.1, 1.9),
    }


residual_scale = 2.0 ** 0.5
epsilon = 1e-05

def norm_rows(values, gain):
    center = lax.optimization_barrier(jnp.mean(values, axis=-1, keepdims=True))
    spread = lax.optimization_barrier(jnp.mean(jnp.square(values - center), axis=-1, keepdims=True))
    return (values - center) * lax.rsqrt(spread + epsilon) * gain.astype(jnp.float32)

def attend(queries, key_rows, value_rows, gates, head_dim):
    total_rows = queries.shape[0]
    heads_here = gates.shape[1]
    block_rows = math.gcd(total_rows, 256)
    block_count = total_rows // block_rows
    key_heads = key_rows.astype(jnp.float32).reshape(total_rows, heads_here, head_dim)
    value_heads = value_rows.astype(jnp.float32).reshape(total_rows, heads_here, head_dim)
    query_blocks = queries.reshape(block_count, block_rows, heads_here, head_dim)
    gate_blocks = gates.reshape(block_count, block_rows, heads_here)
    key_positions = jnp.arange(total_rows)

    def one_block(inputs):
        query_part, gate_part, first_row = inputs
        scores = jnp.einsum('qhd,khd->hqk', query_part.astype(jnp.float32), key_heads) * head_dim ** (-0.5)
        scores = scores + gate_part.T[:, :, None] - gates.T[:, None, :]
        token_positions = first_row + jnp.arange(block_rows)
        allowed = token_positions[:, None] >= key_positions[None, :]
        scores = jnp.where(allowed[None], scores, -jnp.inf)
        highest = lax.optimization_barrier(jnp.max(scores, axis=-1, keepdims=True))
        weights = jnp.exp(scores - highest)
        weight_sum = lax.optimization_barrier(jnp.sum(weights, axis=-1))
        rounded = lax.optimization_barrier(weights.astype(jnp.bfloat16)).astype(jnp.float32)
        output = jnp.einsum('hqk,khd->qhd', rounded, value_heads) / weight_sum.T[:, :, None]
        return output.astype(jnp.bfloat16)
    firsts = jnp.arange(block_count) * block_rows
    output = lax.map(one_block, (query_blocks, gate_blocks, firsts))
    return output.reshape(total_rows, heads_here * head_dim)

def causal_filter(rows_in, taps):
    values = rows_in.astype(jnp.float32)
    padded = jnp.concatenate([jnp.zeros((2, values.shape[1]), jnp.float32), values], axis=0)
    return taps[0] * padded[:-2] + taps[1] * padded[1:-1] + taps[2] * padded[2:]

def reference(query_small, key_small, value_small, gates_small, query_large, key_large, value_large, gates_large, residual, mixer_small, mixer_large, mix_gain, value_weight, gate_weight, value_taps, gate_taps, down_weight, final_gain):
    small_out = attend(query_small, key_small, value_small, gates_small, DS)
    large_out = attend(query_large, key_large, value_large, gates_large, DL)
    mix = jnp.dot(small_out, mixer_small, preferred_element_type=jnp.float32) + jnp.dot(large_out, mixer_large, preferred_element_type=jnp.float32)
    mixed = norm_rows(residual_scale * residual.astype(jnp.float32) + mix, mix_gain).astype(jnp.bfloat16)
    up_value = jnp.dot(mixed, value_weight, preferred_element_type=jnp.float32).astype(jnp.bfloat16)
    up_gate = jnp.dot(mixed, gate_weight, preferred_element_type=jnp.float32).astype(jnp.bfloat16)
    filt_value = causal_filter(up_value, value_taps)
    filt_gate = causal_filter(up_gate, gate_taps)
    hidden = (jax.nn.silu(filt_gate) * filt_value).astype(jnp.bfloat16)
    ffn = jnp.dot(hidden, down_weight, preferred_element_type=jnp.float32)
    return norm_rows(residual_scale * mixed.astype(jnp.float32) + ffn, final_gain).astype(jnp.bfloat16)
```

```python
import functools

import jax
import jax.numpy as jnp
from jax import lax
from jax.experimental import pallas as pl
from jax.experimental.pallas import tpu as pltpu
from jax.sharding import Mesh
from jax.sharding import PartitionSpec as P

TP = ("tp_0", "tp_1")
SP_TP = ("sp", "tp_0", "tp_1")
LOG2E = 1.4426950408889634
residual_scale = 2.0**0.5
epsilon = 1e-05
MESH = pl.DeviceIdType.MESH
BLK = 768
EXTRA = 32
RQ = 256
F32 = jnp.float32
BF16 = jnp.bfloat16
VMEM_ALL = 60 * 1024 * 1024


def gather_attend(
    kv_ref,
    q_ref,
    up_ref,
    down_ref,
    mix_ref,
    att_ref,
    up_all,
    down_all,
    mix_all,
    kvbuf,
    qpair,
    qm,
    gq,
    gk,
    mst,
    lst,
    acc,
    outv,
    ssem,
    rsem,
    lsem,
):
    sp = lax.axis_index("sp")
    y = lax.axis_index("tp_0")
    c = lax.axis_index("tp_1")
    z, x = sp // 4, sp % 4
    role = x // 2
    xr, xl = (x + 1) % 4, (x + 3) % 4
    zu, zd = (z + 1) % 4, (z + 3) % 4
    yu, yd = (y + 1) % 4, (y + 3) % 4
    zf, yf = (z + 2) % 4, (y + 2) % 4
    mate = x + 1 - 2 * (x % 2)
    opp = 3 - x
    diag = opp + 1 - 2 * (opp % 2)
    pair_sp = 15 - sp

    def at(zz, xx):
        return (zz * 4 + xx, y, c)

    right, left = at(z, xr), at(z, xl)
    above, below = at(zu, x), at(zd, x)
    mate_dev, opp_dev = at(z, mate), at(z, opp)
    pair_dev = (pair_sp, y, c)
    y_up, y_down = (sp, yu, c), (sp, yd, c)
    sibling = (sp, y, 1 - c)
    tp = y * 2 + c

    barrier = pltpu.get_barrier_semaphore()
    for dev in (right, left, above, below, pair_dev, y_up, y_down, sibling):
        pl.semaphore_signal(barrier, inc=1, device_id=dev, device_id_type=MESH)
    pl.semaphore_wait(barrier, 8)

    sent = []
    counter = [0]
    incoming = {}

    def send(name, src, dst, dev, landing):
        k = counter[0]
        counter[0] += 1
        copy = pltpu.make_async_remote_copy(
            src_ref=src,
            dst_ref=dst,
            send_sem=ssem.at[k],
            recv_sem=rsem.at[k],
            device_id=dev,
            device_id_type=MESH,
        )
        copy.start()
        sent.append(copy)
        incoming[name] = pltpu.make_async_remote_copy(
            src_ref=landing,
            dst_ref=landing,
            send_sem=ssem.at[k],
            recv_sem=rsem.at[k],
            device_id=dev,
            device_id_type=MESH,
        )

    def take(*names):
        for name in names:
            incoming.pop(name).wait_recv()

    cols = {"own": x, "mate": mate, "opp": opp, "diag": diag}

    send("x1m", kv_ref.at[role], kvbuf.at[sp], mate_dev, kvbuf.at[z * 4 + mate])
    send("x1o", kv_ref.at[1 - role], kvbuf.at[sp], opp_dev, kvbuf.at[z * 4 + opp])
    send("wz1u_up", up_ref, up_all.at[sp], above, up_all.at[zd * 4 + x])
    send("wz1d_up", up_ref, up_all.at[sp], below, up_all.at[zu * 4 + x])
    send("wz1u_dn", down_ref, down_all.at[sp], above, down_all.at[zd * 4 + x])
    send("wz1d_dn", down_ref, down_all.at[sp], below, down_all.at[zu * 4 + x])
    send("q", q_ref.at[1 - role], qpair, pair_dev, qpair)
    send("z1u_own", kv_ref.at[role], kvbuf.at[sp], above, kvbuf.at[zd * 4 + x])
    send("z1d_own", kv_ref.at[role], kvbuf.at[sp], below, kvbuf.at[zu * 4 + x])
    send("y1u", mix_ref, mix_all.at[tp], y_up, mix_all.at[yd * 2 + c])
    send("y1d", mix_ref, mix_all.at[tp], y_down, mix_all.at[yu * 2 + c])
    send("s0", mix_ref, mix_all.at[tp], sibling, mix_all.at[y * 2 + 1 - c])

    def pass_x(tag, zz, up_src, down_src):
        row = zz * 4
        send("wx1r_up" + tag, up_src, up_all.at[row + x], right, up_all.at[row + xl])
        send("wx1l_up" + tag, up_src, up_all.at[row + x], left, up_all.at[row + xr])
        send("wx1r_dn" + tag, down_src, down_all.at[row + x], right, down_all.at[row + xl])
        send("wx1l_dn" + tag, down_src, down_all.at[row + x], left, down_all.at[row + xr])

    pass_x("0", z, up_ref, down_ref)

    locals_ = [
        pltpu.make_async_copy(kv_ref.at[role], kvbuf.at[sp], lsem.at[0]),
        pltpu.make_async_copy(up_ref, up_all.at[sp], lsem.at[1]),
        pltpu.make_async_copy(down_ref, down_all.at[sp], lsem.at[2]),
        pltpu.make_async_copy(mix_ref, mix_all.at[tp], lsem.at[3]),
    ]
    for copy in locals_:
        copy.start()

    heads = 2 - role
    head_dim = 64 + 64 * role
    scale = jnp.where(role == 0, 0.125 * LOG2E, 128.0**-0.5 * LOG2E).astype(F32)
    lane = lax.broadcasted_iota(jnp.int32, (1, 128), 1)

    def head_lanes(h):
        return (lane >= h * 64) & (lane < h * 64 + head_dim)

    def load_queries(qi, ref):
        packed = ref[:, 128:256].astype(F32)
        for h in range(2):
            keep = jnp.where(head_lanes(h), 1.0, 0.0).astype(BF16)
            qm[qi, h] = ref[:, 0:128] * keep
            mine = (lane >= 3 * h) & (lane < 3 * h + 3)
            total = jnp.sum(jnp.where(mine, packed, 0.0), axis=1, keepdims=True)
            gq[qi, h] = jnp.broadcast_to(total, (BLK, 128))

    load_queries(0, q_ref.at[role])
    mst[...] = jnp.full(mst.shape, -1e30, F32)
    lst[...] = jnp.zeros(lst.shape, F32)
    acc[...] = jnp.zeros(acc.shape, F32)

    def pass_z(tag):
        col = cols[tag]
        send("z1u_" + tag, kvbuf.at[z * 4 + col], kvbuf.at[z * 4 + col], above, kvbuf.at[zd * 4 + col])
        send("z1d_" + tag, kvbuf.at[z * 4 + col], kvbuf.at[z * 4 + col], below, kvbuf.at[zu * 4 + col])

    take("x1o")
    send("x2", kvbuf.at[z * 4 + opp], kvbuf.at[z * 4 + opp], mate_dev, kvbuf.at[z * 4 + diag])
    take("x1m")
    take("wz1u_up", "wz1d_up", "wz1u_dn", "wz1d_dn")
    b_d, b_u, b_f = zd * 4 + x, zu * 4 + x, zf * 4 + x
    top, rest = pl.ds(0, 96), pl.ds(96, 32)
    send("wz2u", up_all.at[b_d, top], up_all.at[b_d, top], above, up_all.at[b_f, top])
    send("wz2d", up_all.at[b_u, rest], up_all.at[b_u, rest], below, up_all.at[b_f, rest])
    send("wz2dd", down_all.at[b_u], down_all.at[b_u], below, down_all.at[b_f])
    pass_z("mate")
    pass_z("opp")
    pass_x("d", zd, up_all.at[b_d], down_all.at[b_d])
    pass_x("u", zu, up_all.at[b_u], down_all.at[b_u])
    take("x2")
    pass_z("diag")
    take("q")
    load_queries(1, qpair)
    take("wz2u", "wz2d", "wz2dd")
    pass_x("f", zf, up_all.at[b_f], down_all.at[b_f])
    locals_[0].wait()

    def gate_rows(j):
        rows = kvbuf[j, BLK : BLK + EXTRA, :].astype(F32)
        for h in range(2):
            for p in range(3):
                k = h * 9 + p
                g = rows[k : k + 1] + rows[k + 3 : k + 4] + rows[k + 6 : k + 7]
                gk[j * 2 + h, :, p * 256 : (p + 1) * 256] = jnp.broadcast_to(g, (8, 256))

    def tile(qi, qblk, j, h, sub, masked):
        r0 = pl.multiple_of(sub * RQ, RQ)
        rows = pl.ds(r0, RQ)
        keep = head_lanes(h)
        q = qm[qi, h, rows, :]
        s = lax.dot_general(
            q, kvbuf[j, 0:BLK, 0:128], (((1,), (1,)), ((), ())), preferred_element_type=F32
        )
        gate = gk[j * 2 + h, 0:1, :]
        parts = []
        for g in range(BLK // 128):
            part = s[:, g * 128 : (g + 1) * 128] * scale - gate[:, g * 128 : (g + 1) * 128]
            if masked:
                col = lax.broadcasted_iota(jnp.int32, (RQ, 128), 1) + g * 128
                row = lax.broadcasted_iota(jnp.int32, (RQ, 128), 0) + sub * RQ
                part = jnp.where(col <= row, part, -1e30)
            parts.append(part)
        peak = functools.reduce(jnp.maximum, parts)
        peak = jnp.max(peak, axis=1, keepdims=True)
        g_here = gq[qi, h, rows, :]
        old = mst[qi, h, rows, :]
        new = jnp.maximum(old, peak + g_here)
        alpha = jnp.exp2(old - new)
        shift = new - g_here
        weights = [jnp.exp2(part - shift) for part in parts]
        mst[qi, h, rows, :] = new
        lst[qi, h, rows, :] = lst[qi, h, rows, :] * alpha + functools.reduce(jnp.add, weights)
        w = jnp.concatenate([a.astype(BF16) for a in weights], axis=1)
        v = kvbuf[j, 0:BLK, 128:256] * jnp.where(keep, 1.0, 0.0).astype(BF16)
        update = jnp.dot(w, v, preferred_element_type=F32)
        acc[qi, rows, :] = acc[qi, rows, :] * jnp.where(keep, alpha, 1.0) + update

    def attend_row(zz):
        for xx in range(4):
            gate_rows(zz * 4 + xx)

        def for_queries(qi, _):
            qblk = jnp.where(qi == 0, sp, pair_sp)
            full = jnp.clip(qblk - 4 * zz, 0, 4)

            def for_block(jj, _):
                def for_head(h, _):
                    def for_rows(sub, _):
                        tile(qi, qblk, zz * 4 + jj, h, sub, False)
                        return 0

                    return lax.fori_loop(0, BLK // RQ, for_rows, 0)

                return lax.fori_loop(0, heads, for_head, 0)

            lax.fori_loop(0, full, for_block, 0)

            @pl.when(qblk // 4 == zz)
            def _():
                def for_head(h, _):
                    def for_rows(sub, _):
                        tile(qi, qblk, qblk, h, sub, True)
                        return 0

                    return lax.fori_loop(0, BLK // RQ, for_rows, 0)

                lax.fori_loop(0, heads, for_head, 0)

            return 0

        lax.fori_loop(0, 2, for_queries, 0)

    attend_row(z)

    def pass_on(tag, name, from_z, dev, landing_z):
        col = cols[tag]
        src = kvbuf.at[from_z * 4 + col]
        send(name + tag, src, src, dev, kvbuf.at[landing_z * 4 + col])

    take("z1u_own", "z1d_own", "z1u_mate", "z1d_mate")
    pass_on("own", "z2u_", zd, above, zf)
    pass_on("mate", "z2u_", zd, above, zf)
    take("z1u_opp", "z1d_opp", "z1u_diag", "z1d_diag")
    pass_on("opp", "z2d_", zu, below, zf)
    pass_on("diag", "z2d_", zu, below, zf)

    take("y1u", "y1d")
    m_d, m_u, m_f = yd * 2 + c, yu * 2 + c, yf * 2 + c
    s_d, s_u, s_f = yd * 2 + 1 - c, yu * 2 + 1 - c, yf * 2 + 1 - c
    first, second = pl.ds(0, 128), pl.ds(128, 128)
    send("y2u", mix_all.at[m_d, first], mix_all.at[m_d, first], y_up, mix_all.at[m_f, first])
    send("y2d", mix_all.at[m_u, second], mix_all.at[m_u, second], y_down, mix_all.at[m_f, second])
    send("s1", mix_all.at[m_d], mix_all.at[m_d], sibling, mix_all.at[s_d])
    send("s2", mix_all.at[m_u], mix_all.at[m_u], sibling, mix_all.at[s_u])

    attend_row(zd)

    def pass_x2(tag, zz, name, col, dev, landing):
        for kind, whole in (("_up", up_all), ("_dn", down_all)):
            src = whole.at[zz * 4 + col]
            send(name + kind + tag, src, src, dev, whole.at[zz * 4 + landing])

    xf = (x + 2) % 4
    for tag in ("0", "d"):
        take("wx1r_up" + tag, "wx1r_dn" + tag, "wx1l_up" + tag, "wx1l_dn" + tag)
    pass_x2("0", z, "wx2r", xl, right, xf)
    pass_x2("d", zd, "wx2r", xl, right, xf)

    attend_row(zu)

    for tag in ("u", "f"):
        take("wx1r_up" + tag, "wx1r_dn" + tag, "wx1l_up" + tag, "wx1l_dn" + tag)
    pass_x2("u", zu, "wx2l", xr, left, xf)
    pass_x2("f", zf, "wx2l", xr, left, xf)
    take("y2u", "y2d")
    send("s3", mix_all.at[m_f], mix_all.at[m_f], sibling, mix_all.at[s_f])
    take("z2u_own", "z2u_mate", "z2d_opp", "z2d_diag")

    attend_row(zf)

    keep0 = head_lanes(0)
    for qi in (1, 0):
        l0 = jnp.sum(lst[qi, 0], axis=1, keepdims=True)
        l1 = jnp.sum(lst[qi, 1], axis=1, keepdims=True)
        outv[qi] = (acc[qi] / jnp.where(keep0, l0, l1)).astype(BF16)
    send("out", outv.at[1], att_ref.at[role], pair_dev, att_ref.at[1 - role])
    own_out = pltpu.make_async_copy(outv.at[0], att_ref.at[role], lsem.at[4])
    own_out.start()
    take(*list(incoming))
    own_out.wait()
    for copy in locals_[1:]:
        copy.wait()
    for copy in sent:
        copy.wait_send()


def gather_and_attend(kv, q, up, down, mixers):
    any_ = pl.BlockSpec(memory_space=pl.ANY)
    vmem = pl.BlockSpec(memory_space=pltpu.VMEM)
    return pl.pallas_call(
        gather_attend,
        out_shape=(
            jax.ShapeDtypeStruct((2, BLK, 128), BF16),
            jax.ShapeDtypeStruct((16, *up.shape), BF16),
            jax.ShapeDtypeStruct((16, *down.shape), BF16),
            jax.ShapeDtypeStruct((8, *mixers.shape), BF16),
        ),
        in_specs=[vmem] * 5,
        out_specs=(any_,) * 4,
        scratch_shapes=[
            pltpu.VMEM((16, BLK + EXTRA, 256), BF16),
            pltpu.VMEM((BLK, 256), BF16),
            pltpu.VMEM((2, 2, BLK, 128), BF16),
            pltpu.VMEM((2, 2, BLK, 128), F32),
            pltpu.VMEM((32, 8, BLK), F32),
            pltpu.VMEM((2, 2, BLK, 128), F32),
            pltpu.VMEM((2, 2, BLK, 128), F32),
            pltpu.VMEM((2, BLK, 128), F32),
            pltpu.VMEM((2, BLK, 128), BF16),
            pltpu.SemaphoreType.DMA((72,)),
            pltpu.SemaphoreType.DMA((72,)),
            pltpu.SemaphoreType.DMA((8,)),
        ],
        compiler_params=pltpu.CompilerParams(
            collective_id=1, has_side_effects=True, vmem_limit_bytes=VMEM_ALL
        ),
        cost_estimate=pl.CostEstimate(flops=20_000_000_000, bytes_accessed=40_000_000, transcendentals=0),
    )(kv, q, up, down, mixers)


def three_parts(gates):
    scaled = gates * LOG2E
    high = lax.reduce_precision(scaled, 8, 7)
    middle = lax.reduce_precision(scaled - high, 8, 7)
    low = lax.reduce_precision(scaled - high - middle, 8, 7)
    return jnp.stack([high, middle, low], axis=1).astype(BF16)


def packed_inputs(query, keys, values, gates):
    rows = keys.shape[0]
    parts = three_parts(gates)
    heads = gates.shape[1]
    by_lane = parts.transpose(2, 1, 0).reshape(heads * 9, 256)
    by_lane = jnp.pad(by_lane, ((0, EXTRA - heads * 9), (0, 0)))
    kv = jnp.concatenate([jnp.concatenate([keys, values], axis=1), by_lane], axis=0)
    by_row = parts.transpose(0, 2, 1).reshape(rows, heads * 3)
    by_row = jnp.pad(by_row, ((0, 0), (0, 128 - heads * 3)))
    return kv, jnp.concatenate([query, by_row], axis=1)


def split_up(array, dim, devices):
    shape = array.shape
    pieces = array.reshape(*shape[:dim], devices, shape[dim] // devices, *shape[dim + 1 :])
    return jnp.moveaxis(pieces, dim, 0)


def laid_out(pieces, dim):
    shape = list(pieces.shape[1:])
    shape[dim] *= pieces.shape[0]
    return jnp.moveaxis(pieces, 0, dim).reshape(shape)


def moved_by_axis(pieces, axes, turns):
    shape = [lax.axis_size(a) for a in axes]
    pieces = pieces.reshape(*shape, *pieces.shape[1:])
    for k in turns:
        pieces = lax.all_to_all(pieces, axes[k], split_axis=k, concat_axis=k, tiled=True)
    return pieces.reshape(-1, *pieces.shape[len(axes) :])


def stepwise_exchange(array, axes, turns, split_dim, concat_dim):
    pieces = split_up(array, split_dim, lax.axis_size(axes))
    return laid_out(moved_by_axis(pieces, axes, turns), concat_dim)


def passed_along(value, axis, steps):
    count = lax.axis_size(axis)
    first, last = (max(0, -steps), min(count, count - steps))
    return lax.ppermute(value, axis, [(source, source + steps) for source in range(first, last)])


def norm_rows(values, gain):
    center = jnp.mean(values, axis=-1, keepdims=True)
    spread = jnp.mean(jnp.square(values - center), axis=-1, keepdims=True)
    return (values - center) * lax.rsqrt(spread + epsilon) * gain


def per_device(
    query_small,
    key_small,
    value_small,
    gates_small,
    query_large,
    key_large,
    value_large,
    gates_large,
    residual,
    mixer_small,
    mixer_large,
    mix_gain,
    value_weight,
    gate_weight,
    value_taps,
    gate_taps,
    down_weight,
    final_gain,
):
    shard_rows = query_small.shape[0]
    kv_s, q_s = packed_inputs(query_small, key_small, value_small, gates_small)
    kv_l, q_l = packed_inputs(query_large, key_large, value_large, gates_large)
    up = jnp.concatenate(
        [value_weight[:, :640], gate_weight[:, :640], value_weight[:, 640:], gate_weight[:, 640:]],
        axis=1,
    )
    mixers = jnp.concatenate([mixer_small, mixer_large], axis=0)
    att, up_all, down_all, mix_all = gather_and_attend(
        jnp.stack([kv_s, kv_l]), jnp.stack([q_s, q_l]), up, down_weight, mixers
    )
    up_all = up_all.reshape(-1, up_all.shape[2])
    mix_all = mix_all.reshape(-1, mix_all.shape[2])
    joined = jnp.concatenate([att[0], att[1]], axis=1)
    tensor_parts = lax.axis_size(TP)
    own_rows = shard_rows // tensor_parts
    arrived = stepwise_exchange(joined, TP, (1, 0), 0, 1)
    mix = jnp.dot(arrived.reshape(own_rows, -1), mix_all, preferred_element_type=jnp.float32)
    mixed = norm_rows(residual_scale * residual.astype(jnp.float32) + mix, mix_gain).astype(
        jnp.bfloat16
    )
    block_input = lax.all_gather(mixed, TP, axis=0, tiled=True)
    both = jnp.dot(block_input, up_all, preferred_element_type=jnp.float32).astype(jnp.bfloat16)
    taps = jnp.concatenate(
        [value_taps[:, :640], gate_taps[:, :640], value_taps[:, 640:], gate_taps[:, 640:]], axis=1
    )
    earlier = passed_along(both[-2:], "sp", 1)
    padded = jnp.concatenate([earlier, both], axis=0).astype(jnp.float32)
    filt = taps[0] * padded[:-2] + taps[1] * padded[1:-1] + taps[2] * padded[2:]
    filt_value = jnp.concatenate([filt[:, :640], filt[:, 1280:1344]], axis=1)
    filt_gate = jnp.concatenate([filt[:, 640:1280], filt[:, 1344:]], axis=1)
    hidden = (jax.nn.silu(filt_gate) * filt_value).astype(jnp.bfloat16)
    whole_down = down_all.transpose(1, 0, 2).reshape(down_all.shape[1], -1)
    ffn_terms = jnp.dot(hidden, whole_down, preferred_element_type=jnp.float32)
    ffn = lax.psum_scatter(
        ffn_terms.astype(jnp.bfloat16), TP, scatter_dimension=0, tiled=True
    ).astype(jnp.float32)
    return norm_rows(residual_scale * mixed.astype(jnp.float32) + ffn, final_gain).astype(
        jnp.bfloat16
    )


def solution(mesh):
    split = Mesh(mesh.devices.reshape(mesh.shape["sp"], 4, 2), ("sp", "tp_0", "tp_1"))
    placed = (
        P("sp", TP),
        P("sp", TP),
        P("sp", TP),
        P("sp", TP),
        P("sp", TP),
        P("sp", TP),
        P("sp", TP),
        P("sp", TP),
        P(SP_TP, None),
        P(TP, None),
        P(TP, None),
        P(),
        P("sp", TP),
        P("sp", TP),
        P(None, TP),
        P(None, TP),
        P(TP, "sp"),
        P(),
    )
    return jax.shard_map(
        per_device, mesh=split, in_specs=placed, out_specs=P(SP_TP, None), check_vma=False
    )
```

```python
import functools

import jax
import jax.numpy as jnp
from jax import lax
from jax.experimental import pallas as pl
from jax.experimental.pallas import tpu as pltpu
from jax.sharding import Mesh
from jax.sharding import PartitionSpec as P

TP = ("tp_0", "tp_1")
SP_TP = ("sp", "tp_0", "tp_1")
LOG2E = 1.4426950408889634
residual_scale = 2.0**0.5
epsilon = 1e-05
MESH = pl.DeviceIdType.MESH
BLK = 768
EXTRA = 32
RQ = 256
F32 = jnp.float32
BF16 = jnp.bfloat16
VMEM_ALL = 67_000_000
OWN = 96
HALF = 1024


def layer_kernel(
    qs_ref,
    ks_ref,
    vs_ref,
    ql_ref,
    kl_ref,
    vl_ref,
    gs_ref,
    gl_ref,
    lanes_ref,
    vw_ref,
    gw_ref,
    down_ref,
    ms_ref,
    ml_ref,
    res_ref,
    mgain_ref,
    fgain_ref,
    taps_ref,
    out_ref,
    kvin,
    qin,
    kvbuf,
    qpair,
    qm,
    gq,
    gk,
    mst,
    lst,
    acc,
    outv,
    upbuf,
    downbuf,
    mixbuf,
    arrived,
    ybuf,
    mixed,
    both,
    halo,
    hid,
    keep,
    sib_out,
    sib_in,
    far_out,
    far_in,
    near_out,
    near_in,
    ssem,
    rsem,
    lsem,
):
    sp = lax.axis_index("sp")
    y = lax.axis_index("tp_0")
    c = lax.axis_index("tp_1")
    z, x = sp // 4, sp % 4
    role = x // 2
    xr, xl = (x + 1) % 4, (x + 3) % 4
    zu, zd = (z + 1) % 4, (z + 3) % 4
    yu, yd = (y + 1) % 4, (y + 3) % 4
    xf, zf, yf = (x + 2) % 4, (z + 2) % 4, (y + 2) % 4
    mate = x + 1 - 2 * (x % 2)
    opp = 3 - x
    diag = opp + 1 - 2 * (opp % 2)
    pair_sp = 15 - sp
    tp = y * 2 + c

    def at(zz, xx):
        return (zz * 4 + xx, y, c)

    right, left = at(z, xr), at(z, xl)
    above, below = at(zu, x), at(zd, x)
    mate_dev, opp_dev = at(z, mate), at(z, opp)
    pair_dev = (pair_sp, y, c)
    y_up, y_down = (sp, yu, c), (sp, yd, c)
    sibling = (sp, y, 1 - c)
    after, before = ((sp + 1) % 16, y, c), ((sp + 15) % 16, y, c)

    barrier = pltpu.get_barrier_semaphore()
    greeted = [right, left, above, below, after, before]
    for d in range(8):
        t = (tp + d) % 8
        if d:
            greeted.append((sp, t // 2, t % 2))
        greeted.append((pair_sp, t // 2, t % 2))
    for dev in greeted:
        pl.semaphore_signal(barrier, inc=1, device_id=dev, device_id_type=MESH)

    lane = lax.broadcasted_iota(jnp.int32, (1, 128), 1)

    for r, (q_ref, k_ref, v_ref, g_ref) in enumerate(
        ((qs_ref, ks_ref, vs_ref, gs_ref), (ql_ref, kl_ref, vl_ref, gl_ref))
    ):
        kvin[r, 0:BLK, 0:128] = k_ref[...]
        kvin[r, 0:BLK, 128:256] = v_ref[...]
        kvin[r, BLK : BLK + EXTRA, :] = lanes_ref[r]
        qin[r, :, 0:128] = q_ref[...]
        packed = jnp.zeros((BLK, 128), F32)
        for h in range(2 - r):
            col = g_ref[:, h : h + 1] * LOG2E
            for i in range(3):
                part = col.astype(BF16).astype(F32)
                packed = jnp.where(lane == 3 * h + i, part, packed)
                col = col - part
        qin[r, :, 128:256] = packed.astype(BF16)

    def up_rows(b, start=0, size=128):
        return upbuf.at[pl.ds(pl.multiple_of(b * 128 + start, 32), size)]

    def down_cols(b):
        return downbuf.at[pl.ds(0, 704), pl.ds(pl.multiple_of(b * 128, 128), 128)]

    def mix_rows(t, start=0, size=256):
        return mixbuf.at[pl.ds(pl.multiple_of(t * 256 + start, 128), size)]

    mine = pl.ds(pl.multiple_of(sp * 128, 128), 128)
    upbuf[mine, 0:640] = vw_ref[:, 0:640]
    upbuf[mine, 640:1280] = gw_ref[:, 0:640]
    upbuf[mine, 1280:1408] = jnp.concatenate([vw_ref[:, 640:704], gw_ref[:, 640:704]], axis=1)
    mixbuf[pl.ds(pl.multiple_of(tp * 256, 256), 128), :] = ms_ref[...]
    mixbuf[pl.ds(pl.multiple_of(tp * 256 + 128, 128), 128), :] = ml_ref[...]
    downbuf[704:768, :] = jnp.zeros((64, 2048), BF16)

    pl.semaphore_wait(barrier, len(greeted))

    sent = []
    counter = [0]
    incoming = {}

    def send(name, ends):
        k = counter[0]
        counter[0] += 1

        def copy(arriving):
            src, dst, dev, landing = ends()
            return pltpu.make_async_remote_copy(
                src_ref=landing if arriving else src,
                dst_ref=landing if arriving else dst,
                send_sem=ssem.at[k],
                recv_sem=rsem.at[k],
                device_id=dev,
                device_id_type=MESH,
            )

        copy(False).start()
        sent.append(copy)
        incoming[name] = copy

    def take(*names):
        for name in names:
            incoming.pop(name)(True).wait_recv()

    cols = {"own": x, "mate": mate, "opp": opp, "diag": diag}

    send("x1m", lambda: (kvin.at[role], kvbuf.at[sp], mate_dev, kvbuf.at[z * 4 + mate]))
    send("x1o", lambda: (kvin.at[1 - role], kvbuf.at[sp], opp_dev, kvbuf.at[z * 4 + opp]))
    send("wz1u_up", lambda: (up_rows(sp), up_rows(sp), above, up_rows(zd * 4 + x)))
    send("wz1d_up", lambda: (up_rows(sp), up_rows(sp), below, up_rows(zu * 4 + x)))
    send("wz1u_dn", lambda: (down_ref, down_cols(sp), above, down_cols(zd * 4 + x)))
    send("wz1d_dn", lambda: (down_ref, down_cols(sp), below, down_cols(zu * 4 + x)))
    send("q", lambda: (qin.at[1 - role], qpair, pair_dev, qpair))
    send("z1u_own", lambda: (kvin.at[role], kvbuf.at[sp], above, kvbuf.at[zd * 4 + x]))
    send("z1d_own", lambda: (kvin.at[role], kvbuf.at[sp], below, kvbuf.at[zu * 4 + x]))
    send("y1u", lambda: (mix_rows(tp), mix_rows(tp), y_up, mix_rows(yd * 2 + c)))
    send("y1d", lambda: (mix_rows(tp), mix_rows(tp), y_down, mix_rows(yu * 2 + c)))
    send("s0", lambda: (mix_rows(tp), mix_rows(tp), sibling, mix_rows(y * 2 + 1 - c)))

    def pass_x(tag, zz, down_src=None):
        b, b_l, b_r = zz * 4 + x, zz * 4 + xl, zz * 4 + xr
        down_src = down_cols(b) if down_src is None else down_src
        send("wx1r_up" + tag, lambda: (up_rows(b), up_rows(b), right, up_rows(b_l)))
        send("wx1l_up" + tag, lambda: (up_rows(b), up_rows(b), left, up_rows(b_r)))
        send("wx1r_dn" + tag, lambda: (down_src, down_cols(b), right, down_cols(b_l)))
        send("wx1l_dn" + tag, lambda: (down_src, down_cols(b), left, down_cols(b_r)))

    pass_x("0", z, down_ref)

    own_kv = pltpu.make_async_copy(kvin.at[role], kvbuf.at[sp], lsem.at[0])
    own_down = pltpu.make_async_copy(down_ref, down_cols(sp), lsem.at[1])
    own_kv.start()
    own_down.start()

    heads = 2 - role
    head_dim = 64 + 64 * role
    scale = jnp.where(role == 0, 0.125 * LOG2E, 128.0**-0.5 * LOG2E).astype(F32)

    def head_lanes(h):
        return (lane >= h * 64) & (lane < h * 64 + head_dim)

    def load_queries(qi, ref):
        packed = ref[:, 128:256].astype(F32)
        for h in range(2):
            ones = jnp.where(head_lanes(h), 1.0, 0.0).astype(BF16)
            qm[qi, h] = ref[:, 0:128] * ones
            picked = (lane >= 3 * h) & (lane < 3 * h + 3)
            total = jnp.sum(jnp.where(picked, packed, 0.0), axis=1, keepdims=True)
            gq[qi, h] = jnp.broadcast_to(total, (BLK, 128))

    load_queries(0, qin.at[role])
    mst[...] = jnp.full(mst.shape, -1e30, F32)
    lst[...] = jnp.zeros(lst.shape, F32)
    acc[...] = jnp.zeros(acc.shape, F32)

    def pass_z(tag):
        col = cols[tag]
        src = kvbuf.at[z * 4 + col]
        send("z1u_" + tag, lambda: (src, src, above, kvbuf.at[zd * 4 + col]))
        send("z1d_" + tag, lambda: (src, src, below, kvbuf.at[zu * 4 + col]))

    take("x1o")
    send("x2", lambda: (kvbuf.at[z * 4 + opp], kvbuf.at[z * 4 + opp], mate_dev, kvbuf.at[z * 4 + diag]))
    take("x1m")
    take("wz1u_up", "wz1d_up", "wz1u_dn", "wz1d_dn")
    b_d, b_u, b_f = zd * 4 + x, zu * 4 + x, zf * 4 + x
    send("wz2u", lambda: (up_rows(b_d, 0, 96), up_rows(b_d, 0, 96), above, up_rows(b_f, 0, 96)))
    send("wz2d", lambda: (up_rows(b_u, 96, 32), up_rows(b_u, 96, 32), below, up_rows(b_f, 96, 32)))
    send("wz2dd", lambda: (down_cols(b_u), down_cols(b_u), below, down_cols(b_f)))
    pass_z("mate")
    pass_z("opp")
    pass_x("d", zd)
    pass_x("u", zu)
    take("x2")
    pass_z("diag")
    take("q")
    load_queries(1, qpair)
    take("wz2u", "wz2d", "wz2dd")
    pass_x("f", zf)
    own_kv.wait()

    def gate_rows(j):
        rows = kvbuf[j, BLK : BLK + EXTRA, :].astype(F32)
        for h in range(2):
            for p in range(3):
                k = h * 9 + p
                g = rows[k : k + 1] + rows[k + 3 : k + 4] + rows[k + 6 : k + 7]
                gk[j * 2 + h, :, p * 256 : (p + 1) * 256] = jnp.broadcast_to(g, (8, 256))

    def tile(qi, j, h, sub, masked):
        rows = pl.ds(sub * RQ, RQ)
        span = (sub + 1) * RQ if masked else BLK
        mask = head_lanes(h)
        s = lax.dot_general(
            qm[qi, h, rows, :],
            kvbuf[j, 0:span, 0:128],
            (((1,), (1,)), ((), ())),
            preferred_element_type=F32,
        )
        gate = gk[j * 2 + h, 0:1, 0:span]
        parts = []
        for g in range(span // 128):
            part = s[:, g * 128 : (g + 1) * 128] * scale - gate[:, g * 128 : (g + 1) * 128]
            if masked and (g + 1) * 128 > sub * RQ:
                col = lax.broadcasted_iota(jnp.int32, (RQ, 128), 1) + (g * 128 - sub * RQ)
                row = lax.broadcasted_iota(jnp.int32, (RQ, 128), 0)
                part = jnp.where(col <= row, part, -1e30)
            parts.append(part)
        peak = functools.reduce(jnp.maximum, parts)
        peak = jnp.max(peak, axis=1, keepdims=True)
        g_here = gq[qi, h, rows, :]
        old = mst[qi, h, rows, :]
        new = jnp.maximum(old, peak + g_here)
        alpha = jnp.exp2(old - new)
        shift = new - g_here
        weights = [jnp.exp2(part - shift) for part in parts]
        mst[qi, h, rows, :] = new
        lst[qi, h, rows, :] = lst[qi, h, rows, :] * alpha + functools.reduce(jnp.add, weights)
        w = jnp.concatenate([a.astype(BF16) for a in weights], axis=1)
        v = kvbuf[j, 0:span, 128:256] * jnp.where(mask, 1.0, 0.0).astype(BF16)
        update = jnp.dot(w, v, preferred_element_type=F32)
        acc[qi, rows, :] = acc[qi, rows, :] * jnp.where(mask, alpha, 1.0) + update

    def attend_row(zz):
        for xx in range(4):
            gate_rows(zz * 4 + xx)

        def for_queries(qi, _):
            qblk = jnp.where(qi == 0, sp, pair_sp)
            full = jnp.clip(qblk - 4 * zz, 0, 4)

            def for_block(jj, _):
                def for_head(h, _):
                    for sub in range(BLK // RQ):
                        tile(qi, zz * 4 + jj, h, sub, False)
                    return 0

                return lax.fori_loop(0, heads, for_head, 0)

            lax.fori_loop(0, full, for_block, 0)

            @pl.when(qblk // 4 == zz)
            def _():
                def for_head(h, _):
                    for sub in range(BLK // RQ):
                        tile(qi, qblk, h, sub, True)
                    return 0

                lax.fori_loop(0, heads, for_head, 0)

            return 0

        lax.fori_loop(0, 2, for_queries, 0)

    def pass_on(tag, name, from_z, dev, landing_z):
        col = cols[tag]

        def ends():
            src = kvbuf.at[from_z * 4 + col]
            return src, src, dev, kvbuf.at[landing_z * 4 + col]

        send(name + tag, ends)

    m_d, m_u, m_f = yd * 2 + c, yu * 2 + c, yf * 2 + c
    s_d, s_u, s_f = yd * 2 + 1 - c, yu * 2 + 1 - c, yf * 2 + 1 - c

    def pass_x2(tag, zz, name, col, dev):

        def ends(part):
            src = part(zz * 4 + col)
            return src, src, dev, part(zz * 4 + xf)

        send(name + "_up" + tag, lambda: ends(up_rows))
        send(name + "_dn" + tag, lambda: ends(down_cols))

    def one_row(step, _):
        offset = jnp.where(step == 1, 3, jnp.where(step == 2, 1, jnp.where(step == 3, 2, 0)))
        attend_row((z + offset) % 4)

        @pl.when(step == 0)
        def _():
            take("z1u_own", "z1d_own", "z1u_mate", "z1d_mate")
            pass_on("own", "z2u_", zd, above, zf)
            pass_on("mate", "z2u_", zd, above, zf)
            take("z1u_opp", "z1d_opp", "z1u_diag", "z1d_diag")
            pass_on("opp", "z2d_", zu, below, zf)
            pass_on("diag", "z2d_", zu, below, zf)
            take("y1u", "y1d")
            send("y2u", lambda: (mix_rows(m_d, 0, 128), mix_rows(m_d, 0, 128), y_up, mix_rows(m_f, 0, 128)))
            send("y2d", lambda: (mix_rows(m_u, 128, 128), mix_rows(m_u, 128, 128), y_down, mix_rows(m_f, 128, 128)))
            send("s1", lambda: (mix_rows(m_d), mix_rows(m_d), sibling, mix_rows(s_d)))
            send("s2", lambda: (mix_rows(m_u), mix_rows(m_u), sibling, mix_rows(s_u)))

        @pl.when(step == 2)
        def _():
            for tag in ("0", "d", "u", "f"):
                take("wx1r_up" + tag, "wx1r_dn" + tag, "wx1l_up" + tag, "wx1l_dn" + tag)
            pass_x2("0", z, "wx2r", xl, right)
            pass_x2("u", zu, "wx2l", xr, left)
            take("y2u", "y2d")
            send("s3", lambda: (mix_rows(m_f), mix_rows(m_f), sibling, mix_rows(s_f)))
            take("z2u_own", "z2u_mate", "z2d_opp", "z2d_diag")

        return 0

    lax.fori_loop(0, 4, one_row, 0)

    keep0 = head_lanes(0)
    for qi in (1, 0):
        l0 = jnp.sum(lst[qi, 0], axis=1, keepdims=True)
        l1 = jnp.sum(lst[qi, 1], axis=1, keepdims=True)
        outv[qi] = (acc[qi] / jnp.where(keep0, l0, l1)).astype(BF16)

    def own_rows(t):
        return pl.ds(pl.multiple_of(t * OWN, 32), OWN)

    slot = tp * 2 + role

    def send_out(d):
        t, s = (tp + d) % 8, (tp + 8 - d) % 8
        dst = (t // 2, t % 2)
        send(
            "p%d" % d,
            lambda: (outv.at[1, own_rows(t)], arrived.at[slot], (pair_sp, *dst), arrived.at[s * 2 + 1 - role]),
        )
        if d:
            send(
                "a%d" % d,
                lambda: (outv.at[0, own_rows(t)], arrived.at[slot], (sp, *dst), arrived.at[s * 2 + role]),
            )

    for d in range(8):
        send_out(d)
    pass_x2("d", zd, "wx2r", xl, right)
    pass_x2("f", zf, "wx2l", xr, left)
    arrived[slot] = outv[0, own_rows(tp), :]
    take("s0", "s1", "s2", "s3")
    for d in range(8):
        take("p%d" % d)
        if d:
            take("a%d" % d)

    def project(i, _):
        col = pl.ds(pl.multiple_of(i * 256, 256), 256)
        lhs = jnp.concatenate([arrived[s] for s in range(16)], axis=1)
        part = jnp.dot(lhs, mixbuf[:, col], preferred_element_type=F32)
        ybuf[:, col] = residual_scale * res_ref[:, col].astype(F32) + part
        return 0

    lax.fori_loop(0, 8, project, 0)

    def norm(values, gain):
        center = jnp.mean(values, axis=1, keepdims=True)
        off = values - center
        spread = jnp.mean(jnp.square(off), axis=1, keepdims=True)
        return off * lax.rsqrt(spread + epsilon) * gain

    def first_norm(i, _):
        r = pl.ds(pl.multiple_of(i * 16, 16), 16)
        t = pl.ds(pl.multiple_of(tp * OWN + i * 16, 16), 16)
        mixed[t, :] = norm(ybuf[r, :], mgain_ref[...]).astype(BF16)
        return 0

    lax.fori_loop(0, OWN // 16, first_norm, 0)

    def rows_of(t, start=0, size=OWN):
        return mixed.at[pl.ds(pl.multiple_of(t * OWN + start, 16), size)]

    send("gu", lambda: (rows_of(tp), rows_of(tp), y_up, rows_of(m_d)))
    send("gd", lambda: (rows_of(tp), rows_of(tp), y_down, rows_of(m_u)))
    send("gs", lambda: (rows_of(tp), rows_of(tp), sibling, rows_of(y * 2 + 1 - c)))
    own_down.wait()
    for tag in ("0", "d"):
        take("wx2r_up" + tag, "wx2r_dn" + tag)
    for tag in ("u", "f"):
        take("wx2l_up" + tag, "wx2l_dn" + tag)

    def up_group(yy):
        rows = pl.ds(pl.multiple_of(yy * 192, 64), 192)
        into = pl.ds(pl.multiple_of(yy * 192 + 16, 16), 192)

        def some(i, _):
            col = pl.ds(pl.multiple_of(i * 256, 256), 256)
            part = jnp.dot(mixed[rows, :], upbuf[:, col], preferred_element_type=F32)
            both[into, col] = part.astype(BF16)
            return 0

        lax.fori_loop(0, 5, some, 0)
        part = jnp.dot(mixed[rows, :], upbuf[:, 1280:1408], preferred_element_type=F32)
        both[into, 1280:1408] = part.astype(BF16)

    def up_step(step, _):
        @pl.when(step == 0)
        def _():
            take("gs")

        @pl.when(step == 1)
        def _():
            take("gu", "gd")
            send("g2u", lambda: (rows_of(m_d, 0, 48), rows_of(m_d, 0, 48), y_up, rows_of(m_f, 0, 48)))
            send("g2d", lambda: (rows_of(m_u, 48, 48), rows_of(m_u, 48, 48), y_down, rows_of(m_f, 48, 48)))
            send("gs1", lambda: (rows_of(m_d), rows_of(m_d), sibling, rows_of(s_d)))
            send("gs2", lambda: (rows_of(m_u), rows_of(m_u), sibling, rows_of(s_u)))
            take("gs1")

        @pl.when(step == 2)
        def _():
            take("gs2", "g2u", "g2d")
            send("gs3", lambda: (rows_of(m_f), rows_of(m_f), sibling, rows_of(s_f)))

        @pl.when(step == 3)
        def _():
            take("gs3")

        offset = jnp.where(step == 1, 3, jnp.where(step == 2, 1, jnp.where(step == 3, 2, 0)))
        up_group((y + offset) % 4)
        return 0

    lax.fori_loop(0, 4, up_step, 0)
    send("halo", lambda: (both.at[pl.ds(BLK, 16)], halo, after, halo))

    def filtered(a, lanes_):
        taps = taps_ref[:, lanes_]
        n = a.shape[0] - 16
        return (
            taps[0:1] * a[14 : 14 + n]
            + taps[1:2] * a[15 : 15 + n]
            + taps[2:3] * a[16 : 16 + n]
        )

    def hidden_rows(i):
        src = pl.ds(pl.multiple_of(i * OWN, 32), OWN + 16)
        dst = pl.ds(pl.multiple_of(i * OWN, 32), OWN)
        for g in range(6):
            if g < 5:
                at_v, at_g = slice(g * 128, (g + 1) * 128), slice(640 + g * 128, 768 + g * 128)
                fv = filtered(both[src, at_v].astype(F32), at_v)
                fg = filtered(both[src, at_g].astype(F32), at_g)
            else:
                last = slice(1280, 1408)
                fv = filtered(both[src, last].astype(F32), last)
                fg = pltpu.roll(fv, 64, 1)
            value = fg / (1.0 + jnp.exp(-fg)) * fv
            if g == 5:
                value = jnp.where(lane < 64, value, 0.0)
            hid[dst, g * 128 : (g + 1) * 128] = value.astype(BF16)

    def hidden_step(i, _):
        @pl.when(i == 7)
        def _():
            take("halo")
            both[0:16, :] = jnp.where(sp == 0, 0.0, halo[...].astype(F32)).astype(BF16)

        hidden_rows((i + 1) % 8)
        return 0

    lax.fori_loop(0, 8, hidden_step, 0)

    def down_group(g, yy):
        mine = hid[pl.ds(pl.multiple_of(yy * 192 + c * OWN, 32), OWN), :]
        other = hid[pl.ds(pl.multiple_of(yy * 192 + (1 - c) * OWN, 32), OWN), :]
        lhs = jnp.concatenate([mine, other], axis=0)

        def some(i, _):
            col = pl.ds(pl.multiple_of(i * 256, 256), 256)
            part = jnp.dot(lhs, downbuf[:, col], preferred_element_type=F32)
            keep[g, :, col] = part[:OWN]
            sib_out[g, :, col] = part[OWN:].astype(BF16)
            return 0

        lax.fori_loop(0, 8, some, 0)

    def send_sib(g):
        send("r%d" % g, lambda: (sib_out.at[g], sib_in.at[g], sibling, sib_in.at[g]))

    def pair_sum(g, lo, hi):
        return keep[g, :, lo:hi] + sib_in[g, :, lo:hi].astype(F32)

    down_group(0, yf)
    send_sib(0)
    down_group(1, yd)
    send_sib(1)
    take("r0")
    far_out[0] = pair_sum(0, 0, HALF).astype(BF16)
    far_out[1] = pair_sum(0, HALF, 2 * HALF).astype(BF16)
    send("fu", lambda: (far_out.at[0], far_in.at[0], y_up, far_in.at[0]))
    send("fd", lambda: (far_out.at[1], far_in.at[1], y_down, far_in.at[1]))
    down_group(2, yu)
    send_sib(2)
    down_group(3, y)
    send_sib(3)
    take("r1", "r2")
    near_out[0, :, HALF:] = pair_sum(2, HALF, 2 * HALF).astype(BF16)
    near_out[1, :, :HALF] = pair_sum(1, 0, HALF).astype(BF16)
    take("fu")
    near_out[0, :, :HALF] = (pair_sum(2, 0, HALF) + far_in[0].astype(F32)).astype(BF16)
    send("nu", lambda: (near_out.at[0], near_in.at[0], y_up, near_in.at[0]))
    take("fd")
    near_out[1, :, HALF:] = (pair_sum(1, HALF, 2 * HALF) + far_in[1].astype(F32)).astype(BF16)
    send("nd", lambda: (near_out.at[1], near_in.at[1], y_down, near_in.at[1]))
    take("r3", "nu", "nd")

    def last_norm(i, _):
        r = pl.ds(pl.multiple_of(i * 16, 16), 16)
        t = pl.ds(pl.multiple_of(tp * OWN + i * 16, 16), 16)
        ffn = (
            keep[3, r, :]
            + sib_in[3, r, :].astype(F32)
            + near_in[0, r, :].astype(F32)
            + near_in[1, r, :].astype(F32)
        )
        whole = residual_scale * mixed[t, :].astype(F32) + ffn
        out_ref[r, :] = norm(whole, fgain_ref[...]).astype(BF16)
        return 0

    lax.fori_loop(0, OWN // 16, last_norm, 0)
    for copy in sent:
        copy(False).wait_send()


def whole_layer(*operands):
    vmem = pl.BlockSpec(memory_space=pltpu.VMEM)
    return pl.pallas_call(
        layer_kernel,
        out_shape=jax.ShapeDtypeStruct((OWN, 2048), BF16),
        in_specs=[vmem] * len(operands),
        out_specs=vmem,
        scratch_shapes=[
            pltpu.VMEM((2, BLK + EXTRA, 256), BF16),
            pltpu.VMEM((2, BLK, 256), BF16),
            pltpu.VMEM((16, BLK + EXTRA, 256), BF16),
            pltpu.VMEM((BLK, 256), BF16),
            pltpu.VMEM((2, 2, BLK, 128), BF16),
            pltpu.VMEM((2, 2, BLK, 128), F32),
            pltpu.VMEM((32, 8, BLK), F32),
            pltpu.VMEM((2, 2, BLK, 128), F32),
            pltpu.VMEM((2, 2, BLK, 128), F32),
            pltpu.VMEM((2, BLK, 128), F32),
            pltpu.VMEM((2, BLK, 128), BF16),
            pltpu.VMEM((2048, 1408), BF16),
            pltpu.VMEM((768, 2048), BF16),
            pltpu.VMEM((2048, 2048), BF16),
            pltpu.VMEM((16, OWN, 128), BF16),
            pltpu.VMEM((OWN, 2048), F32),
            pltpu.VMEM((BLK, 2048), BF16),
            pltpu.VMEM((BLK + 16, 1408), BF16),
            pltpu.VMEM((16, 1408), BF16),
            pltpu.VMEM((BLK, 768), BF16),
            pltpu.VMEM((4, OWN, 2048), F32),
            pltpu.VMEM((4, OWN, 2048), BF16),
            pltpu.VMEM((4, OWN, 2048), BF16),
            pltpu.VMEM((2, OWN, HALF), BF16),
            pltpu.VMEM((2, OWN, HALF), BF16),
            pltpu.VMEM((2, OWN, 2048), BF16),
            pltpu.VMEM((2, OWN, 2048), BF16),
            pltpu.SemaphoreType.DMA((112,)),
            pltpu.SemaphoreType.DMA((112,)),
            pltpu.SemaphoreType.DMA((2,)),
        ],
        compiler_params=pltpu.CompilerParams(
            collective_id=1, has_side_effects=True, vmem_limit_bytes=VMEM_ALL
        ),
        cost_estimate=pl.CostEstimate(flops=20_000_000_000, bytes_accessed=40_000_000, transcendentals=0),
    )(*operands)


def gate_lanes(gates):
    scaled = gates.T * LOG2E
    high = lax.reduce_precision(scaled, 8, 7)
    middle = lax.reduce_precision(scaled - high, 8, 7)
    low = lax.reduce_precision(scaled - high - middle, 8, 7)
    parts = jnp.stack([high, middle, low], axis=1).astype(BF16)
    rows = parts.reshape(gates.shape[1] * 9, 256)
    return jnp.pad(rows, ((0, EXTRA - rows.shape[0]), (0, 0)))


def per_device(
    query_small,
    key_small,
    value_small,
    gates_small,
    query_large,
    key_large,
    value_large,
    gates_large,
    residual,
    mixer_small,
    mixer_large,
    mix_gain,
    value_weight,
    gate_weight,
    value_taps,
    gate_taps,
    down_weight,
    final_gain,
):
    lanes = jnp.stack([gate_lanes(gates_small), gate_lanes(gates_large)])
    taps = jnp.concatenate(
        [value_taps[:, :640], gate_taps[:, :640], value_taps[:, 640:], gate_taps[:, 640:]], axis=1
    )
    return whole_layer(
        query_small,
        key_small,
        value_small,
        query_large,
        key_large,
        value_large,
        gates_small,
        gates_large,
        lanes,
        value_weight,
        gate_weight,
        down_weight,
        mixer_small,
        mixer_large,
        residual,
        mix_gain[None],
        final_gain[None],
        taps,
    )


def solution(mesh):
    split = Mesh(mesh.devices.reshape(mesh.shape["sp"], 4, 2), ("sp", "tp_0", "tp_1"))
    placed = (
        P("sp", TP),
        P("sp", TP),
        P("sp", TP),
        P("sp", TP),
        P("sp", TP),
        P("sp", TP),
        P("sp", TP),
        P("sp", TP),
        P(SP_TP, None),
        P(TP, None),
        P(TP, None),
        P(),
        P("sp", TP),
        P("sp", TP),
        P(None, TP),
        P(None, TP),
        P(TP, "sp"),
        P(),
    )
    return jax.shard_map(
        per_device, mesh=split, in_specs=placed, out_specs=P(SP_TP, None), check_vma=False
    )
```

```python
import functools

import jax
import jax.numpy as jnp
from jax import lax
from jax.experimental import pallas as pl
from jax.experimental.pallas import tpu as pltpu
from jax.sharding import Mesh
from jax.sharding import PartitionSpec as P

TP = ("tp_0", "tp_1")
SP_TP = ("sp", "tp_0", "tp_1")
LOG2E = 1.4426950408889634
residual_scale = 2.0**0.5
epsilon = 1e-05
MESH = pl.DeviceIdType.MESH
BLK = 768
EXTRA = 32
WROWS = 2112
WHALF = 1056
RQ = 384
F32 = jnp.float32
BF16 = jnp.bfloat16
VMEM_ALL = 67_000_000
OWN = 96
HALF = 1024


def layer_kernel(
    qs_ref,
    ks_ref,
    vs_ref,
    ql_ref,
    kl_ref,
    vl_ref,
    gs_ref,
    gl_ref,
    vw_ref,
    gw_ref,
    down_ref,
    ms_ref,
    ml_ref,
    res_ref,
    mgain_ref,
    fgain_ref,
    vtaps_ref,
    gtaps_ref,
    out_ref,
    kvin,
    qin,
    kvbuf,
    qpair,
    qgate,
    qm,
    gq,
    gk,
    mst,
    lst,
    acc,
    sbuf,
    pbuf,
    abuf,
    outv,
    wbuf,
    mixbuf,
    arrived,
    ybuf,
    mixed,
    both,
    halo,
    taps,
    hid,
    keep,
    sib_out,
    sib_in,
    far_out,
    far_in,
    near_out,
    near_in,
    ssem,
    rsem,
    lsem,
):
    sp = lax.axis_index("sp")
    y = lax.axis_index("tp_0")
    c = lax.axis_index("tp_1")
    z, x = sp // 4, sp % 4
    role = x // 2
    xr, xl = (x + 1) % 4, (x + 3) % 4
    zu, zd = (z + 1) % 4, (z + 3) % 4
    yu, yd = (y + 1) % 4, (y + 3) % 4
    xf, zf, yf = (x + 2) % 4, (z + 2) % 4, (y + 2) % 4
    mate = x + 1 - 2 * (x % 2)
    opp = 3 - x
    diag = opp + 1 - 2 * (opp % 2)
    pair_sp = 15 - sp
    tp = y * 2 + c

    def at(zz, xx):
        return (zz * 4 + xx, y, c)

    right, left = at(z, xr), at(z, xl)
    above, below = at(zu, x), at(zd, x)
    mate_dev, opp_dev = at(z, mate), at(z, opp)
    pair_dev = (pair_sp, y, c)
    y_up, y_down = (sp, yu, c), (sp, yd, c)
    sibling = (sp, y, 1 - c)
    after, before = ((sp + 1) % 16, y, c), ((sp + 15) % 16, y, c)

    barrier = pltpu.get_barrier_semaphore()
    greeted = [right, left, above, below, after, before]
    for d in range(8):
        t = (tp + d) % 8
        if d:
            greeted.append((sp, t // 2, t % 2))
        greeted.append((pair_sp, t // 2, t % 2))
    for dev in greeted:
        pl.semaphore_signal(barrier, inc=1, device_id=dev, device_id_type=MESH)

    lane = lax.broadcasted_iota(jnp.int32, (1, 128), 1)

    for r, (q_ref, k_ref, v_ref, g_ref) in enumerate(
        ((qs_ref, ks_ref, vs_ref, gs_ref), (ql_ref, kl_ref, vl_ref, gl_ref))
    ):
        kvin[r, 0:BLK, 0:128] = k_ref[...]
        kvin[r, 0:BLK, 128:256] = v_ref[...]
        qin[r] = q_ref[...]
        pieces = []
        for h in range(2 - r):
            left_over = g_ref[h : h + 1, :] * LOG2E
            for i in range(3):
                part = left_over.astype(BF16).astype(F32)
                left_over = left_over - part
                pieces += [part[:, p * 256 : (p + 1) * 256] for p in range(3)]
        pieces.append(jnp.zeros((EXTRA - len(pieces), 256), F32))
        kvin[r, BLK : BLK + EXTRA, :] = jnp.concatenate(pieces, axis=0).astype(BF16)

    def mix_rows(t, start=0, size=256):
        return mixbuf.at[pl.ds(pl.multiple_of(t * 256 + start, 128), size)]

    def weights(b, start=0, size=WROWS):
        return wbuf.at[b, pl.ds(start, size)]

    wbuf[sp, 0:640, :] = vw_ref[0:640, :]
    wbuf[sp, 640:1280, :] = gw_ref[0:640, :]
    wbuf[sp, 1280:1344, :] = vw_ref[640:704, :]
    wbuf[sp, 1344:1408, :] = gw_ref[640:704, :]
    wbuf[sp, 1408:WROWS, :] = down_ref[...]
    for b in range(16):
        wbuf[b, WROWS : WROWS + 64, :] = jnp.zeros((64, 128), BF16)
    mixbuf[pl.ds(pl.multiple_of(tp * 256, 256), 128), :] = ms_ref[...]
    mixbuf[pl.ds(pl.multiple_of(tp * 256 + 128, 128), 128), :] = ml_ref[...]

    pl.semaphore_wait(barrier, len(greeted))

    sent = []
    counter = [0]
    incoming = {}

    def send(name, ends):
        k = counter[0]
        counter[0] += 1

        def copy(arriving):
            src, dst, dev, landing = ends()
            return pltpu.make_async_remote_copy(
                src_ref=landing if arriving else src,
                dst_ref=landing if arriving else dst,
                send_sem=ssem.at[k],
                recv_sem=rsem.at[k],
                device_id=dev,
                device_id_type=MESH,
            )

        copy(False).start()
        sent.append(copy)
        incoming[name] = copy

    def take(*names):
        for name in names:
            incoming.pop(name)(True).wait_recv()

    cols = {"own": x, "mate": mate, "opp": opp, "diag": diag}

    send("x1m", lambda: (kvin.at[role], kvbuf.at[sp], mate_dev, kvbuf.at[z * 4 + mate]))
    send("x1o", lambda: (kvin.at[1 - role], kvbuf.at[sp], opp_dev, kvbuf.at[z * 4 + opp]))
    send("z1u_own", lambda: (kvin.at[role], kvbuf.at[sp], above, kvbuf.at[zd * 4 + x]))
    send("z1d_own", lambda: (kvin.at[role], kvbuf.at[sp], below, kvbuf.at[zu * 4 + x]))
    gate_part = pl.ds(BLK, EXTRA)
    send("qg", lambda: (kvin.at[1 - role, gate_part], qgate, pair_dev, qgate))
    send("q", lambda: (qin.at[1 - role], qpair, pair_dev, qpair))
    send("y1u", lambda: (mix_rows(tp), mix_rows(tp), y_up, mix_rows(yd * 2 + c)))
    send("y1d", lambda: (mix_rows(tp), mix_rows(tp), y_down, mix_rows(yu * 2 + c)))
    send("s0", lambda: (mix_rows(tp), mix_rows(tp), sibling, mix_rows(y * 2 + 1 - c)))

    def pass_x(tag, zz):
        def ends(dev, col):
            mine = weights(zz * 4 + x)
            return mine, mine, dev, weights(zz * 4 + col)

        send("wx1r" + tag, lambda: ends(right, xl))
        send("wx1l" + tag, lambda: ends(left, xr))

    own_kv = pltpu.make_async_copy(kvin.at[role], kvbuf.at[sp], lsem.at[0])
    own_kv.start()

    heads = 2 - role
    head_dim = 64 + 64 * role
    scale = jnp.where(role == 0, 0.125 * LOG2E, 128.0**-0.5 * LOG2E).astype(F32)

    def head_lanes(h):
        return (lane >= h * 64) & (lane < h * 64 + head_dim)

    def gate_row(rows, h, g):
        k, at_ = h * 9 + g // 2, slice((g % 2) * 128, (g % 2) * 128 + 128)
        return rows[k : k + 1, at_] + rows[k + 3 : k + 4, at_] + rows[k + 6 : k + 7, at_]

    same = lax.broadcasted_iota(jnp.int32, (128, 128), 0) == lax.broadcasted_iota(
        jnp.int32, (128, 128), 1
    )

    def load_queries(qi, queries, gate_block):
        rows = gate_block.astype(F32)
        for h in range(2):
            ones = jnp.where(head_lanes(h), 1.0, 0.0).astype(BF16)
            qm[qi, h] = queries * ones
            for g in range(BLK // 128):
                line = jnp.broadcast_to(gate_row(rows, h, g), (128, 128))
                column = jnp.sum(jnp.where(same, line, 0.0), axis=1, keepdims=True)
                gq[qi, h, g * 128 : (g + 1) * 128, :] = jnp.broadcast_to(column, (128, 128))

    load_queries(0, qin[role], kvin[role, BLK : BLK + EXTRA, :])
    mst[...] = jnp.full(mst.shape, -1e30, F32)
    lst[...] = jnp.zeros(lst.shape, F32)
    acc[...] = jnp.zeros(acc.shape, F32)

    def pass_z(tag):
        col = cols[tag]
        src = kvbuf.at[z * 4 + col]
        send("z1u_" + tag, lambda: (src, src, above, kvbuf.at[zd * 4 + col]))
        send("z1d_" + tag, lambda: (src, src, below, kvbuf.at[zu * 4 + col]))

    take("x1o")
    send("x2", lambda: (kvbuf.at[z * 4 + opp], kvbuf.at[z * 4 + opp], mate_dev, kvbuf.at[z * 4 + diag]))
    take("x1m")
    send("wz1u", lambda: (weights(sp), weights(sp), above, weights(zd * 4 + x)))
    send("wz1d", lambda: (weights(sp), weights(sp), below, weights(zu * 4 + x)))
    pass_x("0", z)
    take("q", "qg")
    load_queries(1, qpair[...], qgate[...])
    own_kv.wait()
    take("wz1u", "wz1d")
    b_d, b_u, b_f = zd * 4 + x, zu * 4 + x, zf * 4 + x
    send(
        "wz2u",
        lambda: (weights(b_d, 0, WHALF), weights(b_d, 0, WHALF), above, weights(b_f, 0, WHALF)),
    )
    send(
        "wz2d",
        lambda: (weights(b_u, WHALF, WHALF), weights(b_u, WHALF, WHALF), below, weights(b_f, WHALF, WHALF)),
    )
    pass_z("mate")
    pass_z("opp")
    pass_x("d", zd)
    pass_x("u", zu)
    take("x2")
    pass_z("diag")
    def gate_rows(j):
        rows = kvbuf[j, BLK : BLK + EXTRA, :].astype(F32)
        for h in range(2):
            for g in range(BLK // 128):
                line = jnp.broadcast_to(gate_row(rows, h, g), (8, 128))
                gk[j * 2 + h, :, g * 128 : (g + 1) * 128] = line

    def scores(qi, j, h, sub, masked):
        rows = pl.ds(sub * RQ, RQ)
        span = (sub + 1) * RQ if masked else BLK
        return lax.dot_general(
            qm[qi, h, rows, :],
            kvbuf[j, 0:span, 0:128],
            (((1,), (1,)), ((), ())),
            preferred_element_type=F32,
        )

    def soften(s, qi, j, h, sub, masked):
        rows = pl.ds(sub * RQ, RQ)
        span = (sub + 1) * RQ if masked else BLK
        gate = gk[j * 2 + h, 0:1, 0:span]
        parts = []
        for g in range(span // 128):
            part = s[:, g * 128 : (g + 1) * 128] * scale - gate[:, g * 128 : (g + 1) * 128]
            if masked and (g + 1) * 128 > sub * RQ:
                col = lax.broadcasted_iota(jnp.int32, (RQ, 128), 1) + (g * 128 - sub * RQ)
                row = lax.broadcasted_iota(jnp.int32, (RQ, 128), 0)
                part = jnp.where(col <= row, part, -1e30)
            parts.append(part)
        peak = functools.reduce(jnp.maximum, parts)
        peak = jnp.max(peak, axis=1, keepdims=True)
        g_here = gq[qi, h, rows, :]
        old = mst[qi, h, rows, :]
        new = jnp.maximum(old, peak + g_here)
        alpha = jnp.exp2(old - new)
        shift = new - g_here
        weights = [jnp.exp2(part - shift) for part in parts]
        mst[qi, h, rows, :] = new
        lst[qi, h, rows, :] = lst[qi, h, rows, :] * alpha + functools.reduce(jnp.add, weights)
        return jnp.concatenate([a.astype(BF16) for a in weights], axis=1), alpha

    def spread(w, alpha, qi, j, h, sub, masked):
        rows = pl.ds(sub * RQ, RQ)
        span = (sub + 1) * RQ if masked else BLK
        mask = head_lanes(h)
        v = kvbuf[j, 0:span, 128:256] * jnp.where(mask, 1.0, 0.0).astype(BF16)
        update = jnp.dot(w, v, preferred_element_type=F32)
        acc[qi, rows, :] = acc[qi, rows, :] * jnp.where(mask, alpha, 1.0) + update

    def tiles(qi, j, h, masked):
        count = BLK // RQ
        s = scores(qi, j, h, 0, masked)
        held = None
        for sub in range(count):
            ahead = scores(qi, j, h, sub + 1, masked) if sub + 1 < count else None
            w, alpha = soften(s, qi, j, h, sub, masked)
            spread(w, alpha, qi, j, h, sub, masked)
            s = ahead

    def attend_row(zz):
        for xx in range(4):
            gate_rows(zz * 4 + xx)

        full = [jnp.clip(b - 4 * zz, 0, 4) for b in (sp, pair_sp)]
        split = full[0] * heads
        units = split + full[1] * heads

        def place(u):
            u = jnp.minimum(u, units - 1)
            qi = jnp.where(u >= split, 1, 0)
            r = u - qi * split
            return qi, zz * 4 + r // heads, r % heads

        def finish(u, qi):
            _, j, h = place(u)
            spread(pbuf[...], abuf[...], qi, j, h, 1, False)

        def one_unit(u, _):
            qi, j, h = place(u)
            before_qi = jnp.where(u > 0, place(jnp.maximum(u - 1, 0))[0], 2)
            finish(jnp.maximum(u - 1, 0), before_qi)
            later = scores(qi, j, h, 1, False)
            w, alpha = soften(sbuf[...], qi, j, h, 0, False)
            spread(w, alpha, qi, j, h, 0, False)
            ahead = scores(*place(u + 1), 0, False)
            w, alpha = soften(later, qi, j, h, 1, False)
            sbuf[...] = ahead
            pbuf[...] = w
            abuf[...] = alpha
            return 0

        @pl.when(units > 0)
        def _():
            sbuf[...] = scores(*place(0), 0, False)
            lax.fori_loop(0, units, one_unit, 0)
            finish(units - 1, place(units - 1)[0])

        def for_queries(qi, _):
            qblk = jnp.where(qi == 0, sp, pair_sp)

            @pl.when(qblk // 4 == zz)
            def _():
                def for_head(h, _):
                    tiles(qi, qblk, h, True)
                    return 0

                lax.fori_loop(0, heads, for_head, 0)

            return 0

        lax.fori_loop(0, 2, for_queries, 0)

    def pass_on(tag, name, from_z, dev, landing_z):
        col = cols[tag]

        def ends():
            src = kvbuf.at[from_z * 4 + col]
            return src, src, dev, kvbuf.at[landing_z * 4 + col]

        send(name + tag, ends)

    m_d, m_u, m_f = yd * 2 + c, yu * 2 + c, yf * 2 + c
    s_d, s_u, s_f = yd * 2 + 1 - c, yu * 2 + 1 - c, yf * 2 + 1 - c

    def pass_x2(tag, zz, name, col, dev, start=0, size=WROWS):
        def ends():
            src = weights(zz * 4 + col, start, size)
            return src, src, dev, weights(zz * 4 + xf, start, size)

        send(name + tag, ends)

    def one_row(step, _):
        offset = jnp.where(step == 1, 3, jnp.where(step == 2, 1, jnp.where(step == 3, 2, 0)))
        attend_row((z + offset) % 4)

        @pl.when(step == 0)
        def _():
            take("y1u", "y1d")
            send("y2u", lambda: (mix_rows(m_d, 0, 128), mix_rows(m_d, 0, 128), y_up, mix_rows(m_f, 0, 128)))
            send("y2d", lambda: (mix_rows(m_u, 128, 128), mix_rows(m_u, 128, 128), y_down, mix_rows(m_f, 128, 128)))
            send("s1", lambda: (mix_rows(m_d), mix_rows(m_d), sibling, mix_rows(s_d)))
            send("s2", lambda: (mix_rows(m_u), mix_rows(m_u), sibling, mix_rows(s_u)))
            take("z1u_own", "z1d_own", "z1u_mate", "z1d_mate")
            pass_on("own", "z2u_", zd, above, zf)
            pass_on("mate", "z2u_", zd, above, zf)
            take("z1u_opp", "z1d_opp", "z1u_diag", "z1d_diag")
            pass_on("opp", "z2d_", zu, below, zf)
            pass_on("diag", "z2d_", zu, below, zf)
            take("wz2u", "wz2d")
            pass_x("f", zf)
            take("wx1r0", "wx1l0")
            pass_x2("0", z, "wx2r", xl, right)

        @pl.when(step == 1)
        def _():
            take("wx1rd", "wx1ld", "wx1ru", "wx1lu")
            pass_x2("d", zd, "wx2l", xr, left)
            pass_x2("u", zu, "wx2r", xl, right, 0, WHALF)
            pass_x2("u", zu, "wx2l", xr, left, WHALF, WHALF)

        @pl.when(step == 2)
        def _():
            take("y2u", "y2d")
            send("s3", lambda: (mix_rows(m_f), mix_rows(m_f), sibling, mix_rows(s_f)))
            take("wx1rf", "wx1lf")
            pass_x2("f", zf, "wx2r", xl, right, 0, WHALF)
            pass_x2("f", zf, "wx2l", xr, left, WHALF, WHALF)
            take("z2u_own", "z2u_mate", "z2d_opp", "z2d_diag")

        return 0

    lax.fori_loop(0, 4, one_row, 0)

    keep0 = head_lanes(0)
    for qi in (1, 0):
        l0 = jnp.sum(lst[qi, 0], axis=1, keepdims=True)
        l1 = jnp.sum(lst[qi, 1], axis=1, keepdims=True)
        outv[qi] = (acc[qi] / jnp.where(keep0, l0, l1)).astype(BF16)

    def own_rows(t):
        return pl.ds(pl.multiple_of(t * OWN, 32), OWN)

    slot = tp * 2 + role

    def send_out(d):
        t, s = (tp + d) % 8, (tp + 8 - d) % 8
        dst = (t // 2, t % 2)
        send(
            "p%d" % d,
            lambda: (outv.at[1, own_rows(t)], arrived.at[slot], (pair_sp, *dst), arrived.at[s * 2 + 1 - role]),
        )
        if d:
            send(
                "a%d" % d,
                lambda: (outv.at[0, own_rows(t)], arrived.at[slot], (sp, *dst), arrived.at[s * 2 + role]),
            )

    for d in range(8):
        send_out(d)
    arrived[slot] = outv[0, own_rows(tp), :]
    take("s0", "s1", "s2", "s3")
    for d in range(8):
        take("p%d" % d)
        if d:
            take("a%d" % d)

    def project(i, _):
        col = pl.ds(pl.multiple_of(i * 256, 256), 256)
        lhs = jnp.concatenate([arrived[s] for s in range(16)], axis=1)
        part = jnp.dot(lhs, mixbuf[:, col], preferred_element_type=F32)
        ybuf[:, col] = residual_scale * res_ref[:, col].astype(F32) + part
        return 0

    lax.fori_loop(0, 8, project, 0)

    def norm(values, gain):
        center = jnp.mean(values, axis=1, keepdims=True)
        off = values - center
        spread = jnp.mean(jnp.square(off), axis=1, keepdims=True)
        return off * lax.rsqrt(spread + epsilon) * gain

    def first_norm(i, _):
        r = pl.ds(pl.multiple_of(i * 16, 16), 16)
        t = pl.ds(pl.multiple_of(tp * OWN + i * 16, 16), 16)
        mixed[t, :] = norm(ybuf[r, :], mgain_ref[...]).astype(BF16)
        return 0

    lax.fori_loop(0, OWN // 16, first_norm, 0)

    def rows_of(t, start=0, size=OWN):
        return mixed.at[pl.ds(pl.multiple_of(t * OWN + start, 16), size)]

    send("gu", lambda: (rows_of(tp), rows_of(tp), y_up, rows_of(m_d)))
    send("gd", lambda: (rows_of(tp), rows_of(tp), y_down, rows_of(m_u)))
    send("gs", lambda: (rows_of(tp), rows_of(tp), sibling, rows_of(y * 2 + 1 - c)))
    take("wx2r0", "wx2ld", "wx2ru", "wx2lu", "wx2rf", "wx2lf")

    def up_group(*chips):
        def some(start, width):
            cols_ = pl.ds(start, width)
            rhs = jnp.concatenate([wbuf[b, cols_, :] for b in range(16)], axis=1)
            lhs = [mixed[pl.ds(pl.multiple_of(yy * 192, 64), 192), :] for yy in chips]
            part = lax.dot_general(
                jnp.concatenate(lhs, axis=0), rhs, (((1,), (1,)), ((), ())), preferred_element_type=F32
            ).astype(BF16)
            for k, yy in enumerate(chips):
                into = pl.ds(pl.multiple_of(yy * 192 + 16, 16), 192)
                both[into, cols_] = part[k * 192 : (k + 1) * 192]

        def chunk(i, _):
            some(pl.multiple_of(i * 256, 256), 256)
            return 0

        lax.fori_loop(0, 5, chunk, 0)
        some(1280, 128)

    take("gs")
    up_group(y)
    take("gu", "gd")
    send("g2u", lambda: (rows_of(m_d, 0, 48), rows_of(m_d, 0, 48), y_up, rows_of(m_f, 0, 48)))
    send("g2d", lambda: (rows_of(m_u, 48, 48), rows_of(m_u, 48, 48), y_down, rows_of(m_f, 48, 48)))
    send("gs1", lambda: (rows_of(m_d), rows_of(m_d), sibling, rows_of(s_d)))
    send("gs2", lambda: (rows_of(m_u), rows_of(m_u), sibling, rows_of(s_u)))
    take("gs1", "gs2")
    up_group(yd, yu)
    take("g2u", "g2d")
    send("gs3", lambda: (rows_of(m_f), rows_of(m_f), sibling, rows_of(s_f)))
    take("gs3")
    up_group(yf)
    send("halo", lambda: (both.at[pl.ds(BLK, 16)], halo, after, halo))

    taps[0:3, 0:640] = vtaps_ref[:, 0:640]
    taps[0:3, 640:1280] = gtaps_ref[:, 0:640]
    taps[0:3, 1280:1408] = jnp.concatenate([vtaps_ref[:, 640:704], gtaps_ref[:, 640:704]], axis=1)

    def filtered(a, lanes_):
        n = a.shape[0] - 16
        return (
            taps[0:1, lanes_] * a[14 : 14 + n]
            + taps[1:2, lanes_] * a[15 : 15 + n]
            + taps[2:3, lanes_] * a[16 : 16 + n]
        )

    def hidden_rows(i):
        src = pl.ds(pl.multiple_of(i * OWN, 32), OWN + 16)
        dst = pl.ds(pl.multiple_of(i * OWN, 32), OWN)
        for g in range(6):
            if g < 5:
                at_v, at_g = slice(g * 128, (g + 1) * 128), slice(640 + g * 128, 768 + g * 128)
                fv = filtered(both[src, at_v].astype(F32), at_v)
                fg = filtered(both[src, at_g].astype(F32), at_g)
            else:
                last = slice(1280, 1408)
                fv = filtered(both[src, last].astype(F32), last)
                fg = pltpu.roll(fv, 64, 1)
            value = fg / (1.0 + jnp.exp(-fg)) * fv
            if g == 5:
                value = jnp.where(lane < 64, value, 0.0)
            hid[dst, g * 128 : (g + 1) * 128] = value.astype(BF16)

    def hidden_step(i, _):
        @pl.when(i == 7)
        def _():
            take("halo")
            both[0:16, :] = jnp.where(sp == 0, 0.0, halo[...].astype(F32)).astype(BF16)

        hidden_rows((i + 1) % 8)
        return 0

    lax.fori_loop(0, 8, hidden_step, 0)

    def down_group(g, yy):
        mine = hid[pl.ds(pl.multiple_of(yy * 192 + c * OWN, 32), OWN), :]
        other = hid[pl.ds(pl.multiple_of(yy * 192 + (1 - c) * OWN, 32), OWN), :]
        lhs = jnp.concatenate([mine, other], axis=0)

        def some(i, _):
            col = pl.ds(pl.multiple_of(i * 256, 256), 256)
            rhs = jnp.concatenate(
                [wbuf[2 * i, 1408 : WROWS + 64, :], wbuf[2 * i + 1, 1408 : WROWS + 64, :]], axis=1
            )
            part = jnp.dot(lhs, rhs, preferred_element_type=F32)
            keep[g, :, col] = part[:OWN]
            sib_out[g, :, col] = part[OWN:].astype(BF16)
            return 0

        lax.fori_loop(0, 8, some, 0)

    def send_sib(g):
        send("r%d" % g, lambda: (sib_out.at[g], sib_in.at[g], sibling, sib_in.at[g]))

    def pair_sum(g, lo, hi):
        return keep[g, :, lo:hi] + sib_in[g, :, lo:hi].astype(F32)

    down_group(0, yf)
    send_sib(0)
    down_group(1, yd)
    send_sib(1)
    take("r0")
    far_out[0] = pair_sum(0, 0, HALF).astype(BF16)
    far_out[1] = pair_sum(0, HALF, 2 * HALF).astype(BF16)
    send("fu", lambda: (far_out.at[0], far_in.at[0], y_up, far_in.at[0]))
    send("fd", lambda: (far_out.at[1], far_in.at[1], y_down, far_in.at[1]))
    down_group(2, yu)
    send_sib(2)
    down_group(3, y)
    send_sib(3)
    take("r1", "r2")
    near_out[0, :, HALF:] = pair_sum(2, HALF, 2 * HALF).astype(BF16)
    near_out[1, :, :HALF] = pair_sum(1, 0, HALF).astype(BF16)
    take("fu")
    near_out[0, :, :HALF] = (pair_sum(2, 0, HALF) + far_in[0].astype(F32)).astype(BF16)
    send("nu", lambda: (near_out.at[0], near_in.at[0], y_up, near_in.at[0]))
    take("fd")
    near_out[1, :, HALF:] = (pair_sum(1, HALF, 2 * HALF) + far_in[1].astype(F32)).astype(BF16)
    send("nd", lambda: (near_out.at[1], near_in.at[1], y_down, near_in.at[1]))
    take("r3", "nu", "nd")

    def last_norm(i, _):
        r = pl.ds(pl.multiple_of(i * 16, 16), 16)
        t = pl.ds(pl.multiple_of(tp * OWN + i * 16, 16), 16)
        ffn = (
            keep[3, r, :]
            + sib_in[3, r, :].astype(F32)
            + near_in[0, r, :].astype(F32)
            + near_in[1, r, :].astype(F32)
        )
        whole = residual_scale * mixed[t, :].astype(F32) + ffn
        out_ref[r, :] = norm(whole, fgain_ref[...]).astype(BF16)
        return 0

    lax.fori_loop(0, OWN // 16, last_norm, 0)
    for copy in sent:
        copy(False).wait_send()


def whole_layer(*operands):
    vmem = pl.BlockSpec(memory_space=pltpu.VMEM)
    return pl.pallas_call(
        layer_kernel,
        out_shape=jax.ShapeDtypeStruct((OWN, 2048), BF16),
        in_specs=[vmem] * len(operands),
        out_specs=vmem,
        scratch_shapes=[
            pltpu.VMEM((2, BLK + EXTRA, 256), BF16),
            pltpu.VMEM((2, BLK, 128), BF16),
            pltpu.VMEM((16, BLK + EXTRA, 256), BF16),
            pltpu.VMEM((BLK, 128), BF16),
            pltpu.VMEM((EXTRA, 256), BF16),
            pltpu.VMEM((2, 2, BLK, 128), BF16),
            pltpu.VMEM((2, 2, BLK, 128), F32),
            pltpu.VMEM((32, 8, BLK), F32),
            pltpu.VMEM((2, 2, BLK, 128), F32),
            pltpu.VMEM((2, 2, BLK, 128), F32),
            pltpu.VMEM((3, BLK, 128), F32),
            pltpu.VMEM((RQ, BLK), F32),
            pltpu.VMEM((RQ, BLK), BF16),
            pltpu.VMEM((RQ, 128), F32),
            pltpu.VMEM((2, BLK, 128), BF16),
            pltpu.VMEM((16, WROWS + 64, 128), BF16),
            pltpu.VMEM((2048, 2048), BF16),
            pltpu.VMEM((16, OWN, 128), BF16),
            pltpu.VMEM((OWN, 2048), F32),
            pltpu.VMEM((BLK, 2048), BF16),
            pltpu.VMEM((BLK + 16, 1408), BF16),
            pltpu.VMEM((16, 1408), BF16),
            pltpu.VMEM((8, 1408), F32),
            pltpu.VMEM((BLK, 768), BF16),
            pltpu.VMEM((4, OWN, 2048), F32),
            pltpu.VMEM((4, OWN, 2048), BF16),
            pltpu.VMEM((4, OWN, 2048), BF16),
            pltpu.VMEM((2, OWN, HALF), BF16),
            pltpu.VMEM((2, OWN, HALF), BF16),
            pltpu.VMEM((2, OWN, 2048), BF16),
            pltpu.VMEM((2, OWN, 2048), BF16),
            pltpu.SemaphoreType.DMA((112,)),
            pltpu.SemaphoreType.DMA((112,)),
            pltpu.SemaphoreType.DMA((2,)),
        ],
        compiler_params=pltpu.CompilerParams(
            collective_id=1, has_side_effects=True, vmem_limit_bytes=VMEM_ALL
        ),
        cost_estimate=pl.CostEstimate(flops=20_000_000_000, bytes_accessed=40_000_000, transcendentals=0),
    )(*operands)


def per_device(
    query_small,
    key_small,
    value_small,
    gates_small,
    query_large,
    key_large,
    value_large,
    gates_large,
    residual,
    mixer_small,
    mixer_large,
    mix_gain,
    value_weight,
    gate_weight,
    value_taps,
    gate_taps,
    down_weight,
    final_gain,
):
    return whole_layer(
        query_small,
        key_small,
        value_small,
        query_large,
        key_large,
        value_large,
        gates_small.T,
        gates_large.T,
        value_weight.T,
        gate_weight.T,
        down_weight,
        mixer_small,
        mixer_large,
        residual,
        mix_gain[None],
        final_gain[None],
        value_taps,
        gate_taps,
    )


def solution(mesh):
    split = Mesh(mesh.devices.reshape(mesh.shape["sp"], 4, 2), ("sp", "tp_0", "tp_1"))
    placed = (
        P("sp", TP),
        P("sp", TP),
        P("sp", TP),
        P("sp", TP),
        P("sp", TP),
        P("sp", TP),
        P("sp", TP),
        P("sp", TP),
        P(SP_TP, None),
        P(TP, None),
        P(TP, None),
        P(),
        P("sp", TP),
        P("sp", TP),
        P(None, TP),
        P(None, TP),
        P(TP, "sp"),
        P(),
    )
    return jax.shard_map(
        per_device, mesh=split, in_specs=placed, out_specs=P(SP_TP, None), check_vma=False
    )
```

```python
import functools

import jax
import jax.numpy as jnp
from jax import lax
from jax.experimental import pallas as pl
from jax.experimental.pallas import tpu as pltpu
from jax.sharding import Mesh
from jax.sharding import PartitionSpec as P

TP = ("tp_0", "tp_1")
SP_TP = ("sp", "tp_0", "tp_1")
LOG2E = 1.4426950408889634
residual_scale = 2.0**0.5
epsilon = 1e-05
MESH = pl.DeviceIdType.MESH
BLK = 768
EXTRA = 32
WROWS = 2112
UP = 1408
DOWN = 704
RQ = 384
F32 = jnp.float32
BF16 = jnp.bfloat16
VMEM_ALL = 67_000_000
OWN = 96
HALF = 1024
HALO_SEM = 111


def layer_kernel(
    qs_ref,
    ks_ref,
    vs_ref,
    ql_ref,
    kl_ref,
    vl_ref,
    gs_ref,
    gl_ref,
    vw_ref,
    gw_ref,
    down_ref,
    ms_ref,
    ml_ref,
    res_ref,
    mgain_ref,
    fgain_ref,
    vtaps_ref,
    gtaps_ref,
    out_ref,
    kvin,
    qin,
    kvbuf,
    qpair,
    qgate,
    qm,
    gq,
    gk,
    mst,
    lst,
    acc,
    sbuf,
    mbuf,
    pbuf,
    abuf,
    outv,
    wbuf,
    mixbuf,
    arrived,
    ybuf,
    mixed,
    both,
    halo,
    taps,
    hid,
    keep,
    sib_out,
    sib_in,
    far_out,
    far_in,
    near_out,
    near_in,
    ssem,
    rsem,
    lsem,
):
    sp = lax.axis_index("sp")
    y = lax.axis_index("tp_0")
    c = lax.axis_index("tp_1")
    z, x = sp // 4, sp % 4
    role = x // 2
    xr, xl = (x + 1) % 4, (x + 3) % 4
    zu, zd = (z + 1) % 4, (z + 3) % 4
    yu, yd = (y + 1) % 4, (y + 3) % 4
    xf, zf, yf = (x + 2) % 4, (z + 2) % 4, (y + 2) % 4
    mate = x + 1 - 2 * (x % 2)
    opp = 3 - x
    diag = opp + 1 - 2 * (opp % 2)
    pair_sp = 15 - sp
    tp = y * 2 + c

    def at(zz, xx):
        return (zz * 4 + xx, y, c)

    right, left = at(z, xr), at(z, xl)
    above, below = at(zu, x), at(zd, x)
    mate_dev, opp_dev = at(z, mate), at(z, opp)
    pair_dev = (pair_sp, y, c)
    y_up, y_down = (sp, yu, c), (sp, yd, c)
    sibling = (sp, y, 1 - c)
    after, before = ((sp + 1) % 16, y, c), ((sp + 15) % 16, y, c)

    barrier = pltpu.get_barrier_semaphore()
    greeted = [right, left, above, below, after, before]
    for d in range(8):
        t = (tp + d) % 8
        if d:
            greeted.append((sp, t // 2, t % 2))
        greeted.append((pair_sp, t // 2, t % 2))
    for dev in greeted:
        pl.semaphore_signal(barrier, inc=1, device_id=dev, device_id_type=MESH)

    lane = lax.broadcasted_iota(jnp.int32, (1, 128), 1)

    for r, (q_ref, k_ref, v_ref, g_ref) in enumerate(
        ((qs_ref, ks_ref, vs_ref, gs_ref), (ql_ref, kl_ref, vl_ref, gl_ref))
    ):
        kvin[r, 0:BLK, 0:128] = k_ref[...]
        kvin[r, 0:BLK, 128:256] = v_ref[...]
        qin[r] = q_ref[...]
        pieces = []
        for h in range(2 - r):
            left_over = g_ref[h : h + 1, :] * LOG2E
            for i in range(3):
                part = left_over.astype(BF16).astype(F32)
                left_over = left_over - part
                pieces += [part[:, p * 256 : (p + 1) * 256] for p in range(3)]
        pieces.append(jnp.zeros((EXTRA - len(pieces), 256), F32))
        kvin[r, BLK : BLK + EXTRA, :] = jnp.concatenate(pieces, axis=0).astype(BF16)

    def mix_rows(t, start=0, size=256):
        return mixbuf.at[pl.ds(pl.multiple_of(t * 256 + start, 128), size)]

    def up_block(b, start=0, size=UP):
        return wbuf.at[b, pl.ds(start, size)]

    def down_blocks(b, count=1, start=0, size=DOWN):
        return wbuf.at[pl.ds(b, count), pl.ds(UP + start, size)]

    wbuf[sp, 0:640, :] = vw_ref[0:640, :]
    wbuf[sp, 640:1280, :] = gw_ref[0:640, :]
    wbuf[sp, 1280:1344, :] = vw_ref[640:704, :]
    wbuf[sp, 1344:1408, :] = gw_ref[640:704, :]
    wbuf[sp, 1408:WROWS, :] = down_ref[...]
    for b in range(16):
        wbuf[b, WROWS : WROWS + 64, :] = jnp.zeros((64, 128), BF16)
    mixbuf[pl.ds(pl.multiple_of(tp * 256, 256), 128), :] = ms_ref[...]
    mixbuf[pl.ds(pl.multiple_of(tp * 256 + 128, 128), 128), :] = ml_ref[...]

    pl.semaphore_wait(barrier, len(greeted))

    sent = []
    counter = [0]
    incoming = {}

    def send(name, ends, sends=None, receives=None):
        k = counter[0]
        counter[0] += 1

        def copy(arriving):
            src, dst, dev, landing = ends()
            return pltpu.make_async_remote_copy(
                src_ref=landing if arriving else src,
                dst_ref=landing if arriving else dst,
                send_sem=ssem.at[k],
                recv_sem=rsem.at[k],
                device_id=dev,
                device_id_type=MESH,
            )

        def only(condition, act):
            act() if condition is None else pl.when(condition())(act)

        sent.append(lambda: only(sends, lambda: copy(False).wait_send()))
        incoming[name] = lambda: only(receives, lambda: copy(True).wait_recv())
        only(sends, lambda: copy(False).start())
        return lambda: copy(False).start()

    def take(*names):
        for name in names:
            incoming.pop(name)()

    cols = {"own": x, "mate": mate, "opp": opp, "diag": diag}

    send("x1m", lambda: (kvin.at[role], kvbuf.at[sp], mate_dev, kvbuf.at[z * 4 + mate]))
    send("x1o", lambda: (kvin.at[1 - role], kvbuf.at[sp], opp_dev, kvbuf.at[z * 4 + opp]))
    send("z1u_own", lambda: (kvin.at[role], kvbuf.at[sp], above, kvbuf.at[zd * 4 + x]))
    send("z1d_own", lambda: (kvin.at[role], kvbuf.at[sp], below, kvbuf.at[zu * 4 + x]), lambda: z < 3, lambda: z != 2)
    gate_part = pl.ds(BLK, EXTRA)
    send("qg", lambda: (kvin.at[1 - role, gate_part], qgate, pair_dev, qgate))
    send("q", lambda: (qin.at[1 - role], qpair, pair_dev, qpair))
    send("y1u", lambda: (mix_rows(tp), mix_rows(tp), y_up, mix_rows(yd * 2 + c)))
    send("y1d", lambda: (mix_rows(tp), mix_rows(tp), y_down, mix_rows(yu * 2 + c)))
    send("s0", lambda: (mix_rows(tp), mix_rows(tp), sibling, mix_rows(y * 2 + 1 - c)))

    def pass_x(tag, zz):
        def ends(dev, col):
            mine = up_block(zz * 4 + x)
            return mine, mine, dev, up_block(zz * 4 + col)

        send("wx1r" + tag, lambda: ends(right, xl))
        send("wx1l" + tag, lambda: ends(left, xr))

    own_kv = pltpu.make_async_copy(kvin.at[role], kvbuf.at[sp], lsem.at[0])
    own_kv.start()

    heads = 2 - role
    head_dim = 64 + 64 * role
    scale = jnp.where(role == 0, 0.125 * LOG2E, 128.0**-0.5 * LOG2E).astype(F32)

    def head_lanes(h):
        return (lane >= h * 64) & (lane < h * 64 + head_dim)

    def gate_row(rows, h, g):
        k, at_ = h * 9 + g // 2, slice((g % 2) * 128, (g % 2) * 128 + 128)
        return rows[k : k + 1, at_] + rows[k + 3 : k + 4, at_] + rows[k + 6 : k + 7, at_]

    same = lax.broadcasted_iota(jnp.int32, (128, 128), 0) == lax.broadcasted_iota(
        jnp.int32, (128, 128), 1
    )

    def load_queries(qi, queries, gate_block):
        rows = gate_block.astype(F32)
        for h in range(2):
            ones = jnp.where(head_lanes(h), 1.0, 0.0).astype(BF16)
            qm[qi, h] = queries * ones
            for g in range(BLK // 128):
                line = jnp.broadcast_to(gate_row(rows, h, g), (128, 128))
                column = jnp.sum(jnp.where(same, line, 0.0), axis=1, keepdims=True)
                gq[qi, h, g * 128 : (g + 1) * 128, :] = jnp.broadcast_to(column, (128, 128))

    load_queries(0, qin[role], kvin[role, BLK : BLK + EXTRA, :])
    mst[...] = jnp.full(mst.shape, -1e30, F32)
    lst[...] = jnp.zeros(lst.shape, F32)
    acc[...] = jnp.zeros(acc.shape, F32)

    def pass_z(tag):
        col = cols[tag]
        src = kvbuf.at[z * 4 + col]
        send("z1u_" + tag, lambda: (src, src, above, kvbuf.at[zd * 4 + col]))
        send("z1d_" + tag, lambda: (src, src, below, kvbuf.at[zu * 4 + col]), lambda: z < 3, lambda: z != 2)

    b_d, b_u, b_f = zd * 4 + x, zu * 4 + x, zf * 4 + x
    b_l, b_r, b_o = z * 4 + xl, z * 4 + xr, z * 4 + (x + 2) % 4
    dhalf = DOWN // 2
    take("x1o")
    send("x2", lambda: (kvbuf.at[z * 4 + opp], kvbuf.at[z * 4 + opp], mate_dev, kvbuf.at[z * 4 + diag]))
    pass_z("opp")
    take("x1m")
    pass_z("mate")
    send("wz1u", lambda: (up_block(sp), up_block(sp), above, up_block(b_d)))
    send("wz1d", lambda: (up_block(sp), up_block(sp), below, up_block(b_u)))
    send("bx1r", lambda: (down_blocks(sp), down_blocks(sp), right, down_blocks(b_l)))
    send("bx1l", lambda: (down_blocks(sp), down_blocks(sp), left, down_blocks(b_r)))
    pass_x("0", z)
    own_kv.wait()
    take("x2")
    pass_z("diag")
    take("z1u_own", "z1d_own")
    send(
        "z2u_own",
        lambda: (kvbuf.at[zd * 4 + x], kvbuf.at[zd * 4 + x], above, kvbuf.at[zf * 4 + x]),
        lambda: z >= 2,
        lambda: (z == 0) | (z == 3),
    )
    send(
        "z2x_own",
        lambda: (kvbuf.at[zu * 4 + x], kvbuf.at[zu * 4 + x], below, kvbuf.at[zf * 4 + x]),
        lambda: z == 3,
        lambda: z == 2,
    )
    take("bx1r", "bx1l")
    send(
        "bx2r",
        lambda: (down_blocks(b_l, 1, 0, dhalf), down_blocks(b_l, 1, 0, dhalf), right, down_blocks(b_o, 1, 0, dhalf)),
    )
    send(
        "bx2l",
        lambda: (down_blocks(b_r, 1, dhalf, dhalf), down_blocks(b_r, 1, dhalf, dhalf), left, down_blocks(b_o, 1, dhalf, dhalf)),
    )
    take("q", "qg")
    load_queries(1, qpair[...], qgate[...])

    def gate_rows(j):
        rows = kvbuf[j, BLK : BLK + EXTRA, :].astype(F32)
        for h in range(2):
            for g in range(BLK // 128):
                line = jnp.broadcast_to(gate_row(rows, h, g), (8, 128))
                gk[j * 2 + h, :, g * 128 : (g + 1) * 128] = line

    def scores(qi, j, h, sub, masked):
        rows = pl.ds(sub * RQ, RQ)
        span = (sub + 1) * RQ if masked else BLK
        raw = lax.dot_general(
            qm[qi, h, rows, :],
            kvbuf[j, 0:span, 0:128],
            (((1,), (1,)), ((), ())),
            preferred_element_type=F32,
        )
        gate = gk[j * 2 + h, 0:1, 0:span]
        parts = []
        for g in range(span // 128):
            part = raw[:, g * 128 : (g + 1) * 128] * scale - gate[:, g * 128 : (g + 1) * 128]
            if masked and (g + 1) * 128 > sub * RQ:
                col = lax.broadcasted_iota(jnp.int32, (RQ, 128), 1) + (g * 128 - sub * RQ)
                row = lax.broadcasted_iota(jnp.int32, (RQ, 128), 0)
                part = jnp.where(col <= row, part, -1e30)
            parts.append(part)
        return parts, functools.reduce(jnp.maximum, parts)

    def soften(parts, peak, qi, j, h, sub):
        rows = pl.ds(sub * RQ, RQ)
        peak = jnp.max(peak, axis=1, keepdims=True)
        g_here = gq[qi, h, rows, :]
        old = mst[qi, h, rows, :]
        new = jnp.maximum(old, peak + g_here)
        alpha = jnp.exp2(old - new)
        shift = new - g_here
        weights_ = [jnp.exp2(part - shift) for part in parts]
        mst[qi, h, rows, :] = new
        lst[qi, h, rows, :] = lst[qi, h, rows, :] * alpha + functools.reduce(jnp.add, weights_)
        return jnp.concatenate([a.astype(BF16) for a in weights_], axis=1), alpha

    def hold(parts, peak):
        for g, part in enumerate(parts):
            sbuf[:, g * 128 : (g + 1) * 128] = part
        mbuf[...] = peak

    def held():
        return [sbuf[:, g * 128 : (g + 1) * 128] for g in range(BLK // 128)], mbuf[...]

    def spread(w, alpha, qi, j, h, sub, masked):
        rows = pl.ds(sub * RQ, RQ)
        span = (sub + 1) * RQ if masked else BLK
        mask = head_lanes(h)
        v = kvbuf[j, 0:span, 128:256] * jnp.where(mask, 1.0, 0.0).astype(BF16)
        update = jnp.dot(w, v, preferred_element_type=F32)
        acc[qi, rows, :] = acc[qi, rows, :] * jnp.where(mask, alpha, 1.0) + update

    def tiles(qi, j, h, masked):
        count = BLK // RQ
        ahead = scores(qi, j, h, 0, masked)
        for sub in range(count):
            here = ahead
            ahead = scores(qi, j, h, sub + 1, masked) if sub + 1 < count else None
            w, alpha = soften(*here, qi, j, h, sub)
            spread(w, alpha, qi, j, h, sub, masked)

    blocks_of = (sp, pair_sp)

    def attend(step):
        row = jnp.where(step == 0, z, jnp.where(step == 2, zd, jnp.where(step == 3, zu, zf)))
        second = step == 1
        none = 99
        slots = (
            jnp.where(second, zd * 4 + x, row * 4 + mate),
            jnp.where(second, zu * 4 + x, row * 4 + opp),
            jnp.where(second, none, row * 4 + diag),
            jnp.where(step == 0, sp, jnp.where(step == 3, zf * 4 + x, none)),
        )
        for j in slots:
            pl.when(j <= jnp.maximum(sp, pair_sp))(functools.partial(gate_rows, j))

        found, count = [], 0
        for qi in range(2):
            for j in slots:
                flag = jnp.where(j < blocks_of[qi], 1, 0)
                found.append((qi, j, flag, count))
                count = count + flag
        units = count * heads

        def place(u):
            v = jnp.clip(u, 0, units - 1)
            k = v // heads
            hits = [(qi, j, jnp.where(before_ == k, flag, 0)) for qi, j, flag, before_ in found]
            qi = sum(hit * qi for qi, _, hit in hits)
            j = sum(hit * j for _, j, hit in hits)
            return jnp.where(u == v, qi, 2), j, v % heads

        def two_units(i, _):
            spread(pbuf[...], abuf[...], *place(2 * i - 1), 1, False)
            here = held()
            for t in range(4):
                now = place(2 * i + t // 2)
                ahead = scores(*place(2 * i + (t + 1) // 2), (t + 1) % 2, False)
                w, alpha = soften(*here, *now, t % 2)
                if t < 3:
                    spread(w, alpha, *now, t % 2, False)
                here = ahead
            hold(*here)
            pbuf[...] = w
            abuf[...] = alpha
            return 0

        @pl.when(units > 0)
        def _():
            hold(*scores(*place(0), 0, False))
            steps = (units + 1) // 2
            lax.fori_loop(0, steps, two_units, 0)
            spread(pbuf[...], abuf[...], *place(2 * steps - 1), 1, False)

        @pl.when((step == 0) | (step == 2 + z % 2))
        def _():
            qi = jnp.where(step == 0, 0, 1)

            def for_head(h, _):
                tiles(qi, jnp.where(step == 0, sp, pair_sp), h, True)
                return 0

            lax.fori_loop(0, heads, for_head, 0)

    def pass_on(tag, name, from_z, dev, landing_z, sends, receives):
        col = cols[tag]

        def ends():
            src = kvbuf.at[from_z * 4 + col]
            return src, src, dev, kvbuf.at[landing_z * 4 + col]

        send(name + tag, ends, sends, receives)

    m_d, m_u, m_f = yd * 2 + c, yu * 2 + c, yf * 2 + c
    s_d, s_u, s_f = yd * 2 + 1 - c, yu * 2 + 1 - c, yf * 2 + 1 - c

    def pass_x2(tag, zz, name, col, dev, start=0, size=UP):
        def ends():
            src = up_block(zz * 4 + col, start, size)
            return src, src, dev, up_block(zz * 4 + xf, start, size)

        send(name + tag, ends)

    uhalf = UP // 2

    def one_step(step, _):
        attend(step)

        @pl.when(step == 1)
        def _():
            take("wz1u", "wz1d")
            pass_x("d", zd)
            pass_x("u", zu)
            take("y1u", "y1d")
            send("y2u", lambda: (mix_rows(m_d, 0, 128), mix_rows(m_d, 0, 128), y_up, mix_rows(m_f, 0, 128)))
            send("y2d", lambda: (mix_rows(m_u, 128, 128), mix_rows(m_u, 128, 128), y_down, mix_rows(m_f, 128, 128)))
            send("s1", lambda: (mix_rows(m_d), mix_rows(m_d), sibling, mix_rows(s_d)))
            send("s2", lambda: (mix_rows(m_u), mix_rows(m_u), sibling, mix_rows(s_u)))
            take("z1u_mate", "z1d_mate")
            pass_on("mate", "z2u_", zd, above, zf, lambda: z >= 1, lambda: z != 1)
            take("z1u_opp", "z1d_opp", "z1u_diag", "z1d_diag")
            pass_on("opp", "z2d_", zu, below, zf, lambda: z != 2, lambda: z != 1)
            pass_on("diag", "z2d_", zu, below, zf, lambda: z != 2, lambda: z != 1)
            send("wz2u", lambda: (up_block(b_d, 0, uhalf), up_block(b_d, 0, uhalf), above, up_block(b_f, 0, uhalf)))
            send("wz2d", lambda: (up_block(b_u, uhalf, uhalf), up_block(b_u, uhalf, uhalf), below, up_block(b_f, uhalf, uhalf)))
            take("wx1r0", "wx1l0")
            pass_x2("0", z, "wx2r", xl, right)

        @pl.when(step == 2)
        def _():
            take("z2u_own", "z2x_own")
            take("wx1rd", "wx1ld", "wx1ru", "wx1lu")
            pass_x2("d", zd, "wx2l", xr, left)
            pass_x2("u", zu, "wx2r", xl, right, 0, uhalf)
            pass_x2("u", zu, "wx2l", xr, left, uhalf, uhalf)

        @pl.when(step == 3)
        def _():
            take("y2u", "y2d")
            send("s3", lambda: (mix_rows(m_f), mix_rows(m_f), sibling, mix_rows(s_f)))
            take("wz2u", "wz2d")
            pass_x("f", zf)
            take("z2u_mate", "z2d_opp", "z2d_diag")
            take("bx2r", "bx2l")
            send("bz1u", lambda: (down_blocks(z * 4, 4), down_blocks(z * 4, 4), above, down_blocks(zd * 4, 4)))
            send("bz1d", lambda: (down_blocks(z * 4, 4), down_blocks(z * 4, 4), below, down_blocks(zu * 4, 4)))

        return 0

    lax.fori_loop(0, 5, one_step, 0)

    keep0 = head_lanes(0)
    for qi in (1, 0):
        l0 = jnp.sum(lst[qi, 0], axis=1, keepdims=True)
        l1 = jnp.sum(lst[qi, 1], axis=1, keepdims=True)
        outv[qi] = (acc[qi] / jnp.where(keep0, l0, l1)).astype(BF16)

    def own_rows(t):
        return pl.ds(pl.multiple_of(t * OWN, 32), OWN)

    slot = tp * 2 + role

    def send_out(d):
        t, s = (tp + d) % 8, (tp + 8 - d) % 8
        dst = (t // 2, t % 2)
        send(
            "p%d" % d,
            lambda: (outv.at[1, own_rows(t)], arrived.at[slot], (pair_sp, *dst), arrived.at[s * 2 + 1 - role]),
        )
        if d:
            send(
                "a%d" % d,
                lambda: (outv.at[0, own_rows(t)], arrived.at[slot], (sp, *dst), arrived.at[s * 2 + role]),
            )

    for d in range(8):
        send_out(d)
    take("wx1rf", "wx1lf")
    pass_x2("f", zf, "wx2r", xl, right, 0, uhalf)
    pass_x2("f", zf, "wx2l", xr, left, uhalf, uhalf)
    arrived[slot] = outv[0, own_rows(tp), :]
    take("s0", "s1", "s2", "s3")
    for d in range(8):
        take("p%d" % d)
        if d:
            take("a%d" % d)

    def project(i, _):
        col = pl.ds(pl.multiple_of(i * 256, 256), 256)
        lhs = jnp.concatenate([arrived[s] for s in range(16)], axis=1)
        part = jnp.dot(lhs, mixbuf[:, col], preferred_element_type=F32)
        ybuf[:, col] = residual_scale * res_ref[:, col].astype(F32) + part
        return 0

    lax.fori_loop(0, 8, project, 0)

    def norm(values, gain):
        center = jnp.mean(values, axis=1, keepdims=True)
        off = values - center
        spread = jnp.mean(jnp.square(off), axis=1, keepdims=True)
        return off * lax.rsqrt(spread + epsilon) * gain

    def first_norm(i, _):
        r = pl.ds(pl.multiple_of(i * 16, 16), 16)
        t = pl.ds(pl.multiple_of(tp * OWN + i * 16, 16), 16)
        mixed[t, :] = norm(ybuf[r, :], mgain_ref[...]).astype(BF16)
        return 0

    lax.fori_loop(0, OWN // 16, first_norm, 0)

    def rows_of(t, start=0, size=OWN):
        return mixed.at[pl.ds(pl.multiple_of(t * OWN + start, 16), size)]

    send("gu", lambda: (rows_of(tp), rows_of(tp), y_up, rows_of(m_d)))
    send("gd", lambda: (rows_of(tp), rows_of(tp), y_down, rows_of(m_u)))
    send("gs", lambda: (rows_of(tp), rows_of(tp), sibling, rows_of(y * 2 + 1 - c)))
    take("bz1u", "bz1d")
    send("bz2u", lambda: (down_blocks(zd * 4, 2), down_blocks(zd * 4, 2), above, down_blocks(zf * 4, 2)))
    send("bz2d", lambda: (down_blocks(zu * 4 + 2, 2), down_blocks(zu * 4 + 2, 2), below, down_blocks(zf * 4 + 2, 2)))
    take("wx2r0", "wx2ld", "wx2ru", "wx2lu", "wx2rf", "wx2lf")

    def up_group(*chips):
        def some(start, width):
            cols_ = pl.ds(start, width)
            rhs = jnp.concatenate([wbuf[b, cols_, :] for b in range(16)], axis=1)
            lhs = [mixed[pl.ds(pl.multiple_of(yy * 192, 64), 192), :] for yy in chips]
            part = lax.dot_general(
                jnp.concatenate(lhs, axis=0), rhs, (((1,), (1,)), ((), ())), preferred_element_type=F32
            ).astype(BF16)
            for k, yy in enumerate(chips):
                into = pl.ds(pl.multiple_of(yy * 192 + 16, 16), 192)
                both[into, cols_] = part[k * 192 : (k + 1) * 192]

        def chunk(i, _):
            some(pl.multiple_of(i * 256, 256), 256)
            return 0

        lax.fori_loop(0, 5, chunk, 0)
        some(1280, 128)

    def send_halo():
        pltpu.make_async_remote_copy(
            src_ref=both.at[pl.ds(BLK, 16)],
            dst_ref=halo,
            send_sem=ssem.at[HALO_SEM],
            recv_sem=rsem.at[HALO_SEM],
            device_id=after,
            device_id_type=MESH,
        ).start()

    def wait_halo(which):
        copy = pltpu.make_async_remote_copy(
            src_ref=both.at[pl.ds(BLK, 16)],
            dst_ref=halo,
            send_sem=ssem.at[HALO_SEM],
            recv_sem=rsem.at[HALO_SEM],
            device_id=after,
            device_id_type=MESH,
        )
        copy.wait_recv() if which else copy.wait_send()

    take("gs")
    up_group(y)
    pl.when(y == 3)(send_halo)
    take("gu", "gd")
    send("g2u", lambda: (rows_of(m_d, 0, 48), rows_of(m_d, 0, 48), y_up, rows_of(m_f, 0, 48)))
    send("g2d", lambda: (rows_of(m_u, 48, 48), rows_of(m_u, 48, 48), y_down, rows_of(m_f, 48, 48)))
    send("gs1", lambda: (rows_of(m_d), rows_of(m_d), sibling, rows_of(s_d)))
    send("gs2", lambda: (rows_of(m_u), rows_of(m_u), sibling, rows_of(s_u)))
    take("gs1", "gs2")
    up_group(yd, yu)
    pl.when((yd == 3) | (yu == 3))(send_halo)
    take("g2u", "g2d")
    send("gs3", lambda: (rows_of(m_f), rows_of(m_f), sibling, rows_of(s_f)))
    take("gs3")
    up_group(yf)
    pl.when(yf == 3)(send_halo)

    taps[0:3, 0:640] = vtaps_ref[:, 0:640]
    taps[0:3, 640:1280] = gtaps_ref[:, 0:640]
    taps[0:3, 1280:1408] = jnp.concatenate([vtaps_ref[:, 640:704], gtaps_ref[:, 640:704]], axis=1)

    def filtered(a, lanes_):
        n = a.shape[0] - 16
        return (
            taps[0:1, lanes_] * a[14 : 14 + n]
            + taps[1:2, lanes_] * a[15 : 15 + n]
            + taps[2:3, lanes_] * a[16 : 16 + n]
        )

    def hidden_rows(i):
        src = pl.ds(pl.multiple_of(i * OWN, 32), OWN + 16)
        dst = pl.ds(pl.multiple_of(i * OWN, 32), OWN)
        for g in range(6):
            if g < 5:
                at_v, at_g = slice(g * 128, (g + 1) * 128), slice(640 + g * 128, 768 + g * 128)
                fv = filtered(both[src, at_v].astype(F32), at_v)
                fg = filtered(both[src, at_g].astype(F32), at_g)
            else:
                last = slice(1280, 1408)
                fv = filtered(both[src, last].astype(F32), last)
                fg = pltpu.roll(fv, 64, 1)
            value = fg / (1.0 + jnp.exp(-fg)) * fv
            if g == 5:
                value = jnp.where(lane < 64, value, 0.0)
            hid[dst, g * 128 : (g + 1) * 128] = value.astype(BF16)

    def hidden_group(yy):
        @pl.when(yy == 0)
        def _():
            wait_halo(True)
            both[0:16, :] = jnp.where(sp == 0, 0.0, halo[...].astype(F32)).astype(BF16)

        def chunk(i, _):
            hidden_rows(yy * 2 + i)
            return 0

        lax.fori_loop(0, 2, chunk, 0)

    def down_group(g, yy):
        mine = hid[pl.ds(pl.multiple_of(yy * 192 + c * OWN, 32), OWN), :]
        other = hid[pl.ds(pl.multiple_of(yy * 192 + (1 - c) * OWN, 32), OWN), :]
        lhs = jnp.concatenate([mine, other], axis=0)

        def some(i, _):
            col = pl.ds(pl.multiple_of(i * 256, 256), 256)
            rhs = jnp.concatenate(
                [wbuf[2 * i, 1408 : WROWS + 64, :], wbuf[2 * i + 1, 1408 : WROWS + 64, :]], axis=1
            )
            part = jnp.dot(lhs, rhs, preferred_element_type=F32)
            keep[g, :, col] = part[:OWN]
            sib_out[g, :, col] = part[OWN:].astype(BF16)
            return 0

        lax.fori_loop(0, 8, some, 0)

    def send_sib(g):
        send("r%d" % g, lambda: (sib_out.at[g], sib_in.at[g], sibling, sib_in.at[g]))

    def pair_sum(g, lo, hi):
        return keep[g, :, lo:hi] + sib_in[g, :, lo:hi].astype(F32)

    take("bz2u", "bz2d")

    def near(k, h):
        send(
            "n%d%d" % (k, h),
            lambda: (near_out.at[k, h], near_in.at[k, h], (y_up, y_down)[k], near_in.at[k, h]),
        )

    def ffn_step(g, _):
        yy = (y + jnp.where(g == 0, 2, jnp.where(g == 1, 3, jnp.where(g == 2, 1, 0)))) % 4
        hidden_group(yy)
        down_group(g, yy)

        @pl.when(g == 0)
        def _():
            send_sib(0)

        @pl.when(g == 1)
        def _():
            send_sib(1)
            take("r0")
            far_out[0] = pair_sum(0, 0, HALF).astype(BF16)
            far_out[1] = pair_sum(0, HALF, 2 * HALF).astype(BF16)
            send("fu", lambda: (far_out.at[0], far_in.at[0], y_up, far_in.at[0]))
            send("fd", lambda: (far_out.at[1], far_in.at[1], y_down, far_in.at[1]))

        @pl.when(g == 2)
        def _():
            send_sib(2)
            take("r1")
            near_out[1, 0] = pair_sum(1, 0, HALF).astype(BF16)
            near(1, 0)

        @pl.when(g == 3)
        def _():
            send_sib(3)
            take("r2")
            near_out[0, 1] = pair_sum(2, HALF, 2 * HALF).astype(BF16)
            near(0, 1)

        return 0

    lax.fori_loop(0, 4, ffn_step, 0)
    take("fu")
    near_out[0, 0] = (pair_sum(2, 0, HALF) + far_in[0].astype(F32)).astype(BF16)
    near(0, 0)
    take("fd")
    near_out[1, 1] = (pair_sum(1, HALF, 2 * HALF) + far_in[1].astype(F32)).astype(BF16)
    near(1, 1)
    take("r3", "n00", "n01", "n10", "n11")

    def last_norm(i, _):
        r = pl.ds(pl.multiple_of(i * 16, 16), 16)
        t = pl.ds(pl.multiple_of(tp * OWN + i * 16, 16), 16)
        far = [near_in[0, h, r, :].astype(F32) + near_in[1, h, r, :].astype(F32) for h in range(2)]
        ffn = keep[3, r, :] + sib_in[3, r, :].astype(F32) + jnp.concatenate(far, axis=1)
        whole = residual_scale * mixed[t, :].astype(F32) + ffn
        out_ref[r, :] = norm(whole, fgain_ref[...]).astype(BF16)
        return 0

    lax.fori_loop(0, OWN // 16, last_norm, 0)
    wait_halo(False)
    for wait in sent:
        wait()


def whole_layer(*operands):
    vmem = pl.BlockSpec(memory_space=pltpu.VMEM)
    return pl.pallas_call(
        layer_kernel,
        out_shape=jax.ShapeDtypeStruct((OWN, 2048), BF16),
        in_specs=[vmem] * len(operands),
        out_specs=vmem,
        scratch_shapes=[
            pltpu.VMEM((2, BLK + EXTRA, 256), BF16),
            pltpu.VMEM((2, BLK, 128), BF16),
            pltpu.VMEM((16, BLK + EXTRA, 256), BF16),
            pltpu.VMEM((BLK, 128), BF16),
            pltpu.VMEM((EXTRA, 256), BF16),
            pltpu.VMEM((3, 2, BLK, 128), BF16),
            pltpu.VMEM((3, 2, BLK, 128), F32),
            pltpu.VMEM((32, 8, BLK), F32),
            pltpu.VMEM((3, 2, BLK, 128), F32),
            pltpu.VMEM((3, 2, BLK, 128), F32),
            pltpu.VMEM((3, BLK, 128), F32),
            pltpu.VMEM((RQ, BLK), F32),
            pltpu.VMEM((RQ, 128), F32),
            pltpu.VMEM((RQ, BLK), BF16),
            pltpu.VMEM((RQ, 128), F32),
            pltpu.VMEM((2, BLK, 128), BF16),
            pltpu.VMEM((16, WROWS + 64, 128), BF16),
            pltpu.VMEM((2048, 2048), BF16),
            pltpu.VMEM((16, OWN, 128), BF16),
            pltpu.VMEM((OWN, 2048), F32),
            pltpu.VMEM((BLK, 2048), BF16),
            pltpu.VMEM((BLK + 16, 1408), BF16),
            pltpu.VMEM((16, 1408), BF16),
            pltpu.VMEM((8, 1408), F32),
            pltpu.VMEM((BLK, 768), BF16),
            pltpu.VMEM((4, OWN, 2048), F32),
            pltpu.VMEM((4, OWN, 2048), BF16),
            pltpu.VMEM((4, OWN, 2048), BF16),
            pltpu.VMEM((2, OWN, HALF), BF16),
            pltpu.VMEM((2, OWN, HALF), BF16),
            pltpu.VMEM((2, 2, OWN, HALF), BF16),
            pltpu.VMEM((2, 2, OWN, HALF), BF16),
            pltpu.SemaphoreType.DMA((112,)),
            pltpu.SemaphoreType.DMA((112,)),
            pltpu.SemaphoreType.DMA((2,)),
        ],
        compiler_params=pltpu.CompilerParams(
            collective_id=1, has_side_effects=True, vmem_limit_bytes=VMEM_ALL
        ),
        cost_estimate=pl.CostEstimate(flops=20_000_000_000, bytes_accessed=40_000_000, transcendentals=0),
    )(*operands)


def per_device(
    query_small,
    key_small,
    value_small,
    gates_small,
    query_large,
    key_large,
    value_large,
    gates_large,
    residual,
    mixer_small,
    mixer_large,
    mix_gain,
    value_weight,
    gate_weight,
    value_taps,
    gate_taps,
    down_weight,
    final_gain,
):
    return whole_layer(
        query_small,
        key_small,
        value_small,
        query_large,
        key_large,
        value_large,
        gates_small.T,
        gates_large.T,
        value_weight.T,
        gate_weight.T,
        down_weight,
        mixer_small,
        mixer_large,
        residual,
        mix_gain[None],
        final_gain[None],
        value_taps,
        gate_taps,
    )


def solution(mesh):
    split = Mesh(mesh.devices.reshape(mesh.shape["sp"], 4, 2), ("sp", "tp_0", "tp_1"))
    placed = (
        P("sp", TP),
        P("sp", TP),
        P("sp", TP),
        P("sp", TP),
        P("sp", TP),
        P("sp", TP),
        P("sp", TP),
        P("sp", TP),
        P(SP_TP, None),
        P(TP, None),
        P(TP, None),
        P(),
        P("sp", TP),
        P("sp", TP),
        P(None, TP),
        P(None, TP),
        P(TP, "sp"),
        P(),
    )
    return jax.shard_map(
        per_device, mesh=split, in_specs=placed, out_specs=P(SP_TP, None), check_vma=False
    )
```

```python
import functools

import jax
import jax.numpy as jnp
from jax import lax
from jax.experimental import pallas as pl
from jax.experimental.pallas import tpu as pltpu
from jax.sharding import Mesh
from jax.sharding import PartitionSpec as P

TP = ("tp_0", "tp_1")
SP_TP = ("sp", "tp_0", "tp_1")
LOG2E = 1.4426950408889634
residual_scale = 2.0**0.5
epsilon = 1e-05
MESH = pl.DeviceIdType.MESH
BLK = 768
EXTRA = 32
WROWS = 2112
UP = 1408
DOWN = 704
RQ = 384
F32 = jnp.float32
BF16 = jnp.bfloat16
VMEM_ALL = 67_000_000
OWN = 96
HALF = 1024
HALO_SEM = 111


def layer_kernel(
    qs_ref,
    ks_ref,
    vs_ref,
    ql_ref,
    kl_ref,
    vl_ref,
    gs_ref,
    gl_ref,
    vw_ref,
    gw_ref,
    down_ref,
    ms_ref,
    ml_ref,
    res_ref,
    mgain_ref,
    fgain_ref,
    vtaps_ref,
    gtaps_ref,
    out_ref,
    kvin,
    qin,
    kvbuf,
    qpair,
    qgate,
    qm,
    gq,
    gk,
    mst,
    lst,
    acc,
    sbuf,
    mbuf,
    pbuf,
    abuf,
    outv,
    wbuf,
    mixbuf,
    arrived,
    ybuf,
    mixed,
    both,
    halo,
    taps,
    hid,
    keep,
    sib_out,
    sib_in,
    far_out,
    far_in,
    near_out,
    near_in,
    ssem,
    rsem,
    lsem,
):
    sp = lax.axis_index("sp")
    y = lax.axis_index("tp_0")
    c = lax.axis_index("tp_1")
    z, x = sp // 4, sp % 4
    role = x // 2
    xr, xl = (x + 1) % 4, (x + 3) % 4
    zu, zd = (z + 1) % 4, (z + 3) % 4
    yu, yd = (y + 1) % 4, (y + 3) % 4
    xf, zf, yf = (x + 2) % 4, (z + 2) % 4, (y + 2) % 4
    mate = x + 1 - 2 * (x % 2)
    opp = 3 - x
    diag = opp + 1 - 2 * (opp % 2)
    pair_sp = 15 - sp
    tp = y * 2 + c

    def at(zz, xx):
        return (zz * 4 + xx, y, c)

    right, left = at(z, xr), at(z, xl)
    above, below = at(zu, x), at(zd, x)
    mate_dev, opp_dev = at(z, mate), at(z, opp)
    pair_dev = (pair_sp, y, c)
    y_up, y_down = (sp, yu, c), (sp, yd, c)
    sibling = (sp, y, 1 - c)
    after, before = ((sp + 1) % 16, y, c), ((sp + 15) % 16, y, c)

    barrier = pltpu.get_barrier_semaphore()
    greeted = [right, left, above, below, after, before]
    for d in range(8):
        t = (tp + d) % 8
        if d:
            greeted.append((sp, t // 2, t % 2))
        greeted.append((pair_sp, t // 2, t % 2))
    for dev in greeted:
        pl.semaphore_signal(barrier, inc=1, device_id=dev, device_id_type=MESH)

    lane = lax.broadcasted_iota(jnp.int32, (1, 128), 1)

    for r, (q_ref, k_ref, v_ref, g_ref) in enumerate(
        ((qs_ref, ks_ref, vs_ref, gs_ref), (ql_ref, kl_ref, vl_ref, gl_ref))
    ):
        kvin[r, 0:BLK, 0:128] = k_ref[...]
        kvin[r, 0:BLK, 128:256] = v_ref[...]
        qin[r] = q_ref[...]
        pieces = []
        for h in range(2 - r):
            left_over = g_ref[h : h + 1, :] * LOG2E
            for i in range(3):
                part = left_over.astype(BF16).astype(F32)
                left_over = left_over - part
                pieces += [part[:, p * 256 : (p + 1) * 256] for p in range(3)]
        pieces.append(jnp.zeros((EXTRA - len(pieces), 256), F32))
        kvin[r, BLK : BLK + EXTRA, :] = jnp.concatenate(pieces, axis=0).astype(BF16)

    def mix_rows(t, start=0, size=256):
        return mixbuf.at[pl.ds(pl.multiple_of(t * 256 + start, 128), size)]

    def up_block(b, start=0, size=UP):
        return wbuf.at[b, pl.ds(start, size)]

    def down_blocks(b, count=1, start=0, size=DOWN):
        return wbuf.at[pl.ds(b, count), pl.ds(UP + start, size)]

    wbuf[sp, 0:640, :] = vw_ref[0:640, :]
    wbuf[sp, 640:1280, :] = gw_ref[0:640, :]
    wbuf[sp, 1280:1344, :] = vw_ref[640:704, :]
    wbuf[sp, 1344:1408, :] = gw_ref[640:704, :]
    wbuf[sp, 1408:WROWS, :] = down_ref[...]
    for b in range(16):
        wbuf[b, WROWS : WROWS + 64, :] = jnp.zeros((64, 128), BF16)
    mixbuf[pl.ds(pl.multiple_of(tp * 256, 256), 128), :] = ms_ref[...]
    mixbuf[pl.ds(pl.multiple_of(tp * 256 + 128, 128), 128), :] = ml_ref[...]

    pl.semaphore_wait(barrier, len(greeted))

    sent = []
    counter = [0]
    incoming = {}

    def send(name, ends, sends=None, receives=None, now=None):
        k = counter[0]
        counter[0] += 1

        def copy(arriving):
            src, dst, dev, landing = ends()
            return pltpu.make_async_remote_copy(
                src_ref=landing if arriving else src,
                dst_ref=landing if arriving else dst,
                send_sem=ssem.at[k],
                recv_sem=rsem.at[k],
                device_id=dev,
                device_id_type=MESH,
            )

        def only(condition, act):
            act() if condition is None else pl.when(condition())(act)

        sent.append(lambda: only(sends, lambda: copy(False).wait_send()))
        incoming[name] = lambda: only(receives, lambda: copy(True).wait_recv())
        only(now or sends, lambda: copy(False).start())
        return lambda: copy(False).start()

    def take(*names):
        for name in names:
            incoming.pop(name)()

    cols = {"own": x, "mate": mate, "opp": opp, "diag": diag}

    send("x1m", lambda: (kvin.at[role], kvbuf.at[sp], mate_dev, kvbuf.at[z * 4 + mate]))
    send("x1o", lambda: (kvin.at[1 - role], kvbuf.at[sp], opp_dev, kvbuf.at[z * 4 + opp]))
    send("z1u_own", lambda: (kvin.at[role], kvbuf.at[sp], above, kvbuf.at[zd * 4 + x]))
    send("z1d_own", lambda: (kvin.at[role], kvbuf.at[sp], below, kvbuf.at[zu * 4 + x]), lambda: z < 3, lambda: z != 2)
    gate_part = pl.ds(BLK, EXTRA)
    send("qg", lambda: (kvin.at[1 - role, gate_part], qgate, pair_dev, qgate))
    send("q", lambda: (qin.at[1 - role], qpair, pair_dev, qpair))
    send("y1u", lambda: (mix_rows(tp), mix_rows(tp), y_up, mix_rows(yd * 2 + c)))
    send("y1d", lambda: (mix_rows(tp), mix_rows(tp), y_down, mix_rows(yu * 2 + c)))
    send("s0", lambda: (mix_rows(tp), mix_rows(tp), sibling, mix_rows(y * 2 + 1 - c)))

    def pass_x(tag, zz):
        def ends(dev, col):
            mine = up_block(zz * 4 + x)
            return mine, mine, dev, up_block(zz * 4 + col)

        send("wx1r" + tag, lambda: ends(right, xl))
        send("wx1l" + tag, lambda: ends(left, xr))

    own_kv = pltpu.make_async_copy(kvin.at[role], kvbuf.at[sp], lsem.at[0])
    own_kv.start()

    heads = 2 - role
    head_dim = 64 + 64 * role
    scale = jnp.where(role == 0, 0.125 * LOG2E, 128.0**-0.5 * LOG2E).astype(F32)

    def head_lanes(h):
        return (lane >= h * 64) & (lane < h * 64 + head_dim)

    def gate_row(rows, h, g):
        k, at_ = h * 9 + g // 2, slice((g % 2) * 128, (g % 2) * 128 + 128)
        return rows[k : k + 1, at_] + rows[k + 3 : k + 4, at_] + rows[k + 6 : k + 7, at_]

    same = lax.broadcasted_iota(jnp.int32, (128, 128), 0) == lax.broadcasted_iota(
        jnp.int32, (128, 128), 1
    )

    def load_queries(qi, queries, gate_block):
        rows = gate_block.astype(F32)
        for h in range(2):
            ones = jnp.where(head_lanes(h), 1.0, 0.0).astype(BF16)
            qm[qi, h] = queries * ones
            for g in range(BLK // 128):
                line = jnp.broadcast_to(gate_row(rows, h, g), (128, 128))
                column = jnp.sum(jnp.where(same, line, 0.0), axis=1, keepdims=True)
                gq[qi, h, g * 128 : (g + 1) * 128, :] = jnp.broadcast_to(column, (128, 128))

    load_queries(0, qin[role], kvin[role, BLK : BLK + EXTRA, :])
    mst[...] = jnp.full(mst.shape, -1e30, F32)
    lst[...] = jnp.zeros(lst.shape, F32)
    acc[...] = jnp.zeros(acc.shape, F32)

    def pass_z(tag):
        col = cols[tag]
        src = kvbuf.at[z * 4 + col]
        send("z1u_" + tag, lambda: (src, src, above, kvbuf.at[zd * 4 + col]))
        send("z1d_" + tag, lambda: (src, src, below, kvbuf.at[zu * 4 + col]), lambda: z < 3, lambda: z != 2)

    b_d, b_u, b_f = zd * 4 + x, zu * 4 + x, zf * 4 + x
    b_l, b_r, b_o = z * 4 + xl, z * 4 + xr, z * 4 + (x + 2) % 4
    dhalf = DOWN // 2
    take("x1o")
    send("x2", lambda: (kvbuf.at[z * 4 + opp], kvbuf.at[z * 4 + opp], mate_dev, kvbuf.at[z * 4 + diag]))
    pass_z("opp")
    take("x1m")
    pass_z("mate")
    send("wz1u", lambda: (up_block(sp), up_block(sp), above, up_block(b_d)))
    send("wz1d", lambda: (up_block(sp), up_block(sp), below, up_block(b_u)))
    send("bx1r", lambda: (down_blocks(sp), down_blocks(sp), right, down_blocks(b_l)))
    send("bx1l", lambda: (down_blocks(sp), down_blocks(sp), left, down_blocks(b_r)))
    pass_x("0", z)
    own_kv.wait()
    take("x2")
    pass_z("diag")
    take("z1u_own", "z1d_own")
    send(
        "z2u_own",
        lambda: (kvbuf.at[zd * 4 + x], kvbuf.at[zd * 4 + x], above, kvbuf.at[zf * 4 + x]),
        lambda: z >= 2,
        lambda: (z == 0) | (z == 3),
    )
    send(
        "z2x_own",
        lambda: (kvbuf.at[zu * 4 + x], kvbuf.at[zu * 4 + x], below, kvbuf.at[zf * 4 + x]),
        lambda: z == 3,
        lambda: z == 2,
    )
    take("bx1r", "bx1l")
    send(
        "bx2r",
        lambda: (down_blocks(b_l, 1, 0, dhalf), down_blocks(b_l, 1, 0, dhalf), right, down_blocks(b_o, 1, 0, dhalf)),
    )
    send(
        "bx2l",
        lambda: (down_blocks(b_r, 1, dhalf, dhalf), down_blocks(b_r, 1, dhalf, dhalf), left, down_blocks(b_o, 1, dhalf, dhalf)),
    )
    take("q", "qg")
    load_queries(1, qpair[...], qgate[...])

    def gate_rows(j):
        rows = kvbuf[j, BLK : BLK + EXTRA, :].astype(F32)
        for h in range(2):
            for g in range(BLK // 128):
                line = jnp.broadcast_to(gate_row(rows, h, g), (8, 128))
                gk[j * 2 + h, :, g * 128 : (g + 1) * 128] = line

    def scores(qi, j, h, sub, masked):
        rows = pl.ds(sub * RQ, RQ)
        span = (sub + 1) * RQ if masked else BLK
        raw = lax.dot_general(
            qm[qi, h, rows, :],
            kvbuf[j, 0:span, 0:128],
            (((1,), (1,)), ((), ())),
            preferred_element_type=F32,
        )
        gate = gk[j * 2 + h, 0:1, 0:span]
        parts = []
        for g in range(span // 128):
            part = raw[:, g * 128 : (g + 1) * 128] * scale - gate[:, g * 128 : (g + 1) * 128]
            if masked and (g + 1) * 128 > sub * RQ:
                col = lax.broadcasted_iota(jnp.int32, (RQ, 128), 1) + (g * 128 - sub * RQ)
                row = lax.broadcasted_iota(jnp.int32, (RQ, 128), 0)
                part = jnp.where(col <= row, part, -1e30)
            parts.append(part)
        return parts, functools.reduce(jnp.maximum, parts)

    def soften(parts, peak, qi, j, h, sub):
        rows = pl.ds(sub * RQ, RQ)
        peak = jnp.max(peak, axis=1, keepdims=True)
        g_here = gq[qi, h, rows, :]
        old = mst[qi, h, rows, :]
        new = jnp.maximum(old, peak + g_here)
        alpha = jnp.exp2(old - new)
        shift = new - g_here
        weights_ = [jnp.exp2(part - shift) for part in parts]
        mst[qi, h, rows, :] = new
        lst[qi, h, rows, :] = lst[qi, h, rows, :] * alpha + functools.reduce(jnp.add, weights_)
        return jnp.concatenate([a.astype(BF16) for a in weights_], axis=1), alpha

    def hold(parts, peak):
        for g, part in enumerate(parts):
            sbuf[:, g * 128 : (g + 1) * 128] = part
        mbuf[...] = peak

    def held():
        return [sbuf[:, g * 128 : (g + 1) * 128] for g in range(BLK // 128)], mbuf[...]

    def spread(w, alpha, qi, j, h, sub, masked):
        rows = pl.ds(sub * RQ, RQ)
        span = (sub + 1) * RQ if masked else BLK
        mask = head_lanes(h)
        v = kvbuf[j, 0:span, 128:256] * jnp.where(mask, 1.0, 0.0).astype(BF16)
        update = jnp.dot(w, v, preferred_element_type=F32)
        acc[qi, rows, :] = acc[qi, rows, :] * jnp.where(mask, alpha, 1.0) + update

    def tiles(qi, j, h, masked):
        count = BLK // RQ
        ahead = scores(qi, j, h, 0, masked)
        for sub in range(count):
            here = ahead
            ahead = scores(qi, j, h, sub + 1, masked) if sub + 1 < count else None
            w, alpha = soften(*here, qi, j, h, sub)
            spread(w, alpha, qi, j, h, sub, masked)

    blocks_of = (sp, pair_sp)

    def attend(step):
        row = jnp.where(step == 0, z, jnp.where(step == 2, zd, jnp.where(step == 3, zu, zf)))
        second = step == 1
        none = 99
        slots = (
            jnp.where(second, zd * 4 + x, row * 4 + mate),
            jnp.where(second, zu * 4 + x, row * 4 + opp),
            jnp.where(second, none, row * 4 + diag),
            jnp.where(step == 0, sp, jnp.where(step == 3, zf * 4 + x, none)),
        )
        for j in slots:
            pl.when(j <= jnp.maximum(sp, pair_sp))(functools.partial(gate_rows, j))

        found, count = [], 0
        for qi in range(2):
            for j in slots:
                flag = jnp.where(j < blocks_of[qi], 1, 0)
                found.append((qi, j, flag, count))
                count = count + flag
        units = count * heads

        def place(u):
            v = jnp.clip(u, 0, units - 1)
            k = v // heads
            hits = [(qi, j, jnp.where(before_ == k, flag, 0)) for qi, j, flag, before_ in found]
            qi = sum(hit * qi for qi, _, hit in hits)
            j = sum(hit * j for _, j, hit in hits)
            return jnp.where(u == v, qi, 2), j, v % heads

        def two_units(i, _):
            spread(pbuf[...], abuf[...], *place(2 * i - 1), 1, False)
            here = held()
            for t in range(4):
                now = place(2 * i + t // 2)
                ahead = scores(*place(2 * i + (t + 1) // 2), (t + 1) % 2, False)
                w, alpha = soften(*here, *now, t % 2)
                if t < 3:
                    spread(w, alpha, *now, t % 2, False)
                here = ahead
            hold(*here)
            pbuf[...] = w
            abuf[...] = alpha
            return 0

        @pl.when(units > 0)
        def _():
            hold(*scores(*place(0), 0, False))
            steps = (units + 1) // 2
            lax.fori_loop(0, steps, two_units, 0)
            spread(pbuf[...], abuf[...], *place(2 * steps - 1), 1, False)

        @pl.when((step == 0) | (step == 2 + z % 2))
        def _():
            qi = jnp.where(step == 0, 0, 1)

            def for_head(h, _):
                tiles(qi, jnp.where(step == 0, sp, pair_sp), h, True)
                return 0

            lax.fori_loop(0, heads, for_head, 0)

    def pass_on(tag, name, from_z, dev, landing_z, sends, receives):
        col = cols[tag]

        def ends():
            src = kvbuf.at[from_z * 4 + col]
            return src, src, dev, kvbuf.at[landing_z * 4 + col]

        send(name + tag, ends, sends, receives)

    m_d, m_u, m_f = yd * 2 + c, yu * 2 + c, yf * 2 + c
    s_d, s_u, s_f = yd * 2 + 1 - c, yu * 2 + 1 - c, yf * 2 + 1 - c

    def pass_x2(tag, zz, name, col, dev, start=0, size=UP, now=None):
        def ends():
            src = up_block(zz * 4 + col, start, size)
            return src, src, dev, up_block(zz * 4 + xf, start, size)

        return send(name + tag, ends, now=now)

    uhalf = UP // 2

    def both_ways(tag, zz):
        pass_x2(tag, zz, "wx2r", xl, right, 0, uhalf)
        pass_x2(tag, zz, "wx2l", xr, left, uhalf, uhalf)

    def down_pair(name, zz, first, dev, landing):
        def ends():
            src = down_blocks(zz * 4 + first, 2)
            return src, src, dev, down_blocks(landing * 4 + first, 2)

        send(name, ends)

    def one_step(step, _):
        attend(step)

        @pl.when(step == 1)
        def _():
            take("wz1u", "wz1d")
            send("wz2u", lambda: (up_block(b_d, 0, uhalf), up_block(b_d, 0, uhalf), above, up_block(b_f, 0, uhalf)))
            send("wz2d", lambda: (up_block(b_u, uhalf, uhalf), up_block(b_u, uhalf, uhalf), below, up_block(b_f, uhalf, uhalf)))
            pass_x("d", zd)
            pass_x("u", zu)
            take("y1u", "y1d")
            send("y2u", lambda: (mix_rows(m_d, 0, 128), mix_rows(m_d, 0, 128), y_up, mix_rows(m_f, 0, 128)))
            send("y2d", lambda: (mix_rows(m_u, 128, 128), mix_rows(m_u, 128, 128), y_down, mix_rows(m_f, 128, 128)))
            send("s1", lambda: (mix_rows(m_d), mix_rows(m_d), sibling, mix_rows(s_d)))
            send("s2", lambda: (mix_rows(m_u), mix_rows(m_u), sibling, mix_rows(s_u)))
            take("z1u_mate", "z1d_mate")
            pass_on("mate", "z2u_", zd, above, zf, lambda: z >= 1, lambda: z != 1)
            take("z1u_opp", "z1d_opp", "z1u_diag", "z1d_diag")
            pass_on("opp", "z2d_", zu, below, zf, lambda: z != 2, lambda: z != 1)
            pass_on("diag", "z2d_", zu, below, zf, lambda: z != 2, lambda: z != 1)
            take("wx1r0", "wx1l0")
            both_ways("0", z)

        @pl.when(step == 2)
        def _():
            take("z2u_own", "z2x_own")
            take("wz2u", "wz2d")
            pass_x("f", zf)

        @pl.when(step == 2)
        def _():
            take("wx1rd", "wx1ld", "wx1ru", "wx1lu")
            both_ways("d", zd)
            both_ways("u", zu)

        @pl.when(step == 3)
        def _():
            take("y2u", "y2d")
            send("s3", lambda: (mix_rows(m_f), mix_rows(m_f), sibling, mix_rows(s_f)))
            take("z2u_mate", "z2d_opp", "z2d_diag")
            take("bx2r", "bx2l")
            down_pair("bz1u", z, 0, above, zd)
            down_pair("bz1d", z, 2, below, zu)

        return 0

    lax.fori_loop(0, 5, one_step, 0)

    keep0 = head_lanes(0)
    for qi in (1, 0):
        l0 = jnp.sum(lst[qi, 0], axis=1, keepdims=True)
        l1 = jnp.sum(lst[qi, 1], axis=1, keepdims=True)
        outv[qi] = (acc[qi] / jnp.where(keep0, l0, l1)).astype(BF16)

    def own_rows(t):
        return pl.ds(pl.multiple_of(t * OWN, 32), OWN)

    slot = tp * 2 + role

    def send_out(d):
        t, s = (tp + d) % 8, (tp + 8 - d) % 8
        dst = (t // 2, t % 2)
        send(
            "p%d" % d,
            lambda: (outv.at[1, own_rows(t)], arrived.at[slot], (pair_sp, *dst), arrived.at[s * 2 + 1 - role]),
        )
        if d:
            send(
                "a%d" % d,
                lambda: (outv.at[0, own_rows(t)], arrived.at[slot], (sp, *dst), arrived.at[s * 2 + role]),
            )

    for d in range(8):
        send_out(d)
    far_waits = [incoming.pop("wx1rf"), incoming.pop("wx1lf")]
    is_large = lambda: role == 1

    @pl.when(role == 1)
    def _():
        for wait in far_waits:
            wait()

    far_sends = [
        pass_x2("f", zf, "wx2r", xl, right, 0, uhalf, is_large),
        pass_x2("f", zf, "wx2l", xr, left, uhalf, uhalf, is_large),
    ]
    arrived[slot] = outv[0, own_rows(tp), :]
    take("s0", "s1", "s2", "s3")
    for d in range(8):
        take("p%d" % d)
        if d:
            take("a%d" % d)

    @pl.when(role == 0)
    def _():
        for wait in far_waits:
            wait()
        for start in far_sends:
            start()

    take("bz1u", "bz1d")
    down_pair("bz2u", zd, 0, above, zf)
    down_pair("bz2d", zu, 2, below, zf)
    down_pair("bz3u", z, 2, above, zd)
    down_pair("bz3d", z, 0, below, zu)

    def project(i, _):
        col = pl.ds(pl.multiple_of(i * 256, 256), 256)
        lhs = jnp.concatenate([arrived[s] for s in range(16)], axis=1)
        part = jnp.dot(lhs, mixbuf[:, col], preferred_element_type=F32)
        ybuf[:, col] = residual_scale * res_ref[:, col].astype(F32) + part
        return 0

    lax.fori_loop(0, 8, project, 0)

    def norm(values, gain):
        center = jnp.mean(values, axis=1, keepdims=True)
        off = values - center
        spread = jnp.mean(jnp.square(off), axis=1, keepdims=True)
        return off * lax.rsqrt(spread + epsilon) * gain

    def first_norm(i, _):
        r = pl.ds(pl.multiple_of(i * 16, 16), 16)
        t = pl.ds(pl.multiple_of(tp * OWN + i * 16, 16), 16)
        mixed[t, :] = norm(ybuf[r, :], mgain_ref[...]).astype(BF16)
        return 0

    lax.fori_loop(0, OWN // 16, first_norm, 0)

    def rows_of(t, start=0, size=OWN):
        return mixed.at[pl.ds(pl.multiple_of(t * OWN + start, 16), size)]

    send("gu", lambda: (rows_of(tp), rows_of(tp), y_up, rows_of(m_d)))
    send("gd", lambda: (rows_of(tp), rows_of(tp), y_down, rows_of(m_u)))
    send("gs", lambda: (rows_of(tp), rows_of(tp), sibling, rows_of(y * 2 + 1 - c)))
    take("wx2r0", "wx2l0", "wx2rd", "wx2ld", "wx2ru", "wx2lu", "wx2rf", "wx2lf")

    def up_group(*chips):
        def some(start, width):
            cols_ = pl.ds(start, width)
            rhs = jnp.concatenate([wbuf[b, cols_, :] for b in range(16)], axis=1)
            lhs = [mixed[pl.ds(pl.multiple_of(yy * 192, 64), 192), :] for yy in chips]
            part = lax.dot_general(
                jnp.concatenate(lhs, axis=0), rhs, (((1,), (1,)), ((), ())), preferred_element_type=F32
            ).astype(BF16)
            for k, yy in enumerate(chips):
                into = pl.ds(pl.multiple_of(yy * 192 + 16, 16), 192)
                both[into, cols_] = part[k * 192 : (k + 1) * 192]

        def chunk(i, _):
            some(pl.multiple_of(i * 256, 256), 256)
            return 0

        lax.fori_loop(0, 5, chunk, 0)
        some(1280, 128)

    def send_halo():
        pltpu.make_async_remote_copy(
            src_ref=both.at[pl.ds(BLK, 16)],
            dst_ref=halo,
            send_sem=ssem.at[HALO_SEM],
            recv_sem=rsem.at[HALO_SEM],
            device_id=after,
            device_id_type=MESH,
        ).start()

    def wait_halo(which):
        copy = pltpu.make_async_remote_copy(
            src_ref=both.at[pl.ds(BLK, 16)],
            dst_ref=halo,
            send_sem=ssem.at[HALO_SEM],
            recv_sem=rsem.at[HALO_SEM],
            device_id=after,
            device_id_type=MESH,
        )
        copy.wait_recv() if which else copy.wait_send()

    taps[0:3, 0:640] = vtaps_ref[:, 0:640]
    taps[0:3, 640:1280] = gtaps_ref[:, 0:640]
    taps[0:3, 1280:1408] = jnp.concatenate([vtaps_ref[:, 640:704], gtaps_ref[:, 640:704]], axis=1)

    def filtered(a, lanes_):
        n = a.shape[0] - 16
        return (
            taps[0:1, lanes_] * a[14 : 14 + n]
            + taps[1:2, lanes_] * a[15 : 15 + n]
            + taps[2:3, lanes_] * a[16 : 16 + n]
        )

    def hidden_rows(i):
        src = pl.ds(pl.multiple_of(i * OWN, 32), OWN + 16)
        dst = pl.ds(pl.multiple_of(i * OWN, 32), OWN)
        for g in range(6):
            if g < 5:
                at_v, at_g = slice(g * 128, (g + 1) * 128), slice(640 + g * 128, 768 + g * 128)
                fv = filtered(both[src, at_v].astype(F32), at_v)
                fg = filtered(both[src, at_g].astype(F32), at_g)
            else:
                last = slice(1280, 1408)
                fv = filtered(both[src, last].astype(F32), last)
                fg = pltpu.roll(fv, 64, 1)
            value = fg / (1.0 + jnp.exp(-fg)) * fv
            if g == 5:
                value = jnp.where(lane < 64, value, 0.0)
            hid[dst, g * 128 : (g + 1) * 128] = value.astype(BF16)

    def hidden_group(yy):
        @pl.when(yy == 0)
        def _():
            wait_halo(True)
            both[0:16, :] = jnp.where(sp == 0, 0.0, halo[...].astype(F32)).astype(BF16)

        def chunk(i, _):
            hidden_rows(yy * 2 + i)
            return 0

        lax.fori_loop(0, 2, chunk, 0)

    def down_group(g, yy):
        mine = hid[pl.ds(pl.multiple_of(yy * 192 + c * OWN, 32), OWN), :]
        other = hid[pl.ds(pl.multiple_of(yy * 192 + (1 - c) * OWN, 32), OWN), :]
        lhs = jnp.concatenate([mine, other], axis=0)

        def some(i, _):
            col = pl.ds(pl.multiple_of(i * 256, 256), 256)
            rhs = jnp.concatenate(
                [wbuf[2 * i, 1408 : WROWS + 64, :], wbuf[2 * i + 1, 1408 : WROWS + 64, :]], axis=1
            )
            part = jnp.dot(lhs, rhs, preferred_element_type=F32)
            keep[g, :, col] = part[:OWN]
            sib_out[g, :, col] = part[OWN:].astype(BF16)
            return 0

        lax.fori_loop(0, 8, some, 0)

    def send_sib(g):
        send("r%d" % g, lambda: (sib_out.at[g], sib_in.at[g], sibling, sib_in.at[g]))

    def pair_sum(g, lo, hi):
        return keep[g, :, lo:hi] + sib_in[g, :, lo:hi].astype(F32)

    def near(k, h):
        send(
            "n%d%d" % (k, h),
            lambda: (near_out.at[k, h], near_in.at[k, h], (y_up, y_down)[k], near_in.at[k, h]),
        )

    take("gs")
    up_group(y)
    pl.when(y == 3)(send_halo)
    take("gu", "gd")
    send("g2u", lambda: (rows_of(m_d, 0, 48), rows_of(m_d, 0, 48), y_up, rows_of(m_f, 0, 48)))
    send("g2d", lambda: (rows_of(m_u, 48, 48), rows_of(m_u, 48, 48), y_down, rows_of(m_f, 48, 48)))
    send("gs1", lambda: (rows_of(m_d), rows_of(m_d), sibling, rows_of(s_d)))
    send("gs2", lambda: (rows_of(m_u), rows_of(m_u), sibling, rows_of(s_u)))
    take("gs1", "gs2")
    up_group(yd, yu)
    pl.when((yd == 3) | (yu == 3))(send_halo)
    take("g2u", "g2d")
    send("gs3", lambda: (rows_of(m_f), rows_of(m_f), sibling, rows_of(s_f)))
    take("bz2u", "bz2d", "bz3u", "bz3d")
    hidden_group(yu)
    down_group(2, yu)
    send_sib(2)
    take("gs3")
    up_group(yf)
    pl.when(yf == 3)(send_halo)
    take("r2")
    near_out[0, 1] = pair_sum(2, HALF, 2 * HALF).astype(BF16)
    near(0, 1)
    hidden_group(yf)
    down_group(0, yf)
    send_sib(0)
    hidden_group(yd)
    take("r0")
    far_out[0] = pair_sum(0, 0, HALF).astype(BF16)
    far_out[1] = pair_sum(0, HALF, 2 * HALF).astype(BF16)
    send("fu", lambda: (far_out.at[0], far_in.at[0], y_up, far_in.at[0]))
    send("fd", lambda: (far_out.at[1], far_in.at[1], y_down, far_in.at[1]))
    down_group(1, yd)
    send_sib(1)
    hidden_group(y)
    take("r1")
    near_out[1, 0] = pair_sum(1, 0, HALF).astype(BF16)
    near(1, 0)
    down_group(3, y)
    send_sib(3)

    take("fu")
    near_out[0, 0] = (pair_sum(2, 0, HALF) + far_in[0].astype(F32)).astype(BF16)
    near(0, 0)
    take("fd")
    near_out[1, 1] = (pair_sum(1, HALF, 2 * HALF) + far_in[1].astype(F32)).astype(BF16)
    near(1, 1)
    take("r3", "n00", "n01", "n10", "n11")

    def last_norm(i, _):
        r = pl.ds(pl.multiple_of(i * 16, 16), 16)
        t = pl.ds(pl.multiple_of(tp * OWN + i * 16, 16), 16)
        far = [near_in[0, h, r, :].astype(F32) + near_in[1, h, r, :].astype(F32) for h in range(2)]
        ffn = keep[3, r, :] + sib_in[3, r, :].astype(F32) + jnp.concatenate(far, axis=1)
        whole = residual_scale * mixed[t, :].astype(F32) + ffn
        out_ref[r, :] = norm(whole, fgain_ref[...]).astype(BF16)
        return 0

    lax.fori_loop(0, OWN // 16, last_norm, 0)
    wait_halo(False)
    for wait in sent:
        wait()


def whole_layer(*operands):
    vmem = pl.BlockSpec(memory_space=pltpu.VMEM)
    return pl.pallas_call(
        layer_kernel,
        out_shape=jax.ShapeDtypeStruct((OWN, 2048), BF16),
        in_specs=[vmem] * len(operands),
        out_specs=vmem,
        scratch_shapes=[
            pltpu.VMEM((2, BLK + EXTRA, 256), BF16),
            pltpu.VMEM((2, BLK, 128), BF16),
            pltpu.VMEM((16, BLK + EXTRA, 256), BF16),
            pltpu.VMEM((BLK, 128), BF16),
            pltpu.VMEM((EXTRA, 256), BF16),
            pltpu.VMEM((3, 2, BLK, 128), BF16),
            pltpu.VMEM((3, 2, BLK, 128), F32),
            pltpu.VMEM((32, 8, BLK), F32),
            pltpu.VMEM((3, 2, BLK, 128), F32),
            pltpu.VMEM((3, 2, BLK, 128), F32),
            pltpu.VMEM((3, BLK, 128), F32),
            pltpu.VMEM((RQ, BLK), F32),
            pltpu.VMEM((RQ, 128), F32),
            pltpu.VMEM((RQ, BLK), BF16),
            pltpu.VMEM((RQ, 128), F32),
            pltpu.VMEM((2, BLK, 128), BF16),
            pltpu.VMEM((16, WROWS + 64, 128), BF16),
            pltpu.VMEM((2048, 2048), BF16),
            pltpu.VMEM((16, OWN, 128), BF16),
            pltpu.VMEM((OWN, 2048), F32),
            pltpu.VMEM((BLK, 2048), BF16),
            pltpu.VMEM((BLK + 16, 1408), BF16),
            pltpu.VMEM((16, 1408), BF16),
            pltpu.VMEM((8, 1408), F32),
            pltpu.VMEM((BLK, 768), BF16),
            pltpu.VMEM((4, OWN, 2048), F32),
            pltpu.VMEM((4, OWN, 2048), BF16),
            pltpu.VMEM((4, OWN, 2048), BF16),
            pltpu.VMEM((2, OWN, HALF), BF16),
            pltpu.VMEM((2, OWN, HALF), BF16),
            pltpu.VMEM((2, 2, OWN, HALF), BF16),
            pltpu.VMEM((2, 2, OWN, HALF), BF16),
            pltpu.SemaphoreType.DMA((112,)),
            pltpu.SemaphoreType.DMA((112,)),
            pltpu.SemaphoreType.DMA((2,)),
        ],
        compiler_params=pltpu.CompilerParams(
            collective_id=1, has_side_effects=True, vmem_limit_bytes=VMEM_ALL
        ),
        cost_estimate=pl.CostEstimate(flops=20_000_000_000, bytes_accessed=40_000_000, transcendentals=0),
    )(*operands)


def per_device(
    query_small,
    key_small,
    value_small,
    gates_small,
    query_large,
    key_large,
    value_large,
    gates_large,
    residual,
    mixer_small,
    mixer_large,
    mix_gain,
    value_weight,
    gate_weight,
    value_taps,
    gate_taps,
    down_weight,
    final_gain,
):
    return whole_layer(
        query_small,
        key_small,
        value_small,
        query_large,
        key_large,
        value_large,
        gates_small.T,
        gates_large.T,
        value_weight.T,
        gate_weight.T,
        down_weight,
        mixer_small,
        mixer_large,
        residual,
        mix_gain[None],
        final_gain[None],
        value_taps,
        gate_taps,
    )


def solution(mesh):
    split = Mesh(mesh.devices.reshape(mesh.shape["sp"], 4, 2), ("sp", "tp_0", "tp_1"))
    placed = (
        P("sp", TP),
        P("sp", TP),
        P("sp", TP),
        P("sp", TP),
        P("sp", TP),
        P("sp", TP),
        P("sp", TP),
        P("sp", TP),
        P(SP_TP, None),
        P(TP, None),
        P(TP, None),
        P(),
        P("sp", TP),
        P("sp", TP),
        P(None, TP),
        P(None, TP),
        P(TP, "sp"),
        P(),
    )
    return jax.shard_map(
        per_device, mesh=split, in_specs=placed, out_specs=P(SP_TP, None), check_vma=False
    )
```

```python
import functools

import jax
import jax.numpy as jnp
from jax import lax
from jax.experimental import pallas as pl
from jax.experimental.pallas import tpu as pltpu
from jax.sharding import Mesh
from jax.sharding import PartitionSpec as P

TP = ("tp_0", "tp_1")
SP_TP = ("sp", "tp_0", "tp_1")
LOG2E = 1.4426950408889634
residual_scale = 2.0**0.5
epsilon = 1e-05
MESH = pl.DeviceIdType.MESH
BLK = 768
EXTRA = 32
WROWS = 2112
UP = 1408
DOWN = 704
RQ = 384
F32 = jnp.float32
BF16 = jnp.bfloat16
VMEM_ALL = 67_000_000
OWN = 96
HALF = 1024
HALO_SEM = 111


def layer_kernel(
    qs_ref,
    ks_ref,
    vs_ref,
    ql_ref,
    kl_ref,
    vl_ref,
    gs_ref,
    gl_ref,
    vw_ref,
    gw_ref,
    down_ref,
    ms_ref,
    ml_ref,
    res_ref,
    mgain_ref,
    fgain_ref,
    vtaps_ref,
    gtaps_ref,
    out_ref,
    kvin,
    qin,
    kvbuf,
    qpair,
    qgate,
    qm,
    gq,
    gk,
    mst,
    lst,
    acc,
    sbuf,
    mbuf,
    pbuf,
    abuf,
    outv,
    wbuf,
    mixbuf,
    arrived,
    ybuf,
    mixed,
    both,
    halo,
    taps,
    hid,
    keep,
    sib_out,
    sib_in,
    far_out,
    far_in,
    near_out,
    near_in,
    ssem,
    rsem,
    lsem,
):
    sp = lax.axis_index("sp")
    y = lax.axis_index("tp_0")
    c = lax.axis_index("tp_1")
    z, x = sp // 4, sp % 4
    role = x // 2
    xr, xl = (x + 1) % 4, (x + 3) % 4
    zu, zd = (z + 1) % 4, (z + 3) % 4
    yu, yd = (y + 1) % 4, (y + 3) % 4
    xf, zf, yf = (x + 2) % 4, (z + 2) % 4, (y + 2) % 4
    mate = x + 1 - 2 * (x % 2)
    opp = 3 - x
    diag = opp + 1 - 2 * (opp % 2)
    pair_sp = 15 - sp
    tp = y * 2 + c

    def at(zz, xx):
        return (zz * 4 + xx, y, c)

    right, left = at(z, xr), at(z, xl)
    above, below = at(zu, x), at(zd, x)
    mate_dev, opp_dev = at(z, mate), at(z, opp)
    pair_dev = (pair_sp, y, c)
    y_up, y_down = (sp, yu, c), (sp, yd, c)
    sibling = (sp, y, 1 - c)
    after, before = ((sp + 1) % 16, y, c), ((sp + 15) % 16, y, c)

    barrier = pltpu.get_barrier_semaphore()
    greeted = [right, left, above, below, after, before]
    for d in range(8):
        t = (tp + d) % 8
        if d:
            greeted.append((sp, t // 2, t % 2))
        greeted.append((pair_sp, t // 2, t % 2))
    for dev in greeted:
        pl.semaphore_signal(barrier, inc=1, device_id=dev, device_id_type=MESH)

    lane = lax.broadcasted_iota(jnp.int32, (1, 128), 1)

    for r, (q_ref, k_ref, v_ref, g_ref) in enumerate(
        ((qs_ref, ks_ref, vs_ref, gs_ref), (ql_ref, kl_ref, vl_ref, gl_ref))
    ):
        kvin[r, 0:BLK, 0:128] = k_ref[...]
        kvin[r, 0:BLK, 128:256] = v_ref[...]
        qin[r] = q_ref[...]
        pieces = []
        for h in range(2 - r):
            left_over = g_ref[h : h + 1, :] * LOG2E
            for i in range(3):
                part = left_over.astype(BF16).astype(F32)
                left_over = left_over - part
                pieces += [part[:, p * 256 : (p + 1) * 256] for p in range(3)]
        pieces.append(jnp.zeros((EXTRA - len(pieces), 256), F32))
        kvin[r, BLK : BLK + EXTRA, :] = jnp.concatenate(pieces, axis=0).astype(BF16)

    def mix_rows(t, start=0, size=256):
        return mixbuf.at[pl.ds(pl.multiple_of(t * 256 + start, 128), size)]

    def up_block(b, start=0, size=UP):
        return wbuf.at[b, pl.ds(start, size)]

    def down_blocks(b, count=1, start=0, size=DOWN):
        return wbuf.at[pl.ds(b, count), pl.ds(UP + start, size)]

    wbuf[sp, 0:640, :] = vw_ref[0:640, :]
    wbuf[sp, 640:1280, :] = gw_ref[0:640, :]
    wbuf[sp, 1280:1344, :] = vw_ref[640:704, :]
    wbuf[sp, 1344:1408, :] = gw_ref[640:704, :]
    wbuf[sp, 1408:WROWS, :] = down_ref[...]
    for b in range(16):
        wbuf[b, WROWS : WROWS + 64, :] = jnp.zeros((64, 128), BF16)
    mixbuf[pl.ds(pl.multiple_of(tp * 256, 256), 128), :] = ms_ref[...]
    mixbuf[pl.ds(pl.multiple_of(tp * 256 + 128, 128), 128), :] = ml_ref[...]

    pl.semaphore_wait(barrier, len(greeted))

    sent = []
    counter = [0]
    incoming = {}

    def send(name, ends, sends=None, receives=None, now=None):
        k = counter[0]
        counter[0] += 1

        def copy(arriving):
            src, dst, dev, landing = ends()
            return pltpu.make_async_remote_copy(
                src_ref=landing if arriving else src,
                dst_ref=landing if arriving else dst,
                send_sem=ssem.at[k],
                recv_sem=rsem.at[k],
                device_id=dev,
                device_id_type=MESH,
            )

        def only(condition, act):
            act() if condition is None else pl.when(condition())(act)

        sent.append(lambda: only(sends, lambda: copy(False).wait_send()))
        incoming[name] = lambda: only(receives, lambda: copy(True).wait_recv())
        only(now or sends, lambda: copy(False).start())
        return lambda: copy(False).start()

    def take(*names):
        for name in names:
            incoming.pop(name)()

    cols = {"own": x, "mate": mate, "opp": opp, "diag": diag}

    send("x1m", lambda: (kvin.at[role], kvbuf.at[sp], mate_dev, kvbuf.at[z * 4 + mate]))
    send("x1o", lambda: (kvin.at[1 - role], kvbuf.at[sp], opp_dev, kvbuf.at[z * 4 + opp]))
    send("z1u_own", lambda: (kvin.at[role], kvbuf.at[sp], above, kvbuf.at[zd * 4 + x]))
    send("z1d_own", lambda: (kvin.at[role], kvbuf.at[sp], below, kvbuf.at[zu * 4 + x]), lambda: z < 3, lambda: z != 2)
    gate_part = pl.ds(BLK, EXTRA)
    send("qg", lambda: (kvin.at[1 - role, gate_part], qgate, pair_dev, qgate))
    send("q", lambda: (qin.at[1 - role], qpair, pair_dev, qpair))
    send("y1u", lambda: (mix_rows(tp), mix_rows(tp), y_up, mix_rows(yd * 2 + c)))
    send("y1d", lambda: (mix_rows(tp), mix_rows(tp), y_down, mix_rows(yu * 2 + c)))
    send("s0", lambda: (mix_rows(tp), mix_rows(tp), sibling, mix_rows(y * 2 + 1 - c)))

    def pass_x(tag, zz):
        def ends(dev, col):
            mine = up_block(zz * 4 + x)
            return mine, mine, dev, up_block(zz * 4 + col)

        send("wx1r" + tag, lambda: ends(right, xl))
        send("wx1l" + tag, lambda: ends(left, xr))

    own_kv = pltpu.make_async_copy(kvin.at[role], kvbuf.at[sp], lsem.at[0])
    own_kv.start()

    heads = 2 - role
    head_dim = 64 + 64 * role
    scale = jnp.where(role == 0, 0.125 * LOG2E, 128.0**-0.5 * LOG2E).astype(F32)

    def head_lanes(h):
        return (lane >= h * 64) & (lane < h * 64 + head_dim)

    def gate_row(rows, h, g):
        k, at_ = h * 9 + g // 2, slice((g % 2) * 128, (g % 2) * 128 + 128)
        return rows[k : k + 1, at_] + rows[k + 3 : k + 4, at_] + rows[k + 6 : k + 7, at_]

    same = lax.broadcasted_iota(jnp.int32, (128, 128), 0) == lax.broadcasted_iota(
        jnp.int32, (128, 128), 1
    )

    def load_queries(qi, queries, gate_block):
        rows = gate_block.astype(F32)
        for h in range(2):
            ones = jnp.where(head_lanes(h), 1.0, 0.0).astype(BF16)
            qm[qi, h] = queries * ones
            for g in range(BLK // 128):
                line = jnp.broadcast_to(gate_row(rows, h, g), (128, 128))
                column = jnp.sum(jnp.where(same, line, 0.0), axis=1, keepdims=True)
                gq[qi, h, g * 128 : (g + 1) * 128, :] = jnp.broadcast_to(column, (128, 128))

    load_queries(0, qin[role], kvin[role, BLK : BLK + EXTRA, :])
    mst[...] = jnp.full(mst.shape, -1e30, F32)
    lst[...] = jnp.zeros(lst.shape, F32)
    acc[...] = jnp.zeros(acc.shape, F32)

    def pass_z(tag):
        col = cols[tag]
        src = kvbuf.at[z * 4 + col]
        send("z1u_" + tag, lambda: (src, src, above, kvbuf.at[zd * 4 + col]))
        send("z1d_" + tag, lambda: (src, src, below, kvbuf.at[zu * 4 + col]), lambda: z < 3, lambda: z != 2)

    b_d, b_u, b_f = zd * 4 + x, zu * 4 + x, zf * 4 + x
    b_l, b_r, b_o = z * 4 + xl, z * 4 + xr, z * 4 + (x + 2) % 4
    dhalf = DOWN // 2
    take("x1o")
    send("x2", lambda: (kvbuf.at[z * 4 + opp], kvbuf.at[z * 4 + opp], mate_dev, kvbuf.at[z * 4 + diag]))
    pass_z("opp")
    take("x1m")
    pass_z("mate")
    send("wz1u", lambda: (up_block(sp), up_block(sp), above, up_block(b_d)))
    send("wz1d", lambda: (up_block(sp), up_block(sp), below, up_block(b_u)))
    send("bx1r", lambda: (down_blocks(sp), down_blocks(sp), right, down_blocks(b_l)))
    send("bx1l", lambda: (down_blocks(sp), down_blocks(sp), left, down_blocks(b_r)))
    pass_x("0", z)
    own_kv.wait()
    take("x2")
    pass_z("diag")
    take("z1u_own", "z1d_own")
    send(
        "z2u_own",
        lambda: (kvbuf.at[zd * 4 + x], kvbuf.at[zd * 4 + x], above, kvbuf.at[zf * 4 + x]),
        lambda: z >= 2,
        lambda: (z == 0) | (z == 3),
    )
    send(
        "z2x_own",
        lambda: (kvbuf.at[zu * 4 + x], kvbuf.at[zu * 4 + x], below, kvbuf.at[zf * 4 + x]),
        lambda: z == 3,
        lambda: z == 2,
    )
    take("bx1r", "bx1l")
    send(
        "bx2r",
        lambda: (down_blocks(b_l, 1, 0, dhalf), down_blocks(b_l, 1, 0, dhalf), right, down_blocks(b_o, 1, 0, dhalf)),
    )
    send(
        "bx2l",
        lambda: (down_blocks(b_r, 1, dhalf, dhalf), down_blocks(b_r, 1, dhalf, dhalf), left, down_blocks(b_o, 1, dhalf, dhalf)),
    )
    take("q", "qg")
    load_queries(1, qpair[...], qgate[...])

    def gate_rows(j):
        rows = kvbuf[j, BLK : BLK + EXTRA, :].astype(F32)
        for h in range(2):
            for g in range(BLK // 128):
                line = jnp.broadcast_to(gate_row(rows, h, g), (8, 128))
                gk[j * 2 + h, :, g * 128 : (g + 1) * 128] = line

    def scores(qi, j, h, sub, masked):
        rows = pl.ds(sub * RQ, RQ)
        span = (sub + 1) * RQ if masked else BLK
        raw = lax.dot_general(
            qm[qi, h, rows, :],
            kvbuf[j, 0:span, 0:128],
            (((1,), (1,)), ((), ())),
            preferred_element_type=F32,
        )
        gate = gk[j * 2 + h, 0:1, 0:span]
        parts = []
        for g in range(span // 128):
            part = raw[:, g * 128 : (g + 1) * 128] * scale - gate[:, g * 128 : (g + 1) * 128]
            if masked and (g + 1) * 128 > sub * RQ:
                col = lax.broadcasted_iota(jnp.int32, (RQ, 128), 1) + (g * 128 - sub * RQ)
                row = lax.broadcasted_iota(jnp.int32, (RQ, 128), 0)
                part = jnp.where(col <= row, part, -1e30)
            parts.append(part)
        return parts, functools.reduce(jnp.maximum, parts)

    def soften(parts, peak, qi, j, h, sub):
        rows = pl.ds(sub * RQ, RQ)
        peak = jnp.max(peak, axis=1, keepdims=True)
        g_here = gq[qi, h, rows, :]
        old = mst[qi, h, rows, :]
        new = jnp.maximum(old, peak + g_here)
        alpha = jnp.exp2(old - new)
        shift = new - g_here
        weights_ = [jnp.exp2(part - shift) for part in parts]
        mst[qi, h, rows, :] = new
        lst[qi, h, rows, :] = lst[qi, h, rows, :] * alpha + functools.reduce(jnp.add, weights_)
        return jnp.concatenate([a.astype(BF16) for a in weights_], axis=1), alpha

    def hold(parts, peak):
        for g, part in enumerate(parts):
            sbuf[:, g * 128 : (g + 1) * 128] = part
        mbuf[...] = peak

    def held():
        return [sbuf[:, g * 128 : (g + 1) * 128] for g in range(BLK // 128)], mbuf[...]

    def spread(w, alpha, qi, j, h, sub, masked):
        rows = pl.ds(sub * RQ, RQ)
        span = (sub + 1) * RQ if masked else BLK
        mask = head_lanes(h)
        v = kvbuf[j, 0:span, 128:256] * jnp.where(mask, 1.0, 0.0).astype(BF16)
        update = jnp.dot(w, v, preferred_element_type=F32)
        acc[qi, rows, :] = acc[qi, rows, :] * jnp.where(mask, alpha, 1.0) + update

    def tiles(qi, j, h, masked):
        count = BLK // RQ
        ahead = scores(qi, j, h, 0, masked)
        for sub in range(count):
            here = ahead
            ahead = scores(qi, j, h, sub + 1, masked) if sub + 1 < count else None
            w, alpha = soften(*here, qi, j, h, sub)
            spread(w, alpha, qi, j, h, sub, masked)

    blocks_of = (sp, pair_sp)

    def attend(step):
        row = jnp.where(step == 0, z, jnp.where(step == 2, zd, jnp.where(step == 3, zu, zf)))
        second = step == 1
        none = 99
        slots = (
            jnp.where(second, zd * 4 + x, row * 4 + mate),
            jnp.where(second, zu * 4 + x, row * 4 + opp),
            jnp.where(second, none, row * 4 + diag),
            jnp.where(step == 0, sp, jnp.where(step == 3, zf * 4 + x, none)),
        )
        for j in slots:
            pl.when(j <= jnp.maximum(sp, pair_sp))(functools.partial(gate_rows, j))

        found, count = [], 0
        for qi in range(2):
            for j in slots:
                flag = jnp.where(j < blocks_of[qi], 1, 0)
                found.append((qi, j, flag, count))
                count = count + flag
        units = count * heads

        def place(u):
            v = jnp.clip(u, 0, units - 1)
            k = v // heads
            hits = [(qi, j, jnp.where(before_ == k, flag, 0)) for qi, j, flag, before_ in found]
            qi = sum(hit * qi for qi, _, hit in hits)
            j = sum(hit * j for _, j, hit in hits)
            return jnp.where(u == v, qi, 2), j, v % heads

        def two_units(i, _):
            spread(pbuf[...], abuf[...], *place(2 * i - 1), 1, False)
            here = held()
            for t in range(4):
                now = place(2 * i + t // 2)
                ahead = scores(*place(2 * i + (t + 1) // 2), (t + 1) % 2, False)
                w, alpha = soften(*here, *now, t % 2)
                if t < 3:
                    spread(w, alpha, *now, t % 2, False)
                here = ahead
            hold(*here)
            pbuf[...] = w
            abuf[...] = alpha
            return 0

        @pl.when(units > 0)
        def _():
            hold(*scores(*place(0), 0, False))
            steps = (units + 1) // 2
            lax.fori_loop(0, steps, two_units, 0)
            spread(pbuf[...], abuf[...], *place(2 * steps - 1), 1, False)

        @pl.when((step == 0) | (step == 2 + z % 2))
        def _():
            qi = jnp.where(step == 0, 0, 1)

            def for_head(h, _):
                tiles(qi, jnp.where(step == 0, sp, pair_sp), h, True)
                return 0

            lax.fori_loop(0, heads, for_head, 0)

    def pass_on(tag, name, from_z, dev, landing_z, sends, receives):
        col = cols[tag]

        def ends():
            src = kvbuf.at[from_z * 4 + col]
            return src, src, dev, kvbuf.at[landing_z * 4 + col]

        send(name + tag, ends, sends, receives)

    m_d, m_u, m_f = yd * 2 + c, yu * 2 + c, yf * 2 + c
    s_d, s_u, s_f = yd * 2 + 1 - c, yu * 2 + 1 - c, yf * 2 + 1 - c

    def pass_x2(tag, zz, name, col, dev, start=0, size=UP, now=None):
        def ends():
            src = up_block(zz * 4 + col, start, size)
            return src, src, dev, up_block(zz * 4 + xf, start, size)

        return send(name + tag, ends, now=now)

    uhalf = UP // 2

    def both_ways(tag, zz):
        pass_x2(tag, zz, "wx2r", xl, right, 0, uhalf)
        pass_x2(tag, zz, "wx2l", xr, left, uhalf, uhalf)

    def down_pair(name, zz, first, dev, landing):
        def ends():
            src = down_blocks(zz * 4 + first, 2)
            return src, src, dev, down_blocks(landing * 4 + first, 2)

        send(name, ends)

    def one_step(step, _):
        attend(step)

        @pl.when(step == 1)
        def _():
            take("wz1u", "wz1d")
            send("wz2u", lambda: (up_block(b_d, 0, uhalf), up_block(b_d, 0, uhalf), above, up_block(b_f, 0, uhalf)))
            send("wz2d", lambda: (up_block(b_u, uhalf, uhalf), up_block(b_u, uhalf, uhalf), below, up_block(b_f, uhalf, uhalf)))
            pass_x("d", zd)
            pass_x("u", zu)
            take("y1u", "y1d")
            send("y2u", lambda: (mix_rows(m_d, 0, 128), mix_rows(m_d, 0, 128), y_up, mix_rows(m_f, 0, 128)))
            send("y2d", lambda: (mix_rows(m_u, 128, 128), mix_rows(m_u, 128, 128), y_down, mix_rows(m_f, 128, 128)))
            send("s1", lambda: (mix_rows(m_d), mix_rows(m_d), sibling, mix_rows(s_d)))
            send("s2", lambda: (mix_rows(m_u), mix_rows(m_u), sibling, mix_rows(s_u)))
            take("z1u_mate", "z1d_mate")
            pass_on("mate", "z2u_", zd, above, zf, lambda: z >= 1, lambda: z != 1)
            take("z1u_opp", "z1d_opp", "z1u_diag", "z1d_diag")
            pass_on("opp", "z2d_", zu, below, zf, lambda: z != 2, lambda: z != 1)
            pass_on("diag", "z2d_", zu, below, zf, lambda: z != 2, lambda: z != 1)
            take("wx1r0", "wx1l0")
            both_ways("0", z)

        @pl.when(step == 2)
        def _():
            take("z2u_own", "z2x_own")
            take("wz2u", "wz2d")
            pass_x("f", zf)

        @pl.when(step == 2)
        def _():
            take("wx1rd", "wx1ld", "wx1ru", "wx1lu")
            both_ways("d", zd)
            both_ways("u", zu)

        @pl.when(step == 3)
        def _():
            take("y2u", "y2d")
            send("s3", lambda: (mix_rows(m_f), mix_rows(m_f), sibling, mix_rows(s_f)))
            take("z2u_mate", "z2d_opp", "z2d_diag")
            take("bx2r", "bx2l")
            down_pair("bz1u", z, 0, above, zd)
            down_pair("bz1d", z, 2, below, zu)

        return 0

    lax.fori_loop(0, 5, one_step, 0)

    keep0 = head_lanes(0)
    for qi in (1, 0):
        l0 = jnp.sum(lst[qi, 0], axis=1, keepdims=True)
        l1 = jnp.sum(lst[qi, 1], axis=1, keepdims=True)
        outv[qi] = (acc[qi] / jnp.where(keep0, l0, l1)).astype(BF16)

    def own_rows(t):
        return pl.ds(pl.multiple_of(t * OWN, 32), OWN)

    slot = tp * 2 + role

    def send_out(d):
        t, s = (tp + d) % 8, (tp + 8 - d) % 8
        dst = (t // 2, t % 2)
        send(
            "p%d" % d,
            lambda: (outv.at[1, own_rows(t)], arrived.at[slot], (pair_sp, *dst), arrived.at[s * 2 + 1 - role]),
        )
        if d:
            send(
                "a%d" % d,
                lambda: (outv.at[0, own_rows(t)], arrived.at[slot], (sp, *dst), arrived.at[s * 2 + role]),
            )

    for d in range(8):
        send_out(d)
    far_waits = [incoming.pop("wx1rf"), incoming.pop("wx1lf")]
    is_large = lambda: role == 1

    @pl.when(role == 1)
    def _():
        for wait in far_waits:
            wait()

    far_sends = [
        pass_x2("f", zf, "wx2r", xl, right, 0, uhalf, is_large),
        pass_x2("f", zf, "wx2l", xr, left, uhalf, uhalf, is_large),
    ]
    arrived[slot] = outv[0, own_rows(tp), :]
    take("s0", "s1", "s2", "s3")
    for d in range(8):
        take("p%d" % d)
        if d:
            take("a%d" % d)

    @pl.when(role == 0)
    def _():
        for wait in far_waits:
            wait()
        for start in far_sends:
            start()

    take("bz1u", "bz1d")
    down_pair("bz2u", zd, 0, above, zf)
    down_pair("bz2d", zu, 2, below, zf)
    down_pair("bz3u", z, 2, above, zd)
    down_pair("bz3d", z, 0, below, zu)

    def project(i, _):
        col = pl.ds(pl.multiple_of(i * 1024, 1024), 1024)
        lhs = jnp.concatenate([arrived[s] for s in range(16)], axis=1)
        part = jnp.dot(lhs, mixbuf[:, col], preferred_element_type=F32)
        ybuf[:, col] = residual_scale * res_ref[:, col].astype(F32) + part
        return 0

    lax.fori_loop(0, 2, project, 0)

    def norm(values, gain):
        center = jnp.mean(values, axis=1, keepdims=True)
        off = values - center
        spread = jnp.mean(jnp.square(off), axis=1, keepdims=True)
        return off * lax.rsqrt(spread + epsilon) * gain

    def first_norm(i, _):
        r = pl.ds(pl.multiple_of(i * 48, 48), 48)
        t = pl.ds(pl.multiple_of(tp * OWN + i * 48, 48), 48)
        mixed[t, :] = norm(ybuf[r, :], mgain_ref[...]).astype(BF16)
        return 0

    lax.fori_loop(0, OWN // 48, first_norm, 0)

    def rows_of(t, start=0, size=OWN):
        return mixed.at[pl.ds(pl.multiple_of(t * OWN + start, 16), size)]

    send("gu", lambda: (rows_of(tp), rows_of(tp), y_up, rows_of(m_d)))
    send("gd", lambda: (rows_of(tp), rows_of(tp), y_down, rows_of(m_u)))
    send("gs", lambda: (rows_of(tp), rows_of(tp), sibling, rows_of(y * 2 + 1 - c)))
    take("wx2r0", "wx2l0", "wx2rd", "wx2ld", "wx2ru", "wx2lu", "wx2rf", "wx2lf")

    def up_group(*chips):
        def some(start, width):
            cols_ = pl.ds(start, width)
            rhs = jnp.concatenate([wbuf[b, cols_, :] for b in range(16)], axis=1)
            lhs = [mixed[pl.ds(pl.multiple_of(yy * 192, 64), 192), :] for yy in chips]
            part = lax.dot_general(
                jnp.concatenate(lhs, axis=0), rhs, (((1,), (1,)), ((), ())), preferred_element_type=F32
            ).astype(BF16)
            for k, yy in enumerate(chips):
                into = pl.ds(pl.multiple_of(yy * 192 + 16, 16), 192)
                both[into, cols_] = part[k * 192 : (k + 1) * 192]

        some(0, UP)

    def send_halo():
        pltpu.make_async_remote_copy(
            src_ref=both.at[pl.ds(BLK, 16)],
            dst_ref=halo,
            send_sem=ssem.at[HALO_SEM],
            recv_sem=rsem.at[HALO_SEM],
            device_id=after,
            device_id_type=MESH,
        ).start()

    def wait_halo(which):
        copy = pltpu.make_async_remote_copy(
            src_ref=both.at[pl.ds(BLK, 16)],
            dst_ref=halo,
            send_sem=ssem.at[HALO_SEM],
            recv_sem=rsem.at[HALO_SEM],
            device_id=after,
            device_id_type=MESH,
        )
        copy.wait_recv() if which else copy.wait_send()

    taps[0:3, 0:640] = vtaps_ref[:, 0:640]
    taps[0:3, 640:1280] = gtaps_ref[:, 0:640]
    taps[0:3, 1280:1408] = jnp.concatenate([vtaps_ref[:, 640:704], gtaps_ref[:, 640:704]], axis=1)

    def filtered(a, lanes_):
        n = a.shape[0] - 16
        return (
            taps[0:1, lanes_] * a[14 : 14 + n]
            + taps[1:2, lanes_] * a[15 : 15 + n]
            + taps[2:3, lanes_] * a[16 : 16 + n]
        )

    def hidden_rows(i):
        src = pl.ds(pl.multiple_of(i * OWN, 32), OWN + 16)
        dst = pl.ds(pl.multiple_of(i * OWN, 32), OWN)
        for g in range(6):
            if g < 5:
                at_v, at_g = slice(g * 128, (g + 1) * 128), slice(640 + g * 128, 768 + g * 128)
                fv = filtered(both[src, at_v].astype(F32), at_v)
                fg = filtered(both[src, at_g].astype(F32), at_g)
            else:
                last = slice(1280, 1408)
                fv = filtered(both[src, last].astype(F32), last)
                fg = pltpu.roll(fv, 64, 1)
            value = fg / (1.0 + jnp.exp(-fg)) * fv
            if g == 5:
                value = jnp.where(lane < 64, value, 0.0)
            hid[dst, g * 128 : (g + 1) * 128] = value.astype(BF16)

    def hidden_group(yy):
        @pl.when(yy == 0)
        def _():
            wait_halo(True)
            both[0:16, :] = jnp.where(sp == 0, 0.0, halo[...].astype(F32)).astype(BF16)

        def chunk(i, _):
            hidden_rows(yy * 2 + i)
            return 0

        lax.fori_loop(0, 2, chunk, 0)

    def down_group(g, yy):
        mine = hid[pl.ds(pl.multiple_of(yy * 192 + c * OWN, 32), OWN), :]
        other = hid[pl.ds(pl.multiple_of(yy * 192 + (1 - c) * OWN, 32), OWN), :]
        lhs = jnp.concatenate([mine, other], axis=0)

        def some(i, _):
            col = pl.ds(pl.multiple_of(i * 1024, 1024), 1024)
            rhs = jnp.concatenate([wbuf[8 * i + k, 1408 : WROWS + 64, :] for k in range(8)], axis=1)
            part = jnp.dot(lhs, rhs, preferred_element_type=F32)
            keep[g, :, col] = part[:OWN]
            sib_out[g, :, col] = part[OWN:].astype(BF16)
            return 0

        lax.fori_loop(0, 2, some, 0)

    def send_sib(g):
        send("r%d" % g, lambda: (sib_out.at[g], sib_in.at[g], sibling, sib_in.at[g]))

    def pair_sum(g, lo, hi):
        return keep[g, :, lo:hi] + sib_in[g, :, lo:hi].astype(F32)

    def near(k, h):
        send(
            "n%d%d" % (k, h),
            lambda: (near_out.at[k, h], near_in.at[k, h], (y_up, y_down)[k], near_in.at[k, h]),
        )

    take("gs")
    up_group(y)
    pl.when(y == 3)(send_halo)
    take("gu", "gd")
    send("g2u", lambda: (rows_of(m_d, 0, 48), rows_of(m_d, 0, 48), y_up, rows_of(m_f, 0, 48)))
    send("g2d", lambda: (rows_of(m_u, 48, 48), rows_of(m_u, 48, 48), y_down, rows_of(m_f, 48, 48)))
    send("gs1", lambda: (rows_of(m_d), rows_of(m_d), sibling, rows_of(s_d)))
    send("gs2", lambda: (rows_of(m_u), rows_of(m_u), sibling, rows_of(s_u)))
    take("gs1", "gs2")
    up_group(yd, yu)
    pl.when((yd == 3) | (yu == 3))(send_halo)
    take("g2u", "g2d")
    send("gs3", lambda: (rows_of(m_f), rows_of(m_f), sibling, rows_of(s_f)))
    take("bz2u", "bz2d", "bz3u", "bz3d")
    hidden_group(yu)
    down_group(2, yu)
    send_sib(2)
    take("gs3")
    up_group(yf)
    pl.when(yf == 3)(send_halo)
    take("r2")
    near_out[0, 1] = pair_sum(2, HALF, 2 * HALF).astype(BF16)
    near(0, 1)
    hidden_group(yf)
    down_group(0, yf)
    send_sib(0)
    hidden_group(yd)
    take("r0")
    far_out[0] = pair_sum(0, 0, HALF).astype(BF16)
    far_out[1] = pair_sum(0, HALF, 2 * HALF).astype(BF16)
    send("fu", lambda: (far_out.at[0], far_in.at[0], y_up, far_in.at[0]))
    send("fd", lambda: (far_out.at[1], far_in.at[1], y_down, far_in.at[1]))
    down_group(1, yd)
    send_sib(1)
    hidden_group(y)
    take("r1")
    near_out[1, 0] = pair_sum(1, 0, HALF).astype(BF16)
    near(1, 0)
    down_group(3, y)
    send_sib(3)

    take("fu")
    near_out[0, 0] = (pair_sum(2, 0, HALF) + far_in[0].astype(F32)).astype(BF16)
    near(0, 0)
    take("fd")
    near_out[1, 1] = (pair_sum(1, HALF, 2 * HALF) + far_in[1].astype(F32)).astype(BF16)
    near(1, 1)
    take("r3", "n00", "n01", "n10", "n11")

    def last_norm(i, _):
        r = pl.ds(pl.multiple_of(i * 48, 48), 48)
        t = pl.ds(pl.multiple_of(tp * OWN + i * 48, 48), 48)
        far = [near_in[0, h, r, :].astype(F32) + near_in[1, h, r, :].astype(F32) for h in range(2)]
        ffn = keep[3, r, :] + sib_in[3, r, :].astype(F32) + jnp.concatenate(far, axis=1)
        whole = residual_scale * mixed[t, :].astype(F32) + ffn
        out_ref[r, :] = norm(whole, fgain_ref[...]).astype(BF16)
        return 0

    lax.fori_loop(0, OWN // 48, last_norm, 0)
    wait_halo(False)
    for wait in sent:
        wait()


def whole_layer(*operands):
    vmem = pl.BlockSpec(memory_space=pltpu.VMEM)
    return pl.pallas_call(
        layer_kernel,
        out_shape=jax.ShapeDtypeStruct((OWN, 2048), BF16),
        in_specs=[vmem] * len(operands),
        out_specs=vmem,
        scratch_shapes=[
            pltpu.VMEM((2, BLK + EXTRA, 256), BF16),
            pltpu.VMEM((2, BLK, 128), BF16),
            pltpu.VMEM((16, BLK + EXTRA, 256), BF16),
            pltpu.VMEM((BLK, 128), BF16),
            pltpu.VMEM((EXTRA, 256), BF16),
            pltpu.VMEM((3, 2, BLK, 128), BF16),
            pltpu.VMEM((3, 2, BLK, 128), F32),
            pltpu.VMEM((32, 8, BLK), F32),
            pltpu.VMEM((3, 2, BLK, 128), F32),
            pltpu.VMEM((3, 2, BLK, 128), F32),
            pltpu.VMEM((3, BLK, 128), F32),
            pltpu.VMEM((RQ, BLK), F32),
            pltpu.VMEM((RQ, 128), F32),
            pltpu.VMEM((RQ, BLK), BF16),
            pltpu.VMEM((RQ, 128), F32),
            pltpu.VMEM((2, BLK, 128), BF16),
            pltpu.VMEM((16, WROWS + 64, 128), BF16),
            pltpu.VMEM((2048, 2048), BF16),
            pltpu.VMEM((16, OWN, 128), BF16),
            pltpu.VMEM((OWN, 2048), F32),
            pltpu.VMEM((BLK, 2048), BF16),
            pltpu.VMEM((BLK + 16, 1408), BF16),
            pltpu.VMEM((16, 1408), BF16),
            pltpu.VMEM((8, 1408), F32),
            pltpu.VMEM((BLK, 768), BF16),
            pltpu.VMEM((4, OWN, 2048), F32),
            pltpu.VMEM((4, OWN, 2048), BF16),
            pltpu.VMEM((4, OWN, 2048), BF16),
            pltpu.VMEM((2, OWN, HALF), BF16),
            pltpu.VMEM((2, OWN, HALF), BF16),
            pltpu.VMEM((2, 2, OWN, HALF), BF16),
            pltpu.VMEM((2, 2, OWN, HALF), BF16),
            pltpu.SemaphoreType.DMA((112,)),
            pltpu.SemaphoreType.DMA((112,)),
            pltpu.SemaphoreType.DMA((2,)),
        ],
        compiler_params=pltpu.CompilerParams(
            collective_id=1, has_side_effects=True, vmem_limit_bytes=VMEM_ALL
        ),
        cost_estimate=pl.CostEstimate(flops=20_000_000_000, bytes_accessed=40_000_000, transcendentals=0),
    )(*operands)


def per_device(
    query_small,
    key_small,
    value_small,
    gates_small,
    query_large,
    key_large,
    value_large,
    gates_large,
    residual,
    mixer_small,
    mixer_large,
    mix_gain,
    value_weight,
    gate_weight,
    value_taps,
    gate_taps,
    down_weight,
    final_gain,
):
    return whole_layer(
        query_small,
        key_small,
        value_small,
        query_large,
        key_large,
        value_large,
        gates_small.T,
        gates_large.T,
        value_weight.T,
        gate_weight.T,
        down_weight,
        mixer_small,
        mixer_large,
        residual,
        mix_gain[None],
        final_gain[None],
        value_taps,
        gate_taps,
    )


def solution(mesh):
    split = Mesh(mesh.devices.reshape(mesh.shape["sp"], 4, 2), ("sp", "tp_0", "tp_1"))
    placed = (
        P("sp", TP),
        P("sp", TP),
        P("sp", TP),
        P("sp", TP),
        P("sp", TP),
        P("sp", TP),
        P("sp", TP),
        P("sp", TP),
        P(SP_TP, None),
        P(TP, None),
        P(TP, None),
        P(),
        P("sp", TP),
        P("sp", TP),
        P(None, TP),
        P(None, TP),
        P(TP, "sp"),
        P(),
    )
    return jax.shard_map(
        per_device, mesh=split, in_specs=placed, out_specs=P(SP_TP, None), check_vma=False
    )
```

```python
import functools

import jax
import jax.numpy as jnp
from jax import lax
from jax.experimental import pallas as pl
from jax.experimental.pallas import tpu as pltpu
from jax.sharding import Mesh
from jax.sharding import PartitionSpec as P

TP = ("tp_0", "tp_1")
SP_TP = ("sp", "tp_0", "tp_1")
LOG2E = 1.4426950408889634
residual_scale = 2.0**0.5
epsilon = 1e-05
MESH = pl.DeviceIdType.MESH
BLK = 768
EXTRA = 32
WROWS = 2112
UP = 1408
DOWN = 704
RQ = 384
F32 = jnp.float32
BF16 = jnp.bfloat16
VMEM_ALL = 67_000_000
OWN = 96
HALF = 1024
HALO_SEM = 111


def layer_kernel(
    qs_ref,
    ks_ref,
    vs_ref,
    ql_ref,
    kl_ref,
    vl_ref,
    gs_ref,
    gl_ref,
    vw_ref,
    gw_ref,
    down_ref,
    ms_ref,
    ml_ref,
    res_ref,
    mgain_ref,
    fgain_ref,
    vtaps_ref,
    gtaps_ref,
    out_ref,
    kvin,
    qin,
    kvbuf,
    qpair,
    qgate,
    qm,
    gq,
    gk,
    mst,
    lst,
    acc,
    sbuf,
    mbuf,
    pbuf,
    abuf,
    outv,
    wbuf,
    mixbuf,
    arrived,
    ybuf,
    mixed,
    both,
    halo,
    taps,
    hid,
    keep,
    sib_out,
    sib_in,
    far_out,
    far_in,
    near_out,
    near_in,
    ssem,
    rsem,
    lsem,
):
    sp = lax.axis_index("sp")
    y = lax.axis_index("tp_0")
    c = lax.axis_index("tp_1")
    z, x = sp // 4, sp % 4
    role = x // 2
    xr, xl = (x + 1) % 4, (x + 3) % 4
    zu, zd = (z + 1) % 4, (z + 3) % 4
    yu, yd = (y + 1) % 4, (y + 3) % 4
    xf, zf, yf = (x + 2) % 4, (z + 2) % 4, (y + 2) % 4
    mate = x + 1 - 2 * (x % 2)
    opp = 3 - x
    diag = opp + 1 - 2 * (opp % 2)
    pair_sp = 15 - sp
    tp = y * 2 + c

    def at(zz, xx):
        return (zz * 4 + xx, y, c)

    right, left = at(z, xr), at(z, xl)
    above, below = at(zu, x), at(zd, x)
    mate_dev, opp_dev = at(z, mate), at(z, opp)
    pair_dev = (pair_sp, y, c)
    y_up, y_down = (sp, yu, c), (sp, yd, c)
    sibling = (sp, y, 1 - c)
    after, before = ((sp + 1) % 16, y, c), ((sp + 15) % 16, y, c)

    barrier = pltpu.get_barrier_semaphore()
    greeted = [right, left, above, below, after, before]
    for d in range(8):
        t = (tp + d) % 8
        if d:
            greeted.append((sp, t // 2, t % 2))
        greeted.append((pair_sp, t // 2, t % 2))
    for dev in greeted:
        pl.semaphore_signal(barrier, inc=1, device_id=dev, device_id_type=MESH)

    lane = lax.broadcasted_iota(jnp.int32, (1, 128), 1)

    for r, (q_ref, k_ref, v_ref, g_ref) in enumerate(
        ((qs_ref, ks_ref, vs_ref, gs_ref), (ql_ref, kl_ref, vl_ref, gl_ref))
    ):
        kvin[r, 0:BLK, 0:128] = k_ref[...]
        kvin[r, 0:BLK, 128:256] = v_ref[...]
        qin[r] = q_ref[...]
        pieces = []
        for h in range(2 - r):
            left_over = g_ref[h : h + 1, :] * LOG2E
            for i in range(3):
                part = left_over.astype(BF16).astype(F32)
                left_over = left_over - part
                pieces += [part[:, p * 256 : (p + 1) * 256] for p in range(3)]
        pieces.append(jnp.zeros((EXTRA - len(pieces), 256), F32))
        kvin[r, BLK : BLK + EXTRA, :] = jnp.concatenate(pieces, axis=0).astype(BF16)

    def mix_rows(t, start=0, size=256):
        return mixbuf.at[pl.ds(pl.multiple_of(t * 256 + start, 128), size)]

    def up_block(b, start=0, size=UP):
        return wbuf.at[b, pl.ds(start, size)]

    def down_blocks(b, count=1, start=0, size=DOWN):
        return wbuf.at[pl.ds(b, count), pl.ds(UP + start, size)]

    wbuf[sp, 0:640, :] = vw_ref[0:640, :]
    wbuf[sp, 640:1280, :] = gw_ref[0:640, :]
    wbuf[sp, 1280:1344, :] = vw_ref[640:704, :]
    wbuf[sp, 1344:1408, :] = gw_ref[640:704, :]
    wbuf[sp, 1408:WROWS, :] = down_ref[...]
    for b in range(16):
        wbuf[b, WROWS : WROWS + 64, :] = jnp.zeros((64, 128), BF16)
    mixbuf[pl.ds(pl.multiple_of(tp * 256, 256), 128), :] = ms_ref[...]
    mixbuf[pl.ds(pl.multiple_of(tp * 256 + 128, 128), 128), :] = ml_ref[...]

    pl.semaphore_wait(barrier, len(greeted))

    sent = []
    counter = [0]
    incoming = {}

    def send(name, ends, sends=None, receives=None, now=None):
        k = counter[0]
        counter[0] += 1

        def copy(arriving):
            src, dst, dev, landing = ends()
            return pltpu.make_async_remote_copy(
                src_ref=landing if arriving else src,
                dst_ref=landing if arriving else dst,
                send_sem=ssem.at[k],
                recv_sem=rsem.at[k],
                device_id=dev,
                device_id_type=MESH,
            )

        def only(condition, act):
            act() if condition is None else pl.when(condition())(act)

        sent.append(lambda: only(sends, lambda: copy(False).wait_send()))
        incoming[name] = lambda: only(receives, lambda: copy(True).wait_recv())
        only(now or sends, lambda: copy(False).start())
        return lambda: copy(False).start()

    def take(*names):
        for name in names:
            incoming.pop(name)()

    cols = {"own": x, "mate": mate, "opp": opp, "diag": diag}

    send("x1m", lambda: (kvin.at[role], kvbuf.at[sp], mate_dev, kvbuf.at[z * 4 + mate]))
    send("x1o", lambda: (kvin.at[1 - role], kvbuf.at[sp], opp_dev, kvbuf.at[z * 4 + opp]))
    send("z1u_own", lambda: (kvin.at[role], kvbuf.at[sp], above, kvbuf.at[zd * 4 + x]))
    send("z1d_own", lambda: (kvin.at[role], kvbuf.at[sp], below, kvbuf.at[zu * 4 + x]), lambda: z < 3, lambda: z != 2)
    gate_part = pl.ds(BLK, EXTRA)
    send("qg", lambda: (kvin.at[1 - role, gate_part], qgate, pair_dev, qgate))
    send("q", lambda: (qin.at[1 - role], qpair, pair_dev, qpair))
    send("y1u", lambda: (mix_rows(tp), mix_rows(tp), y_up, mix_rows(yd * 2 + c)))
    send("y1d", lambda: (mix_rows(tp), mix_rows(tp), y_down, mix_rows(yu * 2 + c)))
    send("s0", lambda: (mix_rows(tp), mix_rows(tp), sibling, mix_rows(y * 2 + 1 - c)))

    def pass_x(tag, zz):
        def ends(dev, col):
            mine = up_block(zz * 4 + x)
            return mine, mine, dev, up_block(zz * 4 + col)

        send("wx1r" + tag, lambda: ends(right, xl))
        send("wx1l" + tag, lambda: ends(left, xr))

    own_kv = pltpu.make_async_copy(kvin.at[role], kvbuf.at[sp], lsem.at[0])
    own_kv.start()

    heads = 2 - role
    head_dim = 64 + 64 * role
    scale = jnp.where(role == 0, 0.125 * LOG2E, 128.0**-0.5 * LOG2E).astype(F32)

    def head_lanes(h):
        return (lane >= h * 64) & (lane < h * 64 + head_dim)

    def gate_row(rows, h, g):
        k, at_ = h * 9 + g // 2, slice((g % 2) * 128, (g % 2) * 128 + 128)
        return rows[k : k + 1, at_] + rows[k + 3 : k + 4, at_] + rows[k + 6 : k + 7, at_]

    same = lax.broadcasted_iota(jnp.int32, (128, 128), 0) == lax.broadcasted_iota(
        jnp.int32, (128, 128), 1
    )

    def load_queries(qi, queries, gate_block):
        rows = gate_block.astype(F32)
        for h in range(2):
            ones = jnp.where(head_lanes(h), 1.0, 0.0).astype(BF16)
            qm[qi, h] = queries * ones
            for g in range(BLK // 128):
                line = jnp.broadcast_to(gate_row(rows, h, g), (128, 128))
                column = jnp.sum(jnp.where(same, line, 0.0), axis=1, keepdims=True)
                gq[qi, h, g * 128 : (g + 1) * 128, :] = jnp.broadcast_to(column, (128, 128))

    load_queries(0, qin[role], kvin[role, BLK : BLK + EXTRA, :])
    mst[...] = jnp.full(mst.shape, -1e30, F32)
    lst[...] = jnp.zeros(lst.shape, F32)
    acc[...] = jnp.zeros(acc.shape, F32)

    def pass_z(tag):
        col = cols[tag]
        src = kvbuf.at[z * 4 + col]
        send("z1u_" + tag, lambda: (src, src, above, kvbuf.at[zd * 4 + col]))
        send("z1d_" + tag, lambda: (src, src, below, kvbuf.at[zu * 4 + col]), lambda: z < 3, lambda: z != 2)

    b_d, b_u, b_f = zd * 4 + x, zu * 4 + x, zf * 4 + x
    b_l, b_r, b_o = z * 4 + xl, z * 4 + xr, z * 4 + (x + 2) % 4
    dhalf = DOWN // 2
    take("x1o")
    send("x2", lambda: (kvbuf.at[z * 4 + opp], kvbuf.at[z * 4 + opp], mate_dev, kvbuf.at[z * 4 + diag]))
    pass_z("opp")
    take("x1m")
    pass_z("mate")
    send("wz1u", lambda: (up_block(sp), up_block(sp), above, up_block(b_d)))
    send("wz1d", lambda: (up_block(sp), up_block(sp), below, up_block(b_u)))
    send("bx1r", lambda: (down_blocks(sp), down_blocks(sp), right, down_blocks(b_l)))
    send("bx1l", lambda: (down_blocks(sp), down_blocks(sp), left, down_blocks(b_r)))
    pass_x("0", z)
    own_kv.wait()
    take("x2")
    pass_z("diag")
    take("z1u_own", "z1d_own")
    send(
        "z2u_own",
        lambda: (kvbuf.at[zd * 4 + x], kvbuf.at[zd * 4 + x], above, kvbuf.at[zf * 4 + x]),
        lambda: z >= 2,
        lambda: (z == 0) | (z == 3),
    )
    send(
        "z2x_own",
        lambda: (kvbuf.at[zu * 4 + x], kvbuf.at[zu * 4 + x], below, kvbuf.at[zf * 4 + x]),
        lambda: z == 3,
        lambda: z == 2,
    )
    take("bx1r", "bx1l")
    send(
        "bx2r",
        lambda: (down_blocks(b_l, 1, 0, dhalf), down_blocks(b_l, 1, 0, dhalf), right, down_blocks(b_o, 1, 0, dhalf)),
    )
    send(
        "bx2l",
        lambda: (down_blocks(b_r, 1, dhalf, dhalf), down_blocks(b_r, 1, dhalf, dhalf), left, down_blocks(b_o, 1, dhalf, dhalf)),
    )
    take("q", "qg")
    load_queries(1, qpair[...], qgate[...])

    def gate_rows(j):
        rows = kvbuf[j, BLK : BLK + EXTRA, :].astype(F32)
        for h in range(2):
            for g in range(BLK // 128):
                line = jnp.broadcast_to(gate_row(rows, h, g), (8, 128))
                gk[j * 2 + h, :, g * 128 : (g + 1) * 128] = line

    def scores(qi, j, h, sub, masked):
        rows = pl.ds(sub * RQ, RQ)
        span = (sub + 1) * RQ if masked else BLK
        raw = lax.dot_general(
            qm[qi, h, rows, :],
            kvbuf[j, 0:span, 0:128],
            (((1,), (1,)), ((), ())),
            preferred_element_type=F32,
        )
        gate = gk[j * 2 + h, 0:1, 0:span]
        parts = []
        for g in range(span // 128):
            part = raw[:, g * 128 : (g + 1) * 128] * scale - gate[:, g * 128 : (g + 1) * 128]
            if masked and (g + 1) * 128 > sub * RQ:
                col = lax.broadcasted_iota(jnp.int32, (RQ, 128), 1) + (g * 128 - sub * RQ)
                row = lax.broadcasted_iota(jnp.int32, (RQ, 128), 0)
                part = jnp.where(col <= row, part, -1e30)
            parts.append(part)
        return parts, functools.reduce(jnp.maximum, parts)

    def soften(parts, peak, qi, j, h, sub):
        rows = pl.ds(sub * RQ, RQ)
        peak = jnp.max(peak, axis=1, keepdims=True)
        g_here = gq[qi, h, rows, :]
        old = mst[qi, h, rows, :]
        new = jnp.maximum(old, peak + g_here)
        alpha = jnp.exp2(old - new)
        shift = new - g_here
        weights_ = [jnp.exp2(part - shift) for part in parts]
        mst[qi, h, rows, :] = new
        lst[qi, h, rows, :] = lst[qi, h, rows, :] * alpha + functools.reduce(jnp.add, weights_)
        return jnp.concatenate([a.astype(BF16) for a in weights_], axis=1), alpha

    def hold(parts, peak):
        for g, part in enumerate(parts):
            sbuf[:, g * 128 : (g + 1) * 128] = part
        mbuf[...] = peak

    def held():
        return [sbuf[:, g * 128 : (g + 1) * 128] for g in range(BLK // 128)], mbuf[...]

    def spread(w, alpha, qi, j, h, sub, masked):
        rows = pl.ds(sub * RQ, RQ)
        span = (sub + 1) * RQ if masked else BLK
        mask = head_lanes(h)
        v = kvbuf[j, 0:span, 128:256] * jnp.where(mask, 1.0, 0.0).astype(BF16)
        update = jnp.dot(w, v, preferred_element_type=F32)
        acc[qi, rows, :] = acc[qi, rows, :] * jnp.where(mask, alpha, 1.0) + update

    def tiles(qi, j, h, masked):
        count = BLK // RQ
        ahead = scores(qi, j, h, 0, masked)
        for sub in range(count):
            here = ahead
            ahead = scores(qi, j, h, sub + 1, masked) if sub + 1 < count else None
            w, alpha = soften(*here, qi, j, h, sub)
            spread(w, alpha, qi, j, h, sub, masked)

    blocks_of = (sp, pair_sp)

    def attend(step):
        row = jnp.where(step == 0, z, jnp.where(step == 2, zd, jnp.where(step == 3, zu, zf)))
        second = step == 1
        none = 99
        slots = (
            jnp.where(second, zd * 4 + x, row * 4 + mate),
            jnp.where(second, zu * 4 + x, row * 4 + opp),
            jnp.where(second, none, row * 4 + diag),
            jnp.where(step == 0, sp, jnp.where(step == 3, zf * 4 + x, none)),
        )
        for j in slots:
            pl.when(j <= jnp.maximum(sp, pair_sp))(functools.partial(gate_rows, j))

        found, count = [], 0
        for qi in range(2):
            for j in slots:
                flag = jnp.where((j < blocks_of[qi]) & (step != 4 + qi), 1, 0)
                found.append((qi, j, flag, count))
                count = count + flag
        units = count * heads

        def place(u):
            v = jnp.clip(u, 0, units - 1)
            k = v // heads
            hits = [(qi, j, jnp.where(before_ == k, flag, 0)) for qi, j, flag, before_ in found]
            qi = sum(hit * qi for qi, _, hit in hits)
            j = sum(hit * j for _, j, hit in hits)
            return jnp.where(u == v, qi, 2), j, v % heads

        def two_units(i, _):
            spread(pbuf[...], abuf[...], *place(2 * i - 1), 1, False)
            here = held()
            for t in range(4):
                now = place(2 * i + t // 2)
                ahead = scores(*place(2 * i + (t + 1) // 2), (t + 1) % 2, False)
                w, alpha = soften(*here, *now, t % 2)
                if t < 3:
                    spread(w, alpha, *now, t % 2, False)
                here = ahead
            hold(*here)
            pbuf[...] = w
            abuf[...] = alpha
            return 0

        @pl.when(units > 0)
        def _():
            hold(*scores(*place(0), 0, False))
            steps = (units + 1) // 2
            lax.fori_loop(0, steps, two_units, 0)
            spread(pbuf[...], abuf[...], *place(2 * steps - 1), 1, False)

        @pl.when((step == 0) | (step == 2 + z % 2))
        def _():
            qi = jnp.where(step == 0, 0, 1)

            def for_head(h, _):
                tiles(qi, jnp.where(step == 0, sp, pair_sp), h, True)
                return 0

            lax.fori_loop(0, heads, for_head, 0)

    def pass_on(tag, name, from_z, dev, landing_z, sends, receives):
        col = cols[tag]

        def ends():
            src = kvbuf.at[from_z * 4 + col]
            return src, src, dev, kvbuf.at[landing_z * 4 + col]

        send(name + tag, ends, sends, receives)

    m_d, m_u, m_f = yd * 2 + c, yu * 2 + c, yf * 2 + c
    s_d, s_u, s_f = yd * 2 + 1 - c, yu * 2 + 1 - c, yf * 2 + 1 - c

    def pass_x2(tag, zz, name, col, dev, start=0, size=UP, now=None):
        def ends():
            src = up_block(zz * 4 + col, start, size)
            return src, src, dev, up_block(zz * 4 + xf, start, size)

        return send(name + tag, ends, now=now)

    uhalf = UP // 2

    def both_ways(tag, zz):
        pass_x2(tag, zz, "wx2r", xl, right, 0, uhalf)
        pass_x2(tag, zz, "wx2l", xr, left, uhalf, uhalf)

    def down_pair(name, zz, first, dev, landing):
        def ends():
            src = down_blocks(zz * 4 + first, 2)
            return src, src, dev, down_blocks(landing * 4 + first, 2)

        send(name, ends)

    keep0 = head_lanes(0)
    slot = tp * 2 + role

    def own_rows(t):
        return pl.ds(pl.multiple_of(t * OWN, 32), OWN)

    def finish_out(qi):
        l0 = jnp.sum(lst[qi, 0], axis=1, keepdims=True)
        l1 = jnp.sum(lst[qi, 1], axis=1, keepdims=True)
        outv[qi] = (acc[qi] / jnp.where(keep0, l0, l1)).astype(BF16)

    def send_out(name, qi, d):
        def ends():
            t, s = (tp + d) % 8, (tp + 8 - d) % 8
            dev = ((sp, pair_sp)[qi], t // 2, t % 2)
            from_role = (role, 1 - role)[qi]
            return outv.at[qi, own_rows(t)], arrived.at[slot], dev, arrived.at[s * 2 + from_role]

        send(name + "%d" % d, ends)

    pair_sent = []

    def one_step(step, _):
        attend(step)

        @pl.when(step == 1)
        def _():
            take("wz1u", "wz1d")
            send("wz2u", lambda: (up_block(b_d, 0, uhalf), up_block(b_d, 0, uhalf), above, up_block(b_f, 0, uhalf)))
            send("wz2d", lambda: (up_block(b_u, uhalf, uhalf), up_block(b_u, uhalf, uhalf), below, up_block(b_f, uhalf, uhalf)))
            pass_x("d", zd)
            pass_x("u", zu)
            take("y1u", "y1d")
            send("y2u", lambda: (mix_rows(m_d, 0, 128), mix_rows(m_d, 0, 128), y_up, mix_rows(m_f, 0, 128)))
            send("y2d", lambda: (mix_rows(m_u, 128, 128), mix_rows(m_u, 128, 128), y_down, mix_rows(m_f, 128, 128)))
            send("s1", lambda: (mix_rows(m_d), mix_rows(m_d), sibling, mix_rows(s_d)))
            send("s2", lambda: (mix_rows(m_u), mix_rows(m_u), sibling, mix_rows(s_u)))
            take("z1u_mate", "z1d_mate")
            pass_on("mate", "z2u_", zd, above, zf, lambda: z >= 1, lambda: z != 1)
            take("z1u_opp", "z1d_opp", "z1u_diag", "z1d_diag")
            pass_on("opp", "z2d_", zu, below, zf, lambda: z != 2, lambda: z != 1)
            pass_on("diag", "z2d_", zu, below, zf, lambda: z != 2, lambda: z != 1)
            take("wx1r0", "wx1l0")
            both_ways("0", z)

        @pl.when(step == 2)
        def _():
            take("z2u_own", "z2x_own")
            take("wz2u", "wz2d")
            pass_x("f", zf)

        @pl.when(step == 2)
        def _():
            take("wx1rd", "wx1ld", "wx1ru", "wx1lu")
            both_ways("d", zd)
            both_ways("u", zu)

        @pl.when(step == 3)
        def _():
            take("y2u", "y2d")
            send("s3", lambda: (mix_rows(m_f), mix_rows(m_f), sibling, mix_rows(s_f)))
            take("z2u_mate", "z2d_opp", "z2d_diag")
            take("bx2r", "bx2l")
            down_pair("bz1u", z, 0, above, zd)
            down_pair("bz1d", z, 2, below, zu)

        @pl.when(step == 4)
        def _():
            finish_out(1)
            for d in range(8):
                send_out("p", 1, d)
                pair_sent.append(sent.pop())

        return 0

    lax.fori_loop(0, 6, one_step, 0)
    finish_out(0)
    for d in range(1, 8):
        send_out("a", 0, d)
    for wait in pair_sent:
        wait()
    far_waits = [incoming.pop("wx1rf"), incoming.pop("wx1lf")]
    is_large = lambda: role == 1

    @pl.when(role == 1)
    def _():
        for wait in far_waits:
            wait()

    far_sends = [
        pass_x2("f", zf, "wx2r", xl, right, 0, uhalf, is_large),
        pass_x2("f", zf, "wx2l", xr, left, uhalf, uhalf, is_large),
    ]
    arrived[slot] = outv[0, own_rows(tp), :]
    take("s0", "s1", "s2", "s3")
    for d in range(8):
        take("p%d" % d)
        if d:
            take("a%d" % d)

    @pl.when(role == 0)
    def _():
        for wait in far_waits:
            wait()
        for start in far_sends:
            start()

    take("bz1u", "bz1d")
    down_pair("bz2u", zd, 0, above, zf)
    down_pair("bz2d", zu, 2, below, zf)
    down_pair("bz3u", z, 2, above, zd)
    down_pair("bz3d", z, 0, below, zu)

    def project(i, _):
        col = pl.ds(pl.multiple_of(i * 1024, 1024), 1024)
        lhs = jnp.concatenate([arrived[s] for s in range(16)], axis=1)
        part = jnp.dot(lhs, mixbuf[:, col], preferred_element_type=F32)
        ybuf[:, col] = residual_scale * res_ref[:, col].astype(F32) + part
        return 0

    lax.fori_loop(0, 2, project, 0)

    def norm(values, gain):
        center = jnp.mean(values, axis=1, keepdims=True)
        off = values - center
        spread = jnp.mean(jnp.square(off), axis=1, keepdims=True)
        return off * lax.rsqrt(spread + epsilon) * gain

    def first_norm(i, _):
        r = pl.ds(pl.multiple_of(i * 48, 48), 48)
        t = pl.ds(pl.multiple_of(tp * OWN + i * 48, 48), 48)
        mixed[t, :] = norm(ybuf[r, :], mgain_ref[...]).astype(BF16)
        return 0

    lax.fori_loop(0, OWN // 48, first_norm, 0)

    def rows_of(t, start=0, size=OWN):
        return mixed.at[pl.ds(pl.multiple_of(t * OWN + start, 16), size)]

    send("gu", lambda: (rows_of(tp), rows_of(tp), y_up, rows_of(m_d)))
    send("gd", lambda: (rows_of(tp), rows_of(tp), y_down, rows_of(m_u)))
    send("gs", lambda: (rows_of(tp), rows_of(tp), sibling, rows_of(y * 2 + 1 - c)))
    take("wx2r0", "wx2l0", "wx2rd", "wx2ld", "wx2ru", "wx2lu", "wx2rf", "wx2lf")

    def up_group(*chips):
        def some(start, width):
            cols_ = pl.ds(start, width)
            rhs = jnp.concatenate([wbuf[b, cols_, :] for b in range(16)], axis=1)
            lhs = [mixed[pl.ds(pl.multiple_of(yy * 192, 64), 192), :] for yy in chips]
            part = lax.dot_general(
                jnp.concatenate(lhs, axis=0), rhs, (((1,), (1,)), ((), ())), preferred_element_type=F32
            ).astype(BF16)
            for k, yy in enumerate(chips):
                into = pl.ds(pl.multiple_of(yy * 192 + 16, 16), 192)
                both[into, cols_] = part[k * 192 : (k + 1) * 192]

        some(0, UP)

    def send_halo():
        pltpu.make_async_remote_copy(
            src_ref=both.at[pl.ds(BLK, 16)],
            dst_ref=halo,
            send_sem=ssem.at[HALO_SEM],
            recv_sem=rsem.at[HALO_SEM],
            device_id=after,
            device_id_type=MESH,
        ).start()

    def wait_halo(which):
        copy = pltpu.make_async_remote_copy(
            src_ref=both.at[pl.ds(BLK, 16)],
            dst_ref=halo,
            send_sem=ssem.at[HALO_SEM],
            recv_sem=rsem.at[HALO_SEM],
            device_id=after,
            device_id_type=MESH,
        )
        copy.wait_recv() if which else copy.wait_send()

    taps[0:3, 0:640] = vtaps_ref[:, 0:640]
    taps[0:3, 640:1280] = gtaps_ref[:, 0:640]
    taps[0:3, 1280:1408] = jnp.concatenate([vtaps_ref[:, 640:704], gtaps_ref[:, 640:704]], axis=1)

    def filtered(a, lanes_):
        n = a.shape[0] - 16
        return (
            taps[0:1, lanes_] * a[14 : 14 + n]
            + taps[1:2, lanes_] * a[15 : 15 + n]
            + taps[2:3, lanes_] * a[16 : 16 + n]
        )

    def hidden_rows(i):
        src = pl.ds(pl.multiple_of(i * OWN, 32), OWN + 16)
        dst = pl.ds(pl.multiple_of(i * OWN, 32), OWN)
        for g in range(6):
            if g < 5:
                at_v, at_g = slice(g * 128, (g + 1) * 128), slice(640 + g * 128, 768 + g * 128)
                fv = filtered(both[src, at_v].astype(F32), at_v)
                fg = filtered(both[src, at_g].astype(F32), at_g)
            else:
                last = slice(1280, 1408)
                fv = filtered(both[src, last].astype(F32), last)
                fg = pltpu.roll(fv, 64, 1)
            value = fg / (1.0 + jnp.exp(-fg)) * fv
            if g == 5:
                value = jnp.where(lane < 64, value, 0.0)
            hid[dst, g * 128 : (g + 1) * 128] = value.astype(BF16)

    def hidden_group(yy):
        @pl.when(yy == 0)
        def _():
            wait_halo(True)
            both[0:16, :] = jnp.where(sp == 0, 0.0, halo[...].astype(F32)).astype(BF16)

        def chunk(i, _):
            hidden_rows(yy * 2 + i)
            return 0

        lax.fori_loop(0, 2, chunk, 0)

    def down_group(g, yy):
        mine = hid[pl.ds(pl.multiple_of(yy * 192 + c * OWN, 32), OWN), :]
        other = hid[pl.ds(pl.multiple_of(yy * 192 + (1 - c) * OWN, 32), OWN), :]
        lhs = jnp.concatenate([mine, other], axis=0)

        def some(i, _):
            col = pl.ds(pl.multiple_of(i * 1024, 1024), 1024)
            rhs = jnp.concatenate([wbuf[8 * i + k, 1408 : WROWS + 64, :] for k in range(8)], axis=1)
            part = jnp.dot(lhs, rhs, preferred_element_type=F32)
            keep[g, :, col] = part[:OWN]
            sib_out[g, :, col] = part[OWN:].astype(BF16)
            return 0

        lax.fori_loop(0, 2, some, 0)

    def send_sib(g):
        send("r%d" % g, lambda: (sib_out.at[g], sib_in.at[g], sibling, sib_in.at[g]))

    def pair_sum(g, lo, hi):
        return keep[g, :, lo:hi] + sib_in[g, :, lo:hi].astype(F32)

    def near(k, h):
        send(
            "n%d%d" % (k, h),
            lambda: (near_out.at[k, h], near_in.at[k, h], (y_up, y_down)[k], near_in.at[k, h]),
        )

    take("gs")
    up_group(y)
    pl.when(y == 3)(send_halo)
    take("gu", "gd")
    send("g2u", lambda: (rows_of(m_d, 0, 48), rows_of(m_d, 0, 48), y_up, rows_of(m_f, 0, 48)))
    send("g2d", lambda: (rows_of(m_u, 48, 48), rows_of(m_u, 48, 48), y_down, rows_of(m_f, 48, 48)))
    send("gs1", lambda: (rows_of(m_d), rows_of(m_d), sibling, rows_of(s_d)))
    send("gs2", lambda: (rows_of(m_u), rows_of(m_u), sibling, rows_of(s_u)))
    take("gs1", "gs2")
    up_group(yd, yu)
    pl.when((yd == 3) | (yu == 3))(send_halo)
    take("g2u", "g2d")
    send("gs3", lambda: (rows_of(m_f), rows_of(m_f), sibling, rows_of(s_f)))
    take("bz2u", "bz2d", "bz3u", "bz3d")
    hidden_group(yu)
    down_group(2, yu)
    send_sib(2)
    take("gs3")
    up_group(yf)
    pl.when(yf == 3)(send_halo)
    take("r2")
    near_out[0, 1] = pair_sum(2, HALF, 2 * HALF).astype(BF16)
    near(0, 1)
    hidden_group(yf)
    down_group(0, yf)
    send_sib(0)
    hidden_group(yd)
    take("r0")
    far_out[0] = pair_sum(0, 0, HALF).astype(BF16)
    far_out[1] = pair_sum(0, HALF, 2 * HALF).astype(BF16)
    send("fu", lambda: (far_out.at[0], far_in.at[0], y_up, far_in.at[0]))
    send("fd", lambda: (far_out.at[1], far_in.at[1], y_down, far_in.at[1]))
    down_group(1, yd)
    send_sib(1)
    hidden_group(y)
    take("r1")
    near_out[1, 0] = pair_sum(1, 0, HALF).astype(BF16)
    near(1, 0)
    down_group(3, y)
    send_sib(3)

    take("fu")
    near_out[0, 0] = (pair_sum(2, 0, HALF) + far_in[0].astype(F32)).astype(BF16)
    near(0, 0)
    take("fd")
    near_out[1, 1] = (pair_sum(1, HALF, 2 * HALF) + far_in[1].astype(F32)).astype(BF16)
    near(1, 1)
    take("r3", "n00", "n01", "n10", "n11")

    def last_norm(i, _):
        r = pl.ds(pl.multiple_of(i * 48, 48), 48)
        t = pl.ds(pl.multiple_of(tp * OWN + i * 48, 48), 48)
        far = [near_in[0, h, r, :].astype(F32) + near_in[1, h, r, :].astype(F32) for h in range(2)]
        ffn = keep[3, r, :] + sib_in[3, r, :].astype(F32) + jnp.concatenate(far, axis=1)
        whole = residual_scale * mixed[t, :].astype(F32) + ffn
        out_ref[r, :] = norm(whole, fgain_ref[...]).astype(BF16)
        return 0

    lax.fori_loop(0, OWN // 48, last_norm, 0)
    wait_halo(False)
    for wait in sent:
        wait()


def whole_layer(*operands):
    vmem = pl.BlockSpec(memory_space=pltpu.VMEM)
    return pl.pallas_call(
        layer_kernel,
        out_shape=jax.ShapeDtypeStruct((OWN, 2048), BF16),
        in_specs=[vmem] * len(operands),
        out_specs=vmem,
        scratch_shapes=[
            pltpu.VMEM((2, BLK + EXTRA, 256), BF16),
            pltpu.VMEM((2, BLK, 128), BF16),
            pltpu.VMEM((16, BLK + EXTRA, 256), BF16),
            pltpu.VMEM((BLK, 128), BF16),
            pltpu.VMEM((EXTRA, 256), BF16),
            pltpu.VMEM((3, 2, BLK, 128), BF16),
            pltpu.VMEM((3, 2, BLK, 128), F32),
            pltpu.VMEM((32, 8, BLK), F32),
            pltpu.VMEM((3, 2, BLK, 128), F32),
            pltpu.VMEM((3, 2, BLK, 128), F32),
            pltpu.VMEM((3, BLK, 128), F32),
            pltpu.VMEM((RQ, BLK), F32),
            pltpu.VMEM((RQ, 128), F32),
            pltpu.VMEM((RQ, BLK), BF16),
            pltpu.VMEM((RQ, 128), F32),
            pltpu.VMEM((2, BLK, 128), BF16),
            pltpu.VMEM((16, WROWS + 64, 128), BF16),
            pltpu.VMEM((2048, 2048), BF16),
            pltpu.VMEM((16, OWN, 128), BF16),
            pltpu.VMEM((OWN, 2048), F32),
            pltpu.VMEM((BLK, 2048), BF16),
            pltpu.VMEM((BLK + 16, 1408), BF16),
            pltpu.VMEM((16, 1408), BF16),
            pltpu.VMEM((8, 1408), F32),
            pltpu.VMEM((BLK, 768), BF16),
            pltpu.VMEM((4, OWN, 2048), F32),
            pltpu.VMEM((4, OWN, 2048), BF16),
            pltpu.VMEM((4, OWN, 2048), BF16),
            pltpu.VMEM((2, OWN, HALF), BF16),
            pltpu.VMEM((2, OWN, HALF), BF16),
            pltpu.VMEM((2, 2, OWN, HALF), BF16),
            pltpu.VMEM((2, 2, OWN, HALF), BF16),
            pltpu.SemaphoreType.DMA((112,)),
            pltpu.SemaphoreType.DMA((112,)),
            pltpu.SemaphoreType.DMA((2,)),
        ],
        compiler_params=pltpu.CompilerParams(
            collective_id=1, has_side_effects=True, vmem_limit_bytes=VMEM_ALL
        ),
        cost_estimate=pl.CostEstimate(flops=20_000_000_000, bytes_accessed=40_000_000, transcendentals=0),
    )(*operands)


def per_device(
    query_small,
    key_small,
    value_small,
    gates_small,
    query_large,
    key_large,
    value_large,
    gates_large,
    residual,
    mixer_small,
    mixer_large,
    mix_gain,
    value_weight,
    gate_weight,
    value_taps,
    gate_taps,
    down_weight,
    final_gain,
):
    return whole_layer(
        query_small,
        key_small,
        value_small,
        query_large,
        key_large,
        value_large,
        gates_small.T,
        gates_large.T,
        value_weight.T,
        gate_weight.T,
        down_weight,
        mixer_small,
        mixer_large,
        residual,
        mix_gain[None],
        final_gain[None],
        value_taps,
        gate_taps,
    )


def solution(mesh):
    split = Mesh(mesh.devices.reshape(mesh.shape["sp"], 4, 2), ("sp", "tp_0", "tp_1"))
    placed = (
        P("sp", TP),
        P("sp", TP),
        P("sp", TP),
        P("sp", TP),
        P("sp", TP),
        P("sp", TP),
        P("sp", TP),
        P("sp", TP),
        P(SP_TP, None),
        P(TP, None),
        P(TP, None),
        P(),
        P("sp", TP),
        P("sp", TP),
        P(None, TP),
        P(None, TP),
        P(TP, "sp"),
        P(),
    )
    return jax.shard_map(
        per_device, mesh=split, in_specs=placed, out_specs=P(SP_TP, None), check_vma=False
    )
```

```python
import functools

import jax
import jax.numpy as jnp
from jax import lax
from jax.experimental import pallas as pl
from jax.experimental.pallas import tpu as pltpu
from jax.sharding import Mesh
from jax.sharding import PartitionSpec as P

TP = ("tp_0", "tp_1")
SP_TP = ("sp", "tp_0", "tp_1")
LOG2E = 1.4426950408889634
residual_scale = 2.0**0.5
epsilon = 1e-05
MESH = pl.DeviceIdType.MESH
BLK = 768
EXTRA = 32
WROWS = 2112
UP = 1408
DOWN = 704
RQ = 384
F32 = jnp.float32
BF16 = jnp.bfloat16
VMEM_ALL = 67_000_000
OWN = 96
HALF = 1024
HALO_SEM = 111


def layer_kernel(
    qs_ref,
    ks_ref,
    vs_ref,
    ql_ref,
    kl_ref,
    vl_ref,
    gs_ref,
    gl_ref,
    vw_ref,
    gw_ref,
    down_ref,
    ms_ref,
    ml_ref,
    res_ref,
    mgain_ref,
    fgain_ref,
    vtaps_ref,
    gtaps_ref,
    out_ref,
    kvin,
    qin,
    kvbuf,
    qpair,
    qgate,
    qm,
    gq,
    gk,
    mst,
    lst,
    acc,
    sbuf,
    mbuf,
    pbuf,
    abuf,
    outv,
    wbuf,
    mixbuf,
    arrived,
    ybuf,
    mixed,
    both,
    halo,
    taps,
    hid,
    keep,
    sib_out,
    sib_in,
    far_out,
    far_in,
    near_out,
    near_in,
    ssem,
    rsem,
    lsem,
):
    sp = lax.axis_index("sp")
    y = lax.axis_index("tp_0")
    c = lax.axis_index("tp_1")
    z, x = sp // 4, sp % 4
    role = x // 2
    xr, xl = (x + 1) % 4, (x + 3) % 4
    zu, zd = (z + 1) % 4, (z + 3) % 4
    yu, yd = (y + 1) % 4, (y + 3) % 4
    xf, zf, yf = (x + 2) % 4, (z + 2) % 4, (y + 2) % 4
    mate = x + 1 - 2 * (x % 2)
    opp = 3 - x
    diag = opp + 1 - 2 * (opp % 2)
    pair_sp = 15 - sp
    tp = y * 2 + c

    def at(zz, xx):
        return (zz * 4 + xx, y, c)

    right, left = at(z, xr), at(z, xl)
    above, below = at(zu, x), at(zd, x)
    mate_dev, opp_dev = at(z, mate), at(z, opp)
    pair_dev = (pair_sp, y, c)
    y_up, y_down = (sp, yu, c), (sp, yd, c)
    sibling = (sp, y, 1 - c)
    after, before = ((sp + 1) % 16, y, c), ((sp + 15) % 16, y, c)

    barrier = pltpu.get_barrier_semaphore()
    greeted = [right, left, above, below, after, before]
    for d in range(8):
        t = (tp + d) % 8
        if d:
            greeted.append((sp, t // 2, t % 2))
        greeted.append((pair_sp, t // 2, t % 2))
    for dev in greeted:
        pl.semaphore_signal(barrier, inc=1, device_id=dev, device_id_type=MESH)

    lane = lax.broadcasted_iota(jnp.int32, (1, 128), 1)

    for r, (q_ref, k_ref, v_ref, g_ref) in enumerate(
        ((qs_ref, ks_ref, vs_ref, gs_ref), (ql_ref, kl_ref, vl_ref, gl_ref))
    ):
        kvin[r, 0:BLK, 0:128] = k_ref[...]
        kvin[r, 0:BLK, 128:256] = v_ref[...]
        qin[r] = q_ref[...]
        pieces = []
        for h in range(2 - r):
            left_over = g_ref[h : h + 1, :] * LOG2E
            for i in range(3):
                part = left_over.astype(BF16).astype(F32)
                left_over = left_over - part
                pieces += [part[:, p * 256 : (p + 1) * 256] for p in range(3)]
        pieces.append(jnp.zeros((EXTRA - len(pieces), 256), F32))
        kvin[r, BLK : BLK + EXTRA, :] = jnp.concatenate(pieces, axis=0).astype(BF16)

    def mix_rows(t, start=0, size=256):
        return mixbuf.at[pl.ds(pl.multiple_of(t * 256 + start, 128), size)]

    def up_block(b, start=0, size=UP):
        return wbuf.at[b, pl.ds(start, size)]

    def down_blocks(b, count=1, start=0, size=DOWN):
        return wbuf.at[pl.ds(b, count), pl.ds(UP + start, size)]

    wbuf[sp, 0:640, :] = vw_ref[0:640, :]
    wbuf[sp, 640:1280, :] = gw_ref[0:640, :]
    wbuf[sp, 1280:1344, :] = vw_ref[640:704, :]
    wbuf[sp, 1344:1408, :] = gw_ref[640:704, :]
    wbuf[sp, 1408:WROWS, :] = down_ref[...]
    for b in range(16):
        wbuf[b, WROWS : WROWS + 64, :] = jnp.zeros((64, 128), BF16)
    mixbuf[pl.ds(pl.multiple_of(tp * 256, 256), 128), :] = ms_ref[...]
    mixbuf[pl.ds(pl.multiple_of(tp * 256 + 128, 128), 128), :] = ml_ref[...]

    pl.semaphore_wait(barrier, len(greeted))

    sent = []
    counter = [0]
    incoming = {}

    def send(name, ends, sends=None, receives=None, now=None):
        k = counter[0]
        counter[0] += 1

        def copy(arriving):
            src, dst, dev, landing = ends()
            return pltpu.make_async_remote_copy(
                src_ref=landing if arriving else src,
                dst_ref=landing if arriving else dst,
                send_sem=ssem.at[k],
                recv_sem=rsem.at[k],
                device_id=dev,
                device_id_type=MESH,
            )

        def only(condition, act):
            act() if condition is None else pl.when(condition())(act)

        sent.append(lambda: only(sends, lambda: copy(False).wait_send()))
        incoming[name] = lambda: only(receives, lambda: copy(True).wait_recv())
        only(now or sends, lambda: copy(False).start())
        return lambda: copy(False).start()

    def take(*names):
        for name in names:
            incoming.pop(name)()

    cols = {"own": x, "mate": mate, "opp": opp, "diag": diag}

    send("x1m", lambda: (kvin.at[role], kvbuf.at[sp], mate_dev, kvbuf.at[z * 4 + mate]))
    send("x1o", lambda: (kvin.at[1 - role], kvbuf.at[sp], opp_dev, kvbuf.at[z * 4 + opp]))
    send("z1u_own", lambda: (kvin.at[role], kvbuf.at[sp], above, kvbuf.at[zd * 4 + x]))
    send("z1d_own", lambda: (kvin.at[role], kvbuf.at[sp], below, kvbuf.at[zu * 4 + x]), lambda: z < 3, lambda: z != 2)
    gate_part = pl.ds(BLK, EXTRA)
    send("qg", lambda: (kvin.at[1 - role, gate_part], qgate, pair_dev, qgate))
    send("q", lambda: (qin.at[1 - role], qpair, pair_dev, qpair))
    send("y1u", lambda: (mix_rows(tp), mix_rows(tp), y_up, mix_rows(yd * 2 + c)))
    send("y1d", lambda: (mix_rows(tp), mix_rows(tp), y_down, mix_rows(yu * 2 + c)))
    send("s0", lambda: (mix_rows(tp), mix_rows(tp), sibling, mix_rows(y * 2 + 1 - c)))

    def pass_x(tag, zz):
        def ends(dev, col):
            mine = up_block(zz * 4 + x)
            return mine, mine, dev, up_block(zz * 4 + col)

        send("wx1r" + tag, lambda: ends(right, xl))
        send("wx1l" + tag, lambda: ends(left, xr))

    own_kv = pltpu.make_async_copy(kvin.at[role], kvbuf.at[sp], lsem.at[0])
    own_kv.start()

    heads = 2 - role
    head_dim = 64 + 64 * role
    scale = jnp.where(role == 0, 0.125 * LOG2E, 128.0**-0.5 * LOG2E).astype(F32)

    def head_lanes(h):
        return (lane >= h * 64) & (lane < h * 64 + head_dim)

    def gate_row(rows, h, g):
        k, at_ = h * 9 + g // 2, slice((g % 2) * 128, (g % 2) * 128 + 128)
        return rows[k : k + 1, at_] + rows[k + 3 : k + 4, at_] + rows[k + 6 : k + 7, at_]

    same = lax.broadcasted_iota(jnp.int32, (128, 128), 0) == lax.broadcasted_iota(
        jnp.int32, (128, 128), 1
    )

    def load_queries(qi, queries, gate_block):
        rows = gate_block.astype(F32)
        for h in range(2):
            ones = jnp.where(head_lanes(h), 1.0, 0.0).astype(BF16)
            qm[qi, h] = queries * ones
            for g in range(BLK // 128):
                line = jnp.broadcast_to(gate_row(rows, h, g), (128, 128))
                column = jnp.sum(jnp.where(same, line, 0.0), axis=1, keepdims=True)
                gq[qi, h, g * 128 : (g + 1) * 128, :] = jnp.broadcast_to(column, (128, 128))

    load_queries(0, qin[role], kvin[role, BLK : BLK + EXTRA, :])
    mst[...] = jnp.full(mst.shape, -1e30, F32)
    lst[...] = jnp.zeros(lst.shape, F32)
    acc[...] = jnp.zeros(acc.shape, F32)

    def pass_z(tag):
        col = cols[tag]
        src = kvbuf.at[z * 4 + col]
        send("z1u_" + tag, lambda: (src, src, above, kvbuf.at[zd * 4 + col]))
        send("z1d_" + tag, lambda: (src, src, below, kvbuf.at[zu * 4 + col]), lambda: z < 3, lambda: z != 2)

    b_d, b_u, b_f = zd * 4 + x, zu * 4 + x, zf * 4 + x
    b_l, b_r, b_o = z * 4 + xl, z * 4 + xr, z * 4 + (x + 2) % 4
    dhalf = DOWN // 2
    take("x1o")
    send("x2", lambda: (kvbuf.at[z * 4 + opp], kvbuf.at[z * 4 + opp], mate_dev, kvbuf.at[z * 4 + diag]))
    pass_z("opp")
    take("x1m")
    pass_z("mate")
    send("wz1u", lambda: (up_block(sp), up_block(sp), above, up_block(b_d)))
    send("wz1d", lambda: (up_block(sp), up_block(sp), below, up_block(b_u)))
    send("bx1r", lambda: (down_blocks(sp), down_blocks(sp), right, down_blocks(b_l)))
    send("bx1l", lambda: (down_blocks(sp), down_blocks(sp), left, down_blocks(b_r)))
    pass_x("0", z)
    own_kv.wait()
    take("x2")
    pass_z("diag")
    take("z1u_own", "z1d_own")
    send(
        "z2u_own",
        lambda: (kvbuf.at[zd * 4 + x], kvbuf.at[zd * 4 + x], above, kvbuf.at[zf * 4 + x]),
        lambda: z >= 2,
        lambda: (z == 0) | (z == 3),
    )
    send(
        "z2x_own",
        lambda: (kvbuf.at[zu * 4 + x], kvbuf.at[zu * 4 + x], below, kvbuf.at[zf * 4 + x]),
        lambda: z == 3,
        lambda: z == 2,
    )
    take("bx1r", "bx1l")
    send(
        "bx2r",
        lambda: (down_blocks(b_l, 1, 0, dhalf), down_blocks(b_l, 1, 0, dhalf), right, down_blocks(b_o, 1, 0, dhalf)),
    )
    send(
        "bx2l",
        lambda: (down_blocks(b_r, 1, dhalf, dhalf), down_blocks(b_r, 1, dhalf, dhalf), left, down_blocks(b_o, 1, dhalf, dhalf)),
    )
    take("q", "qg")
    load_queries(1, qpair[...], qgate[...])

    def gate_rows(j):
        rows = kvbuf[j, BLK : BLK + EXTRA, :].astype(F32)
        for h in range(2):
            for g in range(BLK // 128):
                line = jnp.broadcast_to(gate_row(rows, h, g), (8, 128))
                gk[j * 2 + h, :, g * 128 : (g + 1) * 128] = line

    def scores(qi, j, h, sub, masked):
        rows = pl.ds(sub * RQ, RQ)
        span = (sub + 1) * RQ if masked else BLK
        raw = lax.dot_general(
            qm[qi, h, rows, :],
            kvbuf[j, 0:span, 0:128],
            (((1,), (1,)), ((), ())),
            preferred_element_type=F32,
        )
        gate = gk[j * 2 + h, 0:1, 0:span]
        parts = []
        for g in range(span // 128):
            part = raw[:, g * 128 : (g + 1) * 128] * scale - gate[:, g * 128 : (g + 1) * 128]
            if masked and (g + 1) * 128 > sub * RQ:
                col = lax.broadcasted_iota(jnp.int32, (RQ, 128), 1) + (g * 128 - sub * RQ)
                row = lax.broadcasted_iota(jnp.int32, (RQ, 128), 0)
                part = jnp.where(col <= row, part, -1e30)
            parts.append(part)
        return parts, functools.reduce(jnp.maximum, parts)

    def soften(parts, peak, qi, j, h, sub):
        rows = pl.ds(sub * RQ, RQ)
        peak = jnp.max(peak, axis=1, keepdims=True)
        g_here = gq[qi, h, rows, :]
        old = mst[qi, h, rows, :]
        new = jnp.maximum(old, peak + g_here)
        alpha = jnp.exp2(old - new)
        shift = new - g_here
        weights_ = [jnp.exp2(part - shift) for part in parts]
        mst[qi, h, rows, :] = new
        lst[qi, h, rows, :] = lst[qi, h, rows, :] * alpha + functools.reduce(jnp.add, weights_)
        return jnp.concatenate([a.astype(BF16) for a in weights_], axis=1), alpha

    def hold(parts, peak):
        for g, part in enumerate(parts):
            sbuf[:, g * 128 : (g + 1) * 128] = part
        mbuf[...] = peak

    def held():
        return [sbuf[:, g * 128 : (g + 1) * 128] for g in range(BLK // 128)], mbuf[...]

    def spread(w, alpha, qi, j, h, sub, masked):
        rows = pl.ds(sub * RQ, RQ)
        span = (sub + 1) * RQ if masked else BLK
        mask = head_lanes(h)
        v = kvbuf[j, 0:span, 128:256] * jnp.where(mask, 1.0, 0.0).astype(BF16)
        update = jnp.dot(w, v, preferred_element_type=F32)
        acc[qi, rows, :] = acc[qi, rows, :] * jnp.where(mask, alpha, 1.0) + update

    def tiles(qi, j, h, masked):
        count = BLK // RQ
        ahead = scores(qi, j, h, 0, masked)
        for sub in range(count):
            here = ahead
            ahead = scores(qi, j, h, sub + 1, masked) if sub + 1 < count else None
            w, alpha = soften(*here, qi, j, h, sub)
            spread(w, alpha, qi, j, h, sub, masked)

    blocks_of = (sp, pair_sp)

    def attend(step):
        row = jnp.where(step == 0, z, jnp.where(step == 2, zd, jnp.where(step == 3, zu, zf)))
        second = step == 1
        none = 99
        slots = (
            jnp.where(second, zd * 4 + x, row * 4 + mate),
            jnp.where(second, zu * 4 + x, row * 4 + opp),
            jnp.where(second, none, row * 4 + diag),
            jnp.where(step == 0, sp, jnp.where(step == 3, zf * 4 + x, none)),
        )
        for j in slots:
            pl.when((j <= jnp.maximum(sp, pair_sp)) & (step < 5))(functools.partial(gate_rows, j))

        found, count = [], 0
        for qi in range(2):
            for j in slots:
                flag = jnp.where((j < blocks_of[qi]) & (step != 4 + qi), 1, 0)
                found.append((qi, j, flag, count))
                count = count + flag
        units = count * heads

        def place(u):
            v = jnp.clip(u, 0, units - 1)
            k = v // heads
            hits = [(qi, j, jnp.where(before_ == k, flag, 0)) for qi, j, flag, before_ in found]
            qi = sum(hit * qi for qi, _, hit in hits)
            j = sum(hit * j for _, j, hit in hits)
            return jnp.where(u == v, qi, 2), j, v % heads

        def two_units(i, _):
            spread(pbuf[...], abuf[...], *place(2 * i - 1), 1, False)
            here = held()
            for t in range(4):
                now = place(2 * i + t // 2)
                ahead = scores(*place(2 * i + (t + 1) // 2), (t + 1) % 2, False)
                w, alpha = soften(*here, *now, t % 2)
                if t < 3:
                    spread(w, alpha, *now, t % 2, False)
                here = ahead
            hold(*here)
            pbuf[...] = w
            abuf[...] = alpha
            return 0

        @pl.when(units > 0)
        def _():
            hold(*scores(*place(0), 0, False))
            steps = (units + 1) // 2
            lax.fori_loop(0, steps, two_units, 0)
            spread(pbuf[...], abuf[...], *place(2 * steps - 1), 1, False)

        @pl.when((step == 0) | (step == 2 + z % 2))
        def _():
            qi = jnp.where(step == 0, 0, 1)

            def for_head(h, _):
                tiles(qi, jnp.where(step == 0, sp, pair_sp), h, True)
                return 0

            lax.fori_loop(0, heads, for_head, 0)

    def pass_on(tag, name, from_z, dev, landing_z, sends, receives):
        col = cols[tag]

        def ends():
            src = kvbuf.at[from_z * 4 + col]
            return src, src, dev, kvbuf.at[landing_z * 4 + col]

        send(name + tag, ends, sends, receives)

    m_d, m_u, m_f = yd * 2 + c, yu * 2 + c, yf * 2 + c
    s_d, s_u, s_f = yd * 2 + 1 - c, yu * 2 + 1 - c, yf * 2 + 1 - c

    def pass_x2(tag, zz, name, col, dev, start=0, size=UP, now=None):
        def ends():
            src = up_block(zz * 4 + col, start, size)
            return src, src, dev, up_block(zz * 4 + xf, start, size)

        return send(name + tag, ends, now=now)

    uhalf = UP // 2

    def both_ways(tag, zz):
        pass_x2(tag, zz, "wx2r", xl, right, 0, uhalf)
        pass_x2(tag, zz, "wx2l", xr, left, uhalf, uhalf)

    def down_pair(name, zz, first, dev, landing):
        def ends():
            src = down_blocks(zz * 4 + first, 2)
            return src, src, dev, down_blocks(landing * 4 + first, 2)

        send(name, ends)

    keep0 = head_lanes(0)
    slot = tp * 2 + role

    def own_rows(t):
        return pl.ds(pl.multiple_of(t * OWN, 32), OWN)

    def finish_out(qi):
        l0 = jnp.sum(lst[qi, 0], axis=1, keepdims=True)
        l1 = jnp.sum(lst[qi, 1], axis=1, keepdims=True)
        outv[qi] = (acc[qi] / jnp.where(keep0, l0, l1)).astype(BF16)

    def send_out(name, qi, d):
        def ends():
            t, s = (tp + d) % 8, (tp + 8 - d) % 8
            dev = ((sp, pair_sp)[qi], t // 2, t % 2)
            from_role = (role, 1 - role)[qi]
            return outv.at[qi, own_rows(t)], arrived.at[slot], dev, arrived.at[s * 2 + from_role]

        send(name + "%d" % d, ends)

    pair_sent = []

    def one_step(step, _):
        attend(step)

        @pl.when(step == 1)
        def _():
            take("wz1u", "wz1d")
            send("wz2u", lambda: (up_block(b_d, 0, uhalf), up_block(b_d, 0, uhalf), above, up_block(b_f, 0, uhalf)))
            send("wz2d", lambda: (up_block(b_u, uhalf, uhalf), up_block(b_u, uhalf, uhalf), below, up_block(b_f, uhalf, uhalf)))
            pass_x("d", zd)
            pass_x("u", zu)
            take("y1u", "y1d")
            send("y2u", lambda: (mix_rows(m_d, 0, 128), mix_rows(m_d, 0, 128), y_up, mix_rows(m_f, 0, 128)))
            send("y2d", lambda: (mix_rows(m_u, 128, 128), mix_rows(m_u, 128, 128), y_down, mix_rows(m_f, 128, 128)))
            send("s1", lambda: (mix_rows(m_d), mix_rows(m_d), sibling, mix_rows(s_d)))
            send("s2", lambda: (mix_rows(m_u), mix_rows(m_u), sibling, mix_rows(s_u)))
            take("z1u_mate", "z1d_mate")
            pass_on("mate", "z2u_", zd, above, zf, lambda: z >= 1, lambda: z != 1)
            take("z1u_opp", "z1d_opp", "z1u_diag", "z1d_diag")
            pass_on("opp", "z2d_", zu, below, zf, lambda: z != 2, lambda: z != 1)
            pass_on("diag", "z2d_", zu, below, zf, lambda: z != 2, lambda: z != 1)
            take("wx1r0", "wx1l0")
            both_ways("0", z)

        @pl.when(step == 2)
        def _():
            take("z2u_own", "z2x_own")
            take("wz2u", "wz2d")
            pass_x("f", zf)

        @pl.when(step == 2)
        def _():
            take("wx1rd", "wx1ld", "wx1ru", "wx1lu")
            both_ways("d", zd)
            both_ways("u", zu)

        @pl.when(step == 3)
        def _():
            take("y2u", "y2d")
            send("s3", lambda: (mix_rows(m_f), mix_rows(m_f), sibling, mix_rows(s_f)))
            take("z2u_mate", "z2d_opp", "z2d_diag")
            take("bx2r", "bx2l")
            down_pair("bz1u", z, 0, above, zd)
            down_pair("bz1d", z, 2, below, zu)

        @pl.when(step == 4)
        def _():
            finish_out(1)
            for d in range(8):
                send_out("p", 1, d)
                pair_sent.append(sent.pop())

        return 0

    lax.fori_loop(0, 6, one_step, 0)
    finish_out(0)
    for d in range(1, 8):
        send_out("a", 0, d)
    for wait in pair_sent:
        wait()
    take("wx1rf", "wx1lf")
    both_ways("f", zf)
    arrived[slot] = outv[0, own_rows(tp), :]
    take("s0", "s1", "s2", "s3")
    for d in range(8):
        take("p%d" % d)
        if d:
            take("a%d" % d)

    take("bz1u", "bz1d")
    down_pair("bz2u", zd, 0, above, zf)
    down_pair("bz2d", zu, 2, below, zf)
    down_pair("bz3u", z, 2, above, zd)
    down_pair("bz3d", z, 0, below, zu)

    def project(i, _):
        col = pl.ds(pl.multiple_of(i * 1024, 1024), 1024)
        lhs = jnp.concatenate([arrived[s] for s in range(16)], axis=1)
        part = jnp.dot(lhs, mixbuf[:, col], preferred_element_type=F32)
        ybuf[:, col] = residual_scale * res_ref[:, col].astype(F32) + part
        return 0

    lax.fori_loop(0, 2, project, 0)

    def norm(values, gain):
        center = jnp.mean(values, axis=1, keepdims=True)
        off = values - center
        spread = jnp.mean(jnp.square(off), axis=1, keepdims=True)
        return off * lax.rsqrt(spread + epsilon) * gain

    def first_norm(i, _):
        r = pl.ds(pl.multiple_of(i * 48, 48), 48)
        t = pl.ds(pl.multiple_of(tp * OWN + i * 48, 48), 48)
        mixed[t, :] = norm(ybuf[r, :], mgain_ref[...]).astype(BF16)
        return 0

    lax.fori_loop(0, OWN // 48, first_norm, 0)

    def rows_of(t, start=0, size=OWN):
        return mixed.at[pl.ds(pl.multiple_of(t * OWN + start, 16), size)]

    send("gu", lambda: (rows_of(tp), rows_of(tp), y_up, rows_of(m_d)))
    send("gd", lambda: (rows_of(tp), rows_of(tp), y_down, rows_of(m_u)))
    send("gs", lambda: (rows_of(tp), rows_of(tp), sibling, rows_of(y * 2 + 1 - c)))
    take("wx2r0", "wx2l0", "wx2rd", "wx2ld", "wx2ru", "wx2lu", "wx2rf", "wx2lf")

    def up_group(*chips):
        def some(start, width):
            cols_ = pl.ds(start, width)
            rhs = jnp.concatenate([wbuf[b, cols_, :] for b in range(16)], axis=1)
            lhs = [mixed[pl.ds(pl.multiple_of(yy * 192, 64), 192), :] for yy in chips]
            part = lax.dot_general(
                jnp.concatenate(lhs, axis=0), rhs, (((1,), (1,)), ((), ())), preferred_element_type=F32
            ).astype(BF16)
            for k, yy in enumerate(chips):
                into = pl.ds(pl.multiple_of(yy * 192 + 16, 16), 192)
                both[into, cols_] = part[k * 192 : (k + 1) * 192]

        some(0, UP)

    def send_halo():
        pltpu.make_async_remote_copy(
            src_ref=both.at[pl.ds(BLK, 16)],
            dst_ref=halo,
            send_sem=ssem.at[HALO_SEM],
            recv_sem=rsem.at[HALO_SEM],
            device_id=after,
            device_id_type=MESH,
        ).start()

    def wait_halo(which):
        copy = pltpu.make_async_remote_copy(
            src_ref=both.at[pl.ds(BLK, 16)],
            dst_ref=halo,
            send_sem=ssem.at[HALO_SEM],
            recv_sem=rsem.at[HALO_SEM],
            device_id=after,
            device_id_type=MESH,
        )
        copy.wait_recv() if which else copy.wait_send()

    taps[0:3, 0:640] = vtaps_ref[:, 0:640]
    taps[0:3, 640:1280] = gtaps_ref[:, 0:640]
    taps[0:3, 1280:1408] = jnp.concatenate([vtaps_ref[:, 640:704], gtaps_ref[:, 640:704]], axis=1)

    def filtered(a, lanes_):
        n = a.shape[0] - 16
        return (
            taps[0:1, lanes_] * a[14 : 14 + n]
            + taps[1:2, lanes_] * a[15 : 15 + n]
            + taps[2:3, lanes_] * a[16 : 16 + n]
        )

    def hidden_rows(i):
        src = pl.ds(pl.multiple_of(i * OWN, 32), OWN + 16)
        dst = pl.ds(pl.multiple_of(i * OWN, 32), OWN)
        for g in range(6):
            if g < 5:
                at_v, at_g = slice(g * 128, (g + 1) * 128), slice(640 + g * 128, 768 + g * 128)
                fv = filtered(both[src, at_v].astype(F32), at_v)
                fg = filtered(both[src, at_g].astype(F32), at_g)
            else:
                last = slice(1280, 1408)
                fv = filtered(both[src, last].astype(F32), last)
                fg = pltpu.roll(fv, 64, 1)
            value = fg / (1.0 + jnp.exp(-fg)) * fv
            if g == 5:
                value = jnp.where(lane < 64, value, 0.0)
            hid[dst, g * 128 : (g + 1) * 128] = value.astype(BF16)

    def hidden_group(yy):
        @pl.when(yy == 0)
        def _():
            wait_halo(True)
            both[0:16, :] = jnp.where(sp == 0, 0.0, halo[...].astype(F32)).astype(BF16)

        def chunk(i, _):
            hidden_rows(yy * 2 + i)
            return 0

        lax.fori_loop(0, 2, chunk, 0)

    def down_group(g, yy):
        mine = hid[pl.ds(pl.multiple_of(yy * 192 + c * OWN, 32), OWN), :]
        other = hid[pl.ds(pl.multiple_of(yy * 192 + (1 - c) * OWN, 32), OWN), :]
        lhs = jnp.concatenate([mine, other], axis=0)

        def some(i, _):
            col = pl.ds(pl.multiple_of(i * 1024, 1024), 1024)
            rhs = jnp.concatenate([wbuf[8 * i + k, 1408 : WROWS + 64, :] for k in range(8)], axis=1)
            part = jnp.dot(lhs, rhs, preferred_element_type=F32)
            keep[g, :, col] = part[:OWN]
            sib_out[g, :, col] = part[OWN:].astype(BF16)
            return 0

        lax.fori_loop(0, 2, some, 0)

    def send_sib(g):
        send("r%d" % g, lambda: (sib_out.at[g], sib_in.at[g], sibling, sib_in.at[g]))

    def pair_sum(g, lo, hi):
        return keep[g, :, lo:hi] + sib_in[g, :, lo:hi].astype(F32)

    def near(k, h):
        send(
            "n%d%d" % (k, h),
            lambda: (near_out.at[k, h], near_in.at[k, h], (y_up, y_down)[k], near_in.at[k, h]),
        )

    take("gs")
    up_group(y)
    pl.when(y == 3)(send_halo)
    take("gu", "gd")
    send("g2u", lambda: (rows_of(m_d, 0, 48), rows_of(m_d, 0, 48), y_up, rows_of(m_f, 0, 48)))
    send("g2d", lambda: (rows_of(m_u, 48, 48), rows_of(m_u, 48, 48), y_down, rows_of(m_f, 48, 48)))
    send("gs1", lambda: (rows_of(m_d), rows_of(m_d), sibling, rows_of(s_d)))
    send("gs2", lambda: (rows_of(m_u), rows_of(m_u), sibling, rows_of(s_u)))
    take("gs1", "gs2")
    up_group(yd, yu)
    pl.when((yd == 3) | (yu == 3))(send_halo)
    take("g2u", "g2d")
    send("gs3", lambda: (rows_of(m_f), rows_of(m_f), sibling, rows_of(s_f)))
    take("bz2u", "bz2d", "bz3u", "bz3d")
    hidden_group(yu)
    down_group(2, yu)
    send_sib(2)
    take("gs3")
    up_group(yf)
    pl.when(yf == 3)(send_halo)
    take("r2")
    near_out[0, 1] = pair_sum(2, HALF, 2 * HALF).astype(BF16)
    near(0, 1)
    hidden_group(yf)
    down_group(0, yf)
    send_sib(0)
    hidden_group(yd)
    take("r0")
    far_out[0] = pair_sum(0, 0, HALF).astype(BF16)
    far_out[1] = pair_sum(0, HALF, 2 * HALF).astype(BF16)
    send("fu", lambda: (far_out.at[0], far_in.at[0], y_up, far_in.at[0]))
    send("fd", lambda: (far_out.at[1], far_in.at[1], y_down, far_in.at[1]))
    down_group(1, yd)
    send_sib(1)
    hidden_group(y)
    take("r1")
    near_out[1, 0] = pair_sum(1, 0, HALF).astype(BF16)
    near(1, 0)
    down_group(3, y)
    send_sib(3)

    take("fu")
    near_out[0, 0] = (pair_sum(2, 0, HALF) + far_in[0].astype(F32)).astype(BF16)
    near(0, 0)
    take("fd")
    near_out[1, 1] = (pair_sum(1, HALF, 2 * HALF) + far_in[1].astype(F32)).astype(BF16)
    near(1, 1)
    take("r3", "n00", "n01", "n10", "n11")

    def last_norm(i, _):
        r = pl.ds(pl.multiple_of(i * 48, 48), 48)
        t = pl.ds(pl.multiple_of(tp * OWN + i * 48, 48), 48)
        far = [near_in[0, h, r, :].astype(F32) + near_in[1, h, r, :].astype(F32) for h in range(2)]
        ffn = keep[3, r, :] + sib_in[3, r, :].astype(F32) + jnp.concatenate(far, axis=1)
        whole = residual_scale * mixed[t, :].astype(F32) + ffn
        out_ref[r, :] = norm(whole, fgain_ref[...]).astype(BF16)
        return 0

    lax.fori_loop(0, OWN // 48, last_norm, 0)
    wait_halo(False)
    for wait in sent:
        wait()


def whole_layer(*operands):
    vmem = pl.BlockSpec(memory_space=pltpu.VMEM)
    return pl.pallas_call(
        layer_kernel,
        out_shape=jax.ShapeDtypeStruct((OWN, 2048), BF16),
        in_specs=[vmem] * len(operands),
        out_specs=vmem,
        scratch_shapes=[
            pltpu.VMEM((2, BLK + EXTRA, 256), BF16),
            pltpu.VMEM((2, BLK, 128), BF16),
            pltpu.VMEM((16, BLK + EXTRA, 256), BF16),
            pltpu.VMEM((BLK, 128), BF16),
            pltpu.VMEM((EXTRA, 256), BF16),
            pltpu.VMEM((3, 2, BLK, 128), BF16),
            pltpu.VMEM((3, 2, BLK, 128), F32),
            pltpu.VMEM((32, 8, BLK), F32),
            pltpu.VMEM((3, 2, BLK, 128), F32),
            pltpu.VMEM((3, 2, BLK, 128), F32),
            pltpu.VMEM((3, BLK, 128), F32),
            pltpu.VMEM((RQ, BLK), F32),
            pltpu.VMEM((RQ, 128), F32),
            pltpu.VMEM((RQ, BLK), BF16),
            pltpu.VMEM((RQ, 128), F32),
            pltpu.VMEM((2, BLK, 128), BF16),
            pltpu.VMEM((16, WROWS + 64, 128), BF16),
            pltpu.VMEM((2048, 2048), BF16),
            pltpu.VMEM((16, OWN, 128), BF16),
            pltpu.VMEM((OWN, 2048), F32),
            pltpu.VMEM((BLK, 2048), BF16),
            pltpu.VMEM((BLK + 16, 1408), BF16),
            pltpu.VMEM((16, 1408), BF16),
            pltpu.VMEM((8, 1408), F32),
            pltpu.VMEM((BLK, 768), BF16),
            pltpu.VMEM((4, OWN, 2048), F32),
            pltpu.VMEM((4, OWN, 2048), BF16),
            pltpu.VMEM((4, OWN, 2048), BF16),
            pltpu.VMEM((2, OWN, HALF), BF16),
            pltpu.VMEM((2, OWN, HALF), BF16),
            pltpu.VMEM((2, 2, OWN, HALF), BF16),
            pltpu.VMEM((2, 2, OWN, HALF), BF16),
            pltpu.SemaphoreType.DMA((112,)),
            pltpu.SemaphoreType.DMA((112,)),
            pltpu.SemaphoreType.DMA((2,)),
        ],
        compiler_params=pltpu.CompilerParams(
            collective_id=1, has_side_effects=True, vmem_limit_bytes=VMEM_ALL
        ),
        cost_estimate=pl.CostEstimate(flops=20_000_000_000, bytes_accessed=40_000_000, transcendentals=0),
    )(*operands)


def per_device(
    query_small,
    key_small,
    value_small,
    gates_small,
    query_large,
    key_large,
    value_large,
    gates_large,
    residual,
    mixer_small,
    mixer_large,
    mix_gain,
    value_weight,
    gate_weight,
    value_taps,
    gate_taps,
    down_weight,
    final_gain,
):
    return whole_layer(
        query_small,
        key_small,
        value_small,
        query_large,
        key_large,
        value_large,
        gates_small.T,
        gates_large.T,
        value_weight.T,
        gate_weight.T,
        down_weight,
        mixer_small,
        mixer_large,
        residual,
        mix_gain[None],
        final_gain[None],
        value_taps,
        gate_taps,
    )


def solution(mesh):
    split = Mesh(mesh.devices.reshape(mesh.shape["sp"], 4, 2), ("sp", "tp_0", "tp_1"))
    placed = (
        P("sp", TP),
        P("sp", TP),
        P("sp", TP),
        P("sp", TP),
        P("sp", TP),
        P("sp", TP),
        P("sp", TP),
        P("sp", TP),
        P(SP_TP, None),
        P(TP, None),
        P(TP, None),
        P(),
        P("sp", TP),
        P("sp", TP),
        P(None, TP),
        P(None, TP),
        P(TP, "sp"),
        P(),
    )
    return jax.shard_map(
        per_device, mesh=split, in_specs=placed, out_specs=P(SP_TP, None), check_vma=False
    )
```
